32 devices in a mesh: sp: 8 (over z, y), tp: 4 (over x, core).
Axes of the slice: x: 2, y: 2, z: 4, core: 2. Of those that a mesh axis runs over, the one named last changes fastest.
Arguments:
- residual: bfloat16 [4096, 2048], P(('sp', 'tp')), may hold values from -6 to 6
- query_proj: bfloat16 [4096, 2048], P('sp', 'tp'), may hold values from -12 to 12
- key_proj: bfloat16 [4096, 512], P('sp', 'tp'), may hold values from -12 to 12
- value_proj: bfloat16 [4096, 512], P('sp', 'tp'), may hold values from -6 to 6
- query_gain: float32 [128], replicated, may hold values from 0.4 to 4.5
- key_gain: float32 [128], replicated, may hold values from 0.4 to 4.5
- document_ids: int32 [4096], P('sp'), may hold values from 0 to 3, never falling along the last dimension, each value on 1 to 1537 neighbouring positions
- output_weight: bfloat16 [2048, 2048], replicated, may hold values from -0.125 to 0.125
- norm_gain: float32 [2048], replicated, may hold values from 0.1 to 1.9
- expert_ids: int32 [4096, 2], P(('sp', 'tp')), may hold values from 0 to 31, all different within a row; in each aligned block of 128 rows (0 to 127, 128 to 255, ...) at most 16 rows name the same one
- route_weights: float32 [4096, 2], P(('sp', 'tp')), may hold values from 0.2 to 1
- gate_weight: bfloat16 [32, 2048, 512], P(('sp', 'tp')), may hold values from -0.125 to 0.125
- up_weight: bfloat16 [32, 2048, 512], P(('sp', 'tp')), may hold values from -0.125 to 0.125
- down_weight: bfloat16 [32, 512, 2048], P(('sp', 'tp')), may hold values from -0.25 to 0.25
Outputs:
- updated: bfloat16 [4096, 2048], P(('sp', 'tp'))
The draws below stay inside these ranges and needn't reach their ends.
Inputs may be any that keep to these rules, and one draw needn't show every extreme that they name: `document_ids`: document numbers never fall along the positions; each document has at most 1537 positions, and one has exactly 1537. `expert_ids`: each row names 2 different experts; within the rows of one device no expert is named more than 16 times, and in some device's rows an expert is named exactly 16 times.
All inputs are finite; a program needn't handle non-finite values.
Results may differ from the reference program's by a relative error of at most 0.017.
Values may be sent and summed in bfloat16 or wider, within the bound.
A program may use at most 128 MiB of HBM per device.

```python
import math
import jax
import jax.numpy as jnp
import numpy as np
from jax import lax

D = 2048
HEADS = 16
KV_HEADS = 4
HEAD = 128
GRID_W = 64
FFE = 512
TOPK = 2
REACH = 3
TOK_DEV = 512
TOKENS = 4096
EROWS = 128
EXPERTS = 32
CAP = 16
DOC_MOST = 1537
DOCS = 4
N_SP = 8
N_TP = 4


def drawn(key):
    base = jax.random.fold_in(key, 7)
    key_q, key_k, key_g = jax.random.split(base, 3)
    queries = jnp.clip(jax.random.normal(key_q, (TOKENS, HEADS * HEAD), jnp.float32), -6.0, 6.0)
    keys = jnp.clip(jax.random.normal(key_k, (TOKENS, KV_HEADS * HEAD), jnp.float32), -6.0, 6.0)
    gains = jnp.exp(jax.random.uniform(key_g, (2, HEAD), jnp.float32, -0.7, 0.7))
    return (queries, keys, gains)


def draw_query_proj(key, part):
    return drawn(key)[0].astype(jnp.bfloat16)


def draw_key_proj(key, part):
    return drawn(key)[1].astype(jnp.bfloat16)


def draw_query_gain(key, part):
    return drawn(key)[2][0]


def draw_key_gain(key, part):
    return drawn(key)[2][1]


def levels(key, shape, shards, low, high):
    gain = 1.0
    for dim, parts in shards:
        heights = jax.random.uniform(jax.random.fold_in(jax.random.fold_in(key, 6), dim), (parts,), jnp.float32, low / len(shards), high / len(shards))
        gain = gain * jnp.repeat(jnp.exp(heights), shape[dim] // parts).reshape((-1,) + (1,) * (len(shape) - 1 - dim))
    return gain


def length_profile(number_of, total, most, skew):
    weights = [(1 << 20) // math.isqrt(grade ** skew) + 1 for grade in range(2, number_of + 1)]
    spare, given = total - most - (number_of - 1), [1] * (number_of - 1)
    while spare > 0:
        movable = [i for i in range(number_of - 1) if given[i] < most]
        mass, budget = sum([weights[i] for i in movable]), spare
        for i in movable:
            extra = min(most - given[i], max(1, budget * weights[i] // mass), spare)
            given[i] = given[i] + extra
            spare = spare - extra
    return np.array([most] + given)


def uneven(own_key, number_of, total, bound, skew):
    if number_of == 2:
        one = jax.random.randint(own_key, (), max(1, total - bound), min(bound, total - 1) + 1)
        return jnp.stack([one, total - one])
    lengths = jnp.asarray(length_profile(number_of, total, bound, skew), jnp.int32)
    twos = (number_of - 1) // 2
    donor, receiver = lengths[1:1 + 2 * twos:2], lengths[2:2 + 2 * twos:2]
    slack = jnp.minimum(donor - 1, bound - receiver)
    shifted = jax.random.randint(jax.random.fold_in(own_key, 1), (twos,), 0, 1 << 20) % (slack + 1)
    lengths = lengths.at[1:1 + 2 * twos:2].set(donor - shifted).at[2:2 + 2 * twos:2].set(receiver + shifted)
    return lengths[jax.random.permutation(jax.random.fold_in(own_key, 2), number_of)]


def assign_block(stream_key, own, number, rows, number_of, top, reach, lean):
    order = jax.random.permutation(stream_key, number_of)
    packed, common = shares(number_of, rows * top, reach, lean, True), shares(number_of, rows * top, reach, lean, False)
    places = jnp.arange(number_of)

    def named(tallies, offset_by):
        used = int((tallies > 0).sum())
        fixed = max(1, used // 4)
        shifted = fixed + (places - fixed + offset_by * (used - fixed)) % max(1, number_of - fixed)
        return jnp.zeros((number_of,), jnp.int32).at[order[jnp.where(places < fixed, places, shifted)]].set(jnp.asarray(tallies, jnp.int32))

    tallies = jnp.where(number % 4 == 0, named(packed, number // 4), named(common, number - number // 4 - 1))
    mixed = jax.random.permutation(jax.random.fold_in(own, 3), number_of)
    source_of, taker = mixed[0:number_of // 2 * 2:2], mixed[1:number_of // 2 * 2:2]
    room = jnp.minimum(tallies[source_of] - 1, reach - tallies[taker]) // 2
    room = jnp.where((source_of == order[0]) | (taker == order[0]) | (tallies[taker] == 0), 0, jnp.maximum(room, 0))
    shifted = jax.random.randint(jax.random.fold_in(own, 4), (number_of // 2,), 0, 1 << 20) % (room + 1)
    tallies = tallies.at[source_of].add(-shifted).at[taker].add(shifted)
    members = jnp.searchsorted(jnp.cumsum(tallies), jnp.arange(rows * top), side="right").astype(jnp.int32)
    table = members.reshape(top, rows).T
    table = table[jax.random.permutation(jax.random.fold_in(own, 1), rows)]
    offset_by = jax.random.randint(jax.random.fold_in(own, 2), (rows, 1), 0, top)
    return jnp.take_along_axis(table, (jnp.arange(top)[None, :] + offset_by) % top, axis=1)


def shares(number_of, total, most, lean, full):
    portions = [(1 << 20) // math.isqrt(standing ** lean) + 1 for standing in range(1, number_of + 1)]
    largest = most if full else min(most, max(-(-total // number_of), total * portions[0] // sum(portions)))
    least = 1 if total - largest >= number_of - 1 else 0
    given, surplus = [largest] + [least] * (number_of - 1), total - largest - least * (number_of - 1)
    while surplus > 0:
        candidates = [i for i in range(1, number_of) if given[i] < largest] or [i for i in range(1, number_of) if given[i] < most]
        whole, remaining = sum([portions[i] for i in candidates]), surplus
        for i in candidates:
            extra = min(most - given[i], max(1, remaining * portions[i] // whole), surplus)
            given[i] = given[i] + extra
            surplus = surplus - extra
    return np.array(given)


def centred(own_key, extent, width, bound, pieces=(), kind=jnp.bfloat16):
    factor_of = levels(own_key, extent, pieces, -0.22, 0.18) if pieces else 1.0
    values = jax.random.normal(own_key, extent, jnp.float32) * width * factor_of
    return jnp.minimum(jnp.maximum(values, -bound), bound).astype(kind)


def setup_inputs(seed: int = 0) -> dict:
    arg_keys = jax.random.split(jax.random.key(seed), 15)
    residual = centred(arg_keys[0], (TOKENS, D), 1.0, 6.0, ((0, 32),))
    query_proj = draw_query_proj(jax.random.fold_in(arg_keys[14], 71), 0)
    key_proj = draw_key_proj(jax.random.fold_in(arg_keys[14], 71), 0)
    value_proj = centred(arg_keys[3], (TOKENS, KV_HEADS * HEAD), 1.0, 6.0, ((0, 8), (1, 4)))
    query_gain = draw_query_gain(jax.random.fold_in(arg_keys[14], 71), 0)
    key_gain = draw_key_gain(jax.random.fold_in(arg_keys[14], 71), 0)
    document_ids = jnp.searchsorted(jnp.cumsum(uneven(arg_keys[6], DOCS, TOKENS, DOC_MOST, 2)), jnp.arange(TOKENS), side="right").astype(jnp.int32)
    output_weight = centred(arg_keys[7], (HEADS * HEAD, D), (HEADS * HEAD) ** -0.5, 0.125)
    norm_gain = jnp.clip(1.0 + 0.18 * jax.random.normal(arg_keys[8], (D,), jnp.float32), 0.1, 1.9)
    expert_ids_keys = jax.random.split(jax.random.fold_in(arg_keys[9], 1), TOKENS // EROWS)
    expert_ids_turns = jax.random.permutation(jax.random.fold_in(arg_keys[9], 3), TOKENS // EROWS)
    expert_ids = jax.vmap(lambda own, number: assign_block(jax.random.fold_in(arg_keys[9], 2), own, number, EROWS, EXPERTS, TOPK, CAP, 2))(expert_ids_keys, expert_ids_turns).reshape((TOKENS, TOPK))
    route_weights = jnp.clip(0.2 + 0.8 * jax.random.uniform(arg_keys[10], (TOKENS, TOPK), jnp.float32) ** levels(arg_keys[10], (TOKENS, TOPK), ((0, 32),), -0.2, 0.2), 0.2, 1.0)
    gate_weight = centred(arg_keys[11], (EXPERTS, D, FFE), D ** -0.5, 0.125, ((0, 32),))
    up_weight = centred(arg_keys[12], (EXPERTS, D, FFE), D ** -0.5, 0.125, ((0, 32),))
    down_weight = centred(arg_keys[13], (EXPERTS, FFE, D), FFE ** -0.5, 0.25, ((0, 32),))
    return dict(residual=residual, query_proj=query_proj, key_proj=key_proj, value_proj=value_proj, query_gain=query_gain, key_gain=key_gain, document_ids=document_ids, output_weight=output_weight, norm_gain=norm_gain, expert_ids=expert_ids, route_weights=route_weights, gate_weight=gate_weight, up_weight=up_weight, down_weight=down_weight)


norm_eps = 1e-06
rope_base = 10000.0

def rotary_tables(first_row, length):
    freq_count = HEAD // 4
    inverse = 1.0 / rope_base ** (jnp.arange(freq_count, dtype=jnp.float32) / freq_count)
    position = first_row + jnp.arange(length, dtype=jnp.int32)
    grid_row = (position // GRID_W).astype(jnp.float32)
    grid_col = (position % GRID_W).astype(jnp.float32)
    angles = jnp.concatenate([grid_row[:, None] * inverse[None, :], grid_col[:, None] * inverse[None, :]], axis=1)
    return (jnp.cos(angles), jnp.sin(angles))

def norm_rotate(projected, gains, cosine, sine_table):
    length = projected.shape[0]
    values_wide = projected.astype(jnp.float32).reshape(length, -1, HEAD)
    scaled = values_wide * lax.rsqrt(lax.optimization_barrier(jnp.mean(values_wide * values_wide, axis=-1, keepdims=True)) + norm_eps) * gains
    half_size = HEAD // 2
    first_half = scaled[..., :half_size]
    second_half = scaled[..., half_size:]
    cosine_rows = cosine[:, None, :]
    sine_rows = sine_table[:, None, :]
    turned = jnp.concatenate([first_half * cosine_rows - second_half * sine_rows, first_half * sine_rows + second_half * cosine_rows], axis=-1)
    return turned.reshape(length, -1).astype(jnp.bfloat16)

def attend(query_block, key_block, value_block, query_doc, key_doc, groups):
    query_rows = query_block.shape[0]
    key_rows = key_block.shape[0]
    key_heads = key_block.shape[1] // HEAD
    query_grid = query_block.astype(jnp.float32).reshape(query_rows, key_heads, groups, HEAD)
    key_grid = key_block.astype(jnp.float32).reshape(key_rows, key_heads, HEAD)
    value_grid = value_block.astype(jnp.float32).reshape(key_rows, key_heads, HEAD)
    scores = jnp.einsum('qhgd,khd->hgqk', query_grid, key_grid) * HEAD ** (-0.5)
    same_doc = query_doc[:, None] == key_doc[None, :]
    scores = jnp.where(same_doc[None, None], scores, -jnp.inf)
    row_max = lax.optimization_barrier(jnp.max(scores, axis=-1, keepdims=True))
    weights = jnp.exp(scores - row_max)
    denominator = lax.optimization_barrier(jnp.sum(weights, axis=-1))
    rounded = weights.astype(jnp.bfloat16).astype(jnp.float32)
    weighted = jnp.einsum('hgqk,khd->hgqd', rounded, value_grid) / denominator[..., None]
    return jnp.transpose(weighted, (2, 0, 1, 3)).reshape(query_rows, key_heads * groups * HEAD).astype(jnp.bfloat16)

def reference(residual, query_proj, key_proj, value_proj, query_gain, key_gain, document_ids, output_weight, norm_gain, expert_ids, route_weights, gate_weight, up_weight, down_weight):
    tokens = query_proj.shape[0]
    cosine, sine_table = rotary_tables(jnp.int32(0), tokens)
    query_norm = norm_rotate(query_proj, query_gain, cosine, sine_table)
    key_norm = norm_rotate(key_proj, key_gain, cosine, sine_table)
    groups = HEADS // KV_HEADS
    window = min(tokens, TOK_DEV + 2 * REACH * TOK_DEV)

    def one_block(block_index):
        first_row = block_index * TOK_DEV
        key_first = jnp.clip(first_row - REACH * TOK_DEV, 0, tokens - window).astype(jnp.int32)
        query_block = lax.dynamic_slice_in_dim(query_norm, first_row, TOK_DEV, 0)
        query_doc = lax.dynamic_slice_in_dim(document_ids, first_row, TOK_DEV, 0)
        key_block = lax.dynamic_slice_in_dim(key_norm, key_first, window, 0)
        value_block = lax.dynamic_slice_in_dim(value_proj, key_first, window, 0)
        key_doc = lax.dynamic_slice_in_dim(document_ids, key_first, window, 0)
        return attend(query_block, key_block, value_block, query_doc, key_doc, groups)
    attn = lax.map(one_block, jnp.arange(tokens // TOK_DEV, dtype=jnp.int32)).reshape(tokens, HEADS * HEAD)
    hidden = (residual.astype(jnp.float32) + jnp.dot(attn, output_weight, preferred_element_type=jnp.float32)).astype(jnp.bfloat16)
    hidden_wide = hidden.astype(jnp.float32)
    normed = (hidden_wide * lax.rsqrt(lax.optimization_barrier(jnp.mean(hidden_wide * hidden_wide, axis=-1, keepdims=True)) + norm_eps) * norm_gain).astype(jnp.bfloat16)
    flat_ids = expert_ids.reshape(-1)
    flat_weights = route_weights.reshape(-1)
    top_count = expert_ids.shape[1]
    limit = N_SP * N_TP * CAP
    slot_numbers = jnp.arange(limit, dtype=jnp.int32)

    def add_expert(expert_index, running):
        matches = flat_ids == expert_index
        count = jnp.sum(matches.astype(jnp.int32))
        picked = jnp.nonzero(matches, size=limit, fill_value=0)[0].astype(jnp.int32)
        valid = (slot_numbers < count).astype(jnp.float32)
        token_index = picked // top_count
        chosen = normed[token_index]
        gate_part = jnp.dot(chosen, gate_weight[expert_index], preferred_element_type=jnp.float32)
        up_part = jnp.dot(chosen, up_weight[expert_index], preferred_element_type=jnp.float32)
        activity = (jax.nn.silu(gate_part) * up_part).astype(jnp.bfloat16)
        expert_out = jnp.dot(activity, down_weight[expert_index], preferred_element_type=jnp.float32).astype(jnp.bfloat16)
        factor = (flat_weights[picked] * valid)[:, None]
        return running.at[token_index].add(factor * expert_out.astype(jnp.float32))
    combined = lax.fori_loop(0, EXPERTS, add_expert, jnp.zeros((tokens, D), jnp.float32))
    return (hidden_wide + combined).astype(jnp.bfloat16)
```

```python
import functools
import math

import jax
import jax.numpy as jnp
from jax import lax
from jax.experimental import pallas as pl
from jax.experimental.pallas import tpu as pltpu
from jax.sharding import PartitionSpec as P

HEAD = 128
GRID_W = 64
REACH = 3


norm_eps = 1e-06
rope_base = 10000.0
masked_low = -1e30
MESH = pl.DeviceIdType.MESH
DOC_KEY = 128.0
DOC_QUERY = 64.0
PIECES = 2
EXP2_SCALE = math.log2(math.e) / math.sqrt(HEAD)


def rotary_tables(first_row, length):
    freq_count = HEAD // 4
    inverse = 1.0 / rope_base ** (jnp.arange(freq_count, dtype=jnp.float32) / freq_count)
    position = first_row + jnp.arange(length, dtype=jnp.int32)
    grid_row = (position // GRID_W).astype(jnp.float32)
    grid_col = (position % GRID_W).astype(jnp.float32)
    angles = jnp.concatenate(
        [grid_row[:, None] * inverse[None, :], grid_col[:, None] * inverse[None, :]], axis=1
    )
    return (jnp.cos(angles), jnp.sin(angles))


def norm_rotate(projected, gains, cosine, sine_table):
    length = projected.shape[0]
    values_wide = projected.astype(jnp.float32).reshape(length, -1, HEAD)
    scaled = (
        values_wide
        * lax.rsqrt(jnp.mean(values_wide * values_wide, axis=-1, keepdims=True) + norm_eps)
        * gains
    )
    half_size = HEAD // 2
    first_half = scaled[..., :half_size]
    second_half = scaled[..., half_size:]
    cosine_rows = cosine[:, None, :]
    sine_rows = sine_table[:, None, :]
    turned = jnp.concatenate(
        [
            first_half * cosine_rows - second_half * sine_rows,
            first_half * sine_rows + second_half * cosine_rows,
        ],
        axis=-1,
    )
    return turned.reshape(length, -1).astype(jnp.bfloat16)


def attention_kernel(
    n_sp, n_tp, q_ref, k_ref, vt_ref, doc_ref, res_ref, gain_ref, wo_hbm,
    hid_ref, nrm_ref,
    wo_v, k_in, vt_in, doc_in, k_aug, m_s, l_s, acc_s, att_s, all_s,
    send, recv, t_send, t_recv, w_sem,
):
    sp = lax.axis_index("sp")
    tp = lax.axis_index("tp")
    heads = q_ref.shape[0]
    rows = res_ref.shape[0]
    width = att_s.shape[1]
    slots = 2 * REACH

    def distance(j):
        return (j // 2 + 1) * (1 - 2 * (j % 2))

    def inside(index):
        return jnp.logical_and(index >= 0, index < n_sp)

    wo_copy = pltpu.make_async_copy(wo_hbm, wo_v, w_sem)
    wo_copy.start()

    barrier = pltpu.get_barrier_semaphore()
    for j in range(slots):
        there = sp + distance(j)

        @pl.when(inside(there))
        def _():
            pl.semaphore_signal(barrier, inc=1, device_id=(there, tp), device_id_type=MESH)

    for k in range(1, n_tp):
        pl.semaphore_signal(
            barrier, inc=1, device_id=(sp, lax.rem(tp + k, n_tp)), device_id_type=MESH
        )
    beside = jnp.minimum(sp, REACH) + jnp.minimum(n_sp - 1 - sp, REACH)
    pl.semaphore_wait(barrier, n_tp - 1 + beside)

    def copies(j):
        there = (sp + distance(j), tp)
        return [
            pltpu.make_async_remote_copy(
                src_ref=one,
                dst_ref=into.at[j],
                send_sem=send.at[j, i],
                recv_sem=recv.at[j, i],
                device_id=there,
                device_id_type=MESH,
            )
            for i, (one, into) in enumerate(((k_ref, k_in), (vt_ref, vt_in), (doc_ref, doc_in)))
        ]

    for j in range(slots):

        @pl.when(inside(sp + distance(j)))
        def _():
            for copy in copies(j):
                copy.start()

    def take(keys, values_t, docs, first):
        length = keys.shape[0]
        doc_col = jnp.broadcast_to(docs[0:1, :], (HEAD, length)).T
        lanes = lax.broadcasted_iota(jnp.int32, (length, HEAD), 1).astype(jnp.float32)
        k_aug[:, :HEAD] = keys[...]
        k_aug[:, HEAD:] = jnp.where(doc_col == lanes, DOC_KEY, 0.0).astype(jnp.bfloat16)
        for h in range(heads):
            s = jnp.dot(k_aug[...], q_ref[h], preferred_element_type=jnp.float32)
            top = jnp.max(s, axis=0, keepdims=True)
            if not first:
                top = jnp.maximum(m_s[h], top)
            e = jnp.exp2((s - top) * EXP2_SCALE)
            den = jnp.sum(e, axis=0, keepdims=True)
            part = jnp.dot(
                values_t[...], e.astype(jnp.bfloat16), preferred_element_type=jnp.float32
            )
            if first:
                l_s[h] = den
                acc_s[h] = part
            else:
                old = jnp.exp2((m_s[h] - top) * EXP2_SCALE)
                l_s[h] = l_s[h] * old + den
                acc_s[h] = acc_s[h] * old + part
            m_s[h] = top

    take(k_ref, vt_ref, doc_ref, True)

    def step(j, carry):
        @pl.when(inside(sp - distance(j)))
        def _():
            for copy in copies(j):
                copy.wait_recv()
            take(k_in.at[j], vt_in.at[j], doc_in.at[j], False)

        return carry

    lax.fori_loop(0, slots, step, 0)

    for h in range(heads):
        out = acc_s[h] / l_s[h]
        att_s[:, h * HEAD : (h + 1) * HEAD] = out.T.astype(jnp.bfloat16)

    def exchange(k):
        there = lax.rem(tp + k, n_tp)
        return pltpu.make_async_remote_copy(
            src_ref=att_s.at[pl.ds(pl.multiple_of(there * rows, rows), rows), :],
            dst_ref=all_s.at[tp],
            send_sem=t_send.at[k],
            recv_sem=t_recv.at[k],
            device_id=(sp, there),
            device_id_type=MESH,
        )

    for k in range(n_tp - 1, 0, -1):
        exchange(k).start()
    wo_copy.wait()

    def weight_rows(i):
        return wo_v[pl.ds(pl.multiple_of(i * width, width), width), :]

    projected = jnp.dot(
        att_s[pl.ds(pl.multiple_of(tp * rows, rows), rows), :],
        weight_rows(tp),
        preferred_element_type=jnp.float32,
    )
    for k in range(1, n_tp):
        exchange(k).wait_recv()
        source = lax.rem(tp - k + n_tp, n_tp)
        projected += jnp.dot(
            all_s[source], weight_rows(source), preferred_element_type=jnp.float32
        )
    hidden = (res_ref[...].astype(jnp.float32) + projected).astype(jnp.bfloat16)
    hid_ref[...] = hidden
    wide = hidden.astype(jnp.float32)
    mean = jnp.mean(wide * wide, axis=-1, keepdims=True)
    nrm_ref[...] = (wide * lax.rsqrt(mean + norm_eps) * gain_ref[...]).astype(jnp.bfloat16)

    for j in range(slots):

        @pl.when(inside(sp + distance(j)))
        def _():
            for copy in copies(j):
                copy.wait_send()

    for k in range(1, n_tp):
        exchange(k).wait_send()


def attend(q_aug, key_norm, value_t, doc_rows, residual, norm_gain, output_weight):
    n_sp, n_tp = lax.axis_size("sp"), lax.axis_size("tp")
    heads, deep, length = q_aug.shape
    rows, model = residual.shape
    vmem = pl.BlockSpec(memory_space=pltpu.VMEM)
    slots = 2 * REACH
    return pl.pallas_call(
        functools.partial(attention_kernel, n_sp, n_tp),
        out_shape=[jax.ShapeDtypeStruct((rows, model), jnp.bfloat16)] * 2,
        in_specs=[vmem] * 6 + [pl.BlockSpec(memory_space=pl.ANY)],
        out_specs=[vmem] * 2,
        scratch_shapes=[
            pltpu.VMEM(output_weight.shape, jnp.bfloat16),
            pltpu.VMEM((slots,) + key_norm.shape, jnp.bfloat16),
            pltpu.VMEM((slots,) + value_t.shape, jnp.bfloat16),
            pltpu.VMEM((slots,) + doc_rows.shape, jnp.float32),
            pltpu.VMEM((length, deep), jnp.bfloat16),
            pltpu.VMEM((heads, 1, length), jnp.float32),
            pltpu.VMEM((heads, 1, length), jnp.float32),
            pltpu.VMEM((heads, HEAD, length), jnp.float32),
            pltpu.VMEM((length, heads * HEAD), jnp.bfloat16),
            pltpu.VMEM((n_tp, rows, heads * HEAD), jnp.bfloat16),
            pltpu.SemaphoreType.DMA((slots, 3)),
            pltpu.SemaphoreType.DMA((slots, 3)),
            pltpu.SemaphoreType.DMA((n_tp,)),
            pltpu.SemaphoreType.DMA((n_tp,)),
            pltpu.SemaphoreType.DMA(()),
        ],
        compiler_params=pltpu.CompilerParams(
            collective_id=1, has_side_effects=True, vmem_limit_bytes=48 * 1024 * 1024
        ),
    )(q_aug, key_norm, value_t, doc_rows, residual, norm_gain.reshape(1, -1), output_weight)


def expert_kernel(
    n_sp, n_tp, capacity, top_count,
    nrm_ref, meta_ref, hid_ref, gate_hbm, up_hbm, down_hbm,
    new_ref,
    gate_v, up_v, down_v, metas, blocks, picked, arrived, answer, returned, spread,
    m_send, m_recv, z_send, z_recv, d_send, d_recv, r_send, r_recv, w_sem,
):
    devices = n_sp * n_tp
    rows = hid_ref.shape[0]
    members = rows // capacity
    groups = devices // members
    piece = rows // PIECES
    me = lax.axis_index("sp") * n_tp + lax.axis_index("tp")
    plane = lax.div(me, members)
    pos = lax.rem(me, members)

    loads = [
        pltpu.make_async_copy(source.at[0], into, w_sem.at[i])
        for i, (source, into) in enumerate(
            ((gate_hbm, gate_v), (up_hbm, up_v), (down_hbm, down_v))
        )
    ]
    for load in loads:
        load.start()

    def place(device):
        return (lax.div(device, n_tp), lax.rem(device, n_tp))

    def slots(index):
        return pl.ds(pl.multiple_of(index * capacity, capacity), capacity)

    def inside(block):
        return jnp.logical_and(block >= 0, block < groups)

    barrier = pltpu.get_barrier_semaphore()

    def greet(i, carry):
        there = lax.rem(me + i, devices)
        pl.semaphore_signal(barrier, inc=1, device_id=place(there), device_id_type=MESH)
        return carry

    lax.fori_loop(1, devices, greet, 0)
    pl.semaphore_wait(barrier, devices - 1)

    def tell(i, block):
        return pltpu.make_async_remote_copy(
            src_ref=meta_ref,
            dst_ref=metas.at[block],
            send_sem=m_send.at[i],
            recv_sem=m_recv.at[block],
            device_id=place(lax.rem(plane + i, groups) * members + pos),
            device_id_type=MESH,
        )

    def pass_on(source, block, way, c):
        part = pl.ds(c * piece, piece)
        return pltpu.make_async_remote_copy(
            src_ref=source.at[part],
            dst_ref=blocks.at[block, part],
            send_sem=z_send.at[way, block, c],
            recv_sem=z_recv.at[block, c],
            device_id=place(me + (2 * way - 1) * members),
            device_id_type=MESH,
        )

    def dispatch(block, peer, landing):
        return pltpu.make_async_remote_copy(
            src_ref=picked.at[block, slots(peer)],
            dst_ref=arrived.at[block, slots(landing)],
            send_sem=d_send.at[block, peer],
            recv_sem=d_recv.at[block, landing],
            device_id=place(plane * members + peer),
            device_id_type=MESH,
        )

    def give_back(block, member, landing):
        return pltpu.make_async_remote_copy(
            src_ref=answer.at[block, slots(member)],
            dst_ref=returned.at[slots(landing)],
            send_sem=r_send.at[block, member],
            recv_sem=r_recv.at[landing],
            device_id=place(block * members + member),
            device_id_type=MESH,
        )

    def others(act, first=1):
        def one(i, carry):
            act(lax.rem(pos + i, members))
            return carry

        lax.fori_loop(first, members, one, 0)

    for i in range(1, groups):
        tell(i, plane).start()
    for way in range(2):

        @pl.when(inside(plane + 2 * way - 1))
        def _():
            for c in range(PIECES):
                pass_on(nrm_ref, plane, way, c).start()

    def slot_rows(meta):
        experts = lax.broadcasted_iota(jnp.int32, (devices, rows), 0).astype(jnp.float32)
        hits = [experts == meta[k : k + 1, :] for k in range(top_count)]
        named = sum(hit.astype(jnp.float32) for hit in hits)
        ahead = (
            lax.broadcasted_iota(jnp.int32, (rows, rows), 0)
            < lax.broadcasted_iota(jnp.int32, (rows, rows), 1)
        )
        before = jnp.dot(
            named.astype(jnp.bfloat16),
            ahead.astype(jnp.float32).astype(jnp.bfloat16),
            preferred_element_type=jnp.float32,
        )
        return [
            meta[k : k + 1, :] * capacity
            + jnp.sum(jnp.where(hits[k], before, 0.0), axis=0, keepdims=True)
            for k in range(top_count)
        ]

    def slot_numbers(group):
        return (
            lax.broadcasted_iota(jnp.int32, (rows, rows), 0) + group * rows
        ).astype(jnp.float32)

    def gather(source, meta, block):
        numbers = slot_numbers(plane)
        choice = sum((numbers == row).astype(jnp.float32) for row in slot_rows(meta))
        picked[block] = jnp.dot(
            choice.astype(jnp.bfloat16), source[...], preferred_element_type=jnp.float32
        ).astype(jnp.bfloat16)
        others(lambda peer: dispatch(block, peer, pos).start())
        arrived[block, slots(pos), :] = picked[block, slots(pos), :]

    def expert(block):
        others(lambda peer: dispatch(block, peer, peer).wait_recv())
        x = arrived[block]
        gate_part = jnp.dot(x, gate_v[...], preferred_element_type=jnp.float32)
        up_part = jnp.dot(x, up_v[...], preferred_element_type=jnp.float32)
        activity = (jax.nn.silu(gate_part) * up_part).astype(jnp.bfloat16)
        answer[block] = jnp.dot(
            activity, down_v[...], preferred_element_type=jnp.float32
        ).astype(jnp.bfloat16)

    def both_ways(distance, act):
        def one(way, carry):
            block = plane - (2 * way - 1) * distance

            @pl.when(inside(block))
            def _():
                act(block, way)

            return carry

        lax.fori_loop(0, 2, one, 0)

    gather(nrm_ref, meta_ref[...], plane)
    own_slots = slot_rows(meta_ref[...])
    for g in range(groups):
        numbers = slot_numbers(g)
        weights = sum(
            jnp.where(numbers == own_slots[k], meta_ref[top_count + k : top_count + k + 1, :], 0.0)
            for k in range(top_count)
        ).T
        high = weights.astype(jnp.bfloat16)
        spread[g, 0] = high
        spread[g, 1] = (weights - high.astype(jnp.float32)).astype(jnp.bfloat16)
    for load in loads:
        load.wait()

    def receive(block, way, c):
        pass_on(nrm_ref, block, way, c).wait_recv()

        @pl.when(inside(plane + 2 * way - 1))
        def _():
            pass_on(blocks.at[block], block, way, c).start()

    def collect(block, way):
        tell(1, block).wait_recv()
        gather(blocks.at[block], metas[block], block)

    def serve(block, way):
        expert(block)
        others(lambda member: give_back(block, member, me).start(), 0)

    for distance in range(1, groups):
        for c in range(PIECES):
            if c == PIECES - 1:
                if distance == 1:
                    expert(plane)
                    others(lambda member: give_back(plane, member, me).start())
                    returned[slots(me), :] = answer[plane, slots(pos), :]
                else:
                    both_ways(distance - 1, serve)
            both_ways(distance, functools.partial(receive, c=c))
        both_ways(distance, collect)
    both_ways(groups - 1, serve)

    total = hid_ref[...].astype(jnp.float32)

    def combine(group):
        back = returned[pl.ds(pl.multiple_of(group * rows, rows), rows), :]
        part = jnp.dot(spread[group, 0], back, preferred_element_type=jnp.float32)
        return part + jnp.dot(spread[group, 1], back, preferred_element_type=jnp.float32)

    for i in range(groups):
        group = lax.rem(plane + i, groups)
        home = group * members
        others(
            lambda member: give_back(plane, member, home + member).wait_recv(), 1 if i == 0 else 0
        )
        total += combine(group)
    new_ref[...] = total.astype(jnp.bfloat16)

    for i in range(1, groups):
        tell(i, plane).wait_send()
    for way in range(2):

        @pl.when(inside(plane + 2 * way - 1))
        def _():
            for c in range(PIECES):
                pass_on(nrm_ref, plane, way, c).wait_send()

    def sent(block, way):
        @pl.when(inside(plane + 2 * way - 1))
        def _():
            for c in range(PIECES):
                pass_on(nrm_ref, block, way, c).wait_send()

        others(lambda peer: dispatch(block, peer, pos).wait_send())
        others(lambda member: give_back(block, member, me).wait_send(), 0)

    others(lambda peer: dispatch(plane, peer, pos).wait_send())
    others(lambda member: give_back(plane, member, me).wait_send())
    for distance in range(1, groups):
        both_ways(distance, sent)


def run_experts(normed, meta, hidden, gate_weight, up_weight, down_weight, capacity, top_count):
    n_sp, n_tp = lax.axis_size("sp"), lax.axis_size("tp")
    rows, model = hidden.shape
    members = rows // capacity
    groups = n_sp * n_tp // members
    vmem = pl.BlockSpec(memory_space=pltpu.VMEM)
    anywhere = pl.BlockSpec(memory_space=pl.ANY)
    buffer = pltpu.VMEM((groups, rows, model), jnp.bfloat16)
    return pl.pallas_call(
        functools.partial(expert_kernel, n_sp, n_tp, capacity, top_count),
        out_shape=jax.ShapeDtypeStruct(hidden.shape, jnp.bfloat16),
        in_specs=[vmem] * 3 + [anywhere] * 3,
        out_specs=vmem,
        scratch_shapes=[
            pltpu.VMEM(gate_weight.shape[1:], jnp.bfloat16),
            pltpu.VMEM(up_weight.shape[1:], jnp.bfloat16),
            pltpu.VMEM(down_weight.shape[1:], jnp.bfloat16),
            pltpu.VMEM((groups,) + meta.shape, jnp.float32),
            buffer,
            buffer,
            buffer,
            buffer,
            pltpu.VMEM((groups * rows, model), jnp.bfloat16),
            pltpu.VMEM((groups, 2, rows, rows), jnp.bfloat16),
            pltpu.SemaphoreType.DMA((groups,)),
            pltpu.SemaphoreType.DMA((groups,)),
            pltpu.SemaphoreType.DMA((2, groups, PIECES)),
            pltpu.SemaphoreType.DMA((groups, PIECES)),
            pltpu.SemaphoreType.DMA((groups, members)),
            pltpu.SemaphoreType.DMA((groups, members)),
            pltpu.SemaphoreType.DMA((groups, members)),
            pltpu.SemaphoreType.DMA((n_sp * n_tp,)),
            pltpu.SemaphoreType.DMA((3,)),
        ],
        compiler_params=pltpu.CompilerParams(
            collective_id=2, has_side_effects=True, vmem_limit_bytes=40 * 1024 * 1024
        ),
    )(normed, meta, hidden, gate_weight, up_weight, down_weight)


def on_device(
    residual,
    query_proj,
    key_proj,
    value_proj,
    query_gain,
    key_gain,
    document_ids,
    output_weight,
    norm_gain,
    expert_ids,
    route_weights,
    gate_weight,
    up_weight,
    down_weight,
):
    rows_here = query_proj.shape[0]
    cosine, sine_table = rotary_tables(lax.axis_index("sp") * rows_here, rows_here)
    query_norm = norm_rotate(query_proj, query_gain, cosine, sine_table)
    key_norm = norm_rotate(key_proj, key_gain, cosine, sine_table)
    heads = query_proj.shape[1] // HEAD
    docs = document_ids.astype(jnp.float32)
    query_t = jnp.transpose(query_norm.reshape(rows_here, heads, HEAD), (1, 2, 0))
    query_doc = jnp.where(
        docs[None, :] == jnp.arange(HEAD, dtype=jnp.float32)[:, None], DOC_QUERY, 0.0
    ).astype(jnp.bfloat16)
    q_aug = jnp.concatenate(
        [query_t, jnp.broadcast_to(query_doc[None], (heads, HEAD, rows_here))], axis=1
    )
    doc_rows = jnp.broadcast_to(docs[None, :], (8, rows_here))
    hidden, normed = attend(
        q_aug, key_norm, value_proj.T, doc_rows, residual, norm_gain, output_weight
    )
    token_rows = residual.shape[0]
    top_count = expert_ids.shape[1]
    experts_all = lax.axis_size("sp") * lax.axis_size("tp")
    capacity = max(2, 2 * token_rows * top_count // experts_all)
    if (
        capacity % 16 == 0
        and token_rows % HEAD == 0
        and token_rows % capacity == 0
        and experts_all % (token_rows // capacity) == 0
    ):
        meta = jnp.concatenate([expert_ids.astype(jnp.float32), route_weights], axis=1).T
        meta = jnp.pad(meta, ((0, 8 - 2 * top_count), (0, 0)))
        return run_experts(
            normed, meta, hidden, gate_weight, up_weight, down_weight, capacity, top_count
        )
    flat_ids = expert_ids.reshape(-1)
    order = jnp.arange(flat_ids.shape[0], dtype=jnp.int32)
    earlier = jnp.logical_and(
        flat_ids[:, None] == flat_ids[None, :], order[None, :] < order[:, None]
    )
    arrival = jnp.sum(earlier.astype(jnp.int32), axis=1)
    slot_index = flat_ids * capacity + arrival
    slot_grid = slot_index.reshape(token_rows, top_count)
    placing = jnp.sum(
        (
            jnp.arange(experts_all * capacity, dtype=jnp.int32)[:, None, None] == slot_grid[None]
        ).astype(jnp.float32),
        axis=2,
    ).astype(jnp.bfloat16)
    outgoing = jnp.dot(placing, normed, preferred_element_type=jnp.float32).astype(jnp.bfloat16)
    spread = jnp.sum(
        jnp.where(
            jnp.arange(experts_all * capacity, dtype=jnp.int32)[None, None, :]
            == slot_grid[:, :, None],
            route_weights[:, :, None],
            0.0,
        ),
        axis=1,
    )
    high = spread.astype(jnp.bfloat16)
    low = (spread - high.astype(jnp.float32)).astype(jnp.bfloat16)
    outgoing = outgoing.reshape(experts_all, capacity, normed.shape[1])
    arrived = lax.all_to_all(outgoing, ("sp", "tp"), split_axis=0, concat_axis=0, tiled=True)
    sources, slots, width = arrived.shape
    flat_rows = arrived.reshape(sources * slots, width)
    gate_part = jnp.dot(flat_rows, gate_weight[0], preferred_element_type=jnp.float32)
    up_part = jnp.dot(flat_rows, up_weight[0], preferred_element_type=jnp.float32)
    activity = (jax.nn.silu(gate_part) * up_part).astype(jnp.bfloat16)
    expert_out = jnp.dot(activity, down_weight[0], preferred_element_type=jnp.float32).astype(
        jnp.bfloat16
    )
    returned = lax.all_to_all(
        expert_out.reshape(sources, slots, width),
        ("sp", "tp"),
        split_axis=0,
        concat_axis=0,
        tiled=True,
    )
    rows_back = returned.reshape(experts_all * capacity, -1)
    combined = jnp.dot(high, rows_back, preferred_element_type=jnp.float32) + jnp.dot(
        low, rows_back, preferred_element_type=jnp.float32
    )
    return (hidden.astype(jnp.float32) + combined).astype(jnp.bfloat16)


def solution(mesh):
    in_specs = (
        P(("sp", "tp"), None),
        P("sp", "tp"),
        P("sp", "tp"),
        P("sp", "tp"),
        P(),
        P(),
        P("sp"),
        P(),
        P(),
        P(("sp", "tp"), None),
        P(("sp", "tp"), None),
        P(("sp", "tp"), None, None),
        P(("sp", "tp"), None, None),
        P(("sp", "tp"), None, None),
    )
    out_specs = P(("sp", "tp"), None)
    return jax.shard_map(
        on_device, mesh=mesh, in_specs=in_specs, out_specs=out_specs, check_vma=False
    )
```

```python
import functools
import math

import jax
import jax.numpy as jnp
from jax import lax
from jax.experimental import pallas as pl
from jax.experimental.pallas import tpu as pltpu
from jax.sharding import PartitionSpec as P

HEAD = 128
GRID_W = 64
REACH = 3


norm_eps = 1e-06
rope_base = 10000.0
masked_low = -1e30
MESH = pl.DeviceIdType.MESH
DOC_KEY = 128.0
DOC_QUERY = 64.0
PIECES = 2
OFFSETS = (1, -2, 2, -1, 3, -3)
EXP2_SCALE = math.log2(math.e) / math.sqrt(HEAD)


def layer_kernel(
    n_sp, n_tp, capacity, top_count,
    q_ref, k_ref, v_ref, doc_ref, qg_ref, kg_ref, ids_ref, rw_ref, res_ref, gain_ref,
    wo_hbm, gate_hbm, up_hbm, down_hbm,
    new_ref,
    wo_v, gate_v, up_v, down_v, cos_s, sin_s, meta_s, q_aug, k_own, k_in, v_in, doc_in,
    k_aug, vt_s, m_s, l_s, acc_s, att_s, all_s, hid_s, nrm_s,
    metas, blocks, picked, arrived, answer, homing, returned, spread, total_s,
    back, joined, midway, summed,
    k_send, k_recv, v_send, v_recv, c_send, c_recv, t_send, t_recv,
    m_send, m_recv, z_send, z_recv, d_send, d_recv, h_send, h_recv, r_send, r_recv,
    b_send, b_recv, j_send, y_recv, s_recv, w_sem,
):
    devices = n_sp * n_tp
    rows = res_ref.shape[0]
    members = rows // capacity
    groups = devices // members
    piece = rows // PIECES
    sp = lax.axis_index("sp")
    tp = lax.axis_index("tp")
    me = sp * n_tp + tp
    plane = lax.div(me, members)
    pos = lax.rem(me, members)

    loads = [
        pltpu.make_async_copy(source.at[0], into, w_sem.at[i])
        for i, (source, into) in enumerate(
            ((gate_hbm, gate_v), (up_hbm, up_v), (down_hbm, down_v))
        )
    ]

    def place(device):
        return (lax.div(device, n_tp), lax.rem(device, n_tp))

    def region(index):
        return pl.ds(pl.multiple_of(index * capacity, capacity), capacity)

    def level(block):
        return jnp.logical_and(block >= 0, block < groups)

    length = k_ref.shape[0]
    heads = q_ref.shape[1] // HEAD
    width = att_s.shape[1]
    slots = len(OFFSETS)
    half = HEAD // 2
    side = 1 - 2 * lax.rem(sp, 2)
    across, ahead, behind = sp + side, sp + 2 * side, sp - 2 * side

    def inside(index):
        return jnp.logical_and(index >= 0, index < n_sp)

    has_ahead, has_behind = inside(ahead), inside(behind)
    has_spare = inside(sp + 4 * side)

    def offset(j):
        return sum(jnp.where(j == i, o, 0) for i, o in enumerate(OFFSETS))

    def exists(j):
        return inside(sp + side * offset(j))

    def reader(j):
        odd = OFFSETS[j] % 2 == 1
        return sp + side * OFFSETS[j] if odd else sp - side * OFFSETS[j]

    wo_copy = pltpu.make_async_copy(wo_hbm, wo_v, w_sem.at[3])
    wo_copy.start()
    for load in loads:
        load.start()

    barrier = pltpu.get_barrier_semaphore()

    def greet(i, carry):
        there = lax.rem(me + i, devices)
        pl.semaphore_signal(barrier, inc=1, device_id=place(there), device_id_type=MESH)
        return carry

    lax.fori_loop(1, devices, greet, 0)

    def column(row):
        return jnp.broadcast_to(row, (HEAD, HEAD)).T[:, :1]

    freq_count = HEAD // 4
    exponent = lax.broadcasted_iota(jnp.int32, (freq_count, 1), 0).astype(jnp.float32) / freq_count
    inverse = jnp.exp2(exponent * -math.log2(rope_base))
    position = sp * length + lax.broadcasted_iota(jnp.int32, (1, length), 1)
    grid_row = lax.div(position, GRID_W).astype(jnp.float32)
    grid_col = lax.rem(position, GRID_W).astype(jnp.float32)
    angles = jnp.concatenate([inverse * grid_row, inverse * grid_col], axis=0)
    cos_s[...] = jnp.cos(angles)
    sin_s[...] = jnp.sin(angles)

    def turned(projected, gains):
        wide = projected.astype(jnp.float32).T
        scaled = (
            wide * lax.rsqrt(jnp.mean(wide * wide, axis=0, keepdims=True) + norm_eps) * gains
        )
        upper, lower = scaled[:half], scaled[half:]
        cosine, sine = cos_s[...], sin_s[...]
        return jnp.concatenate(
            [upper * cosine - lower * sine, upper * sine + lower * cosine], axis=0
        )

    k_own[...] = turned(k_ref[...], column(kg_ref[...])).T.astype(jnp.bfloat16)
    for k in range(top_count):
        for r, table in ((k, ids_ref), (top_count + k, rw_ref)):
            meta_s[r : r + 1, :] = table[k : k + 1, :].astype(jnp.float32)
    pl.semaphore_wait(barrier, devices - 1)

    def shift(source, into, sends, receives, i, there):
        return pltpu.make_async_remote_copy(
            src_ref=source,
            dst_ref=into.at[i],
            send_sem=sends.at[i],
            recv_sem=receives.at[i],
            device_id=(there, tp),
            device_id_type=MESH,
        )

    key_plan = (
        (k_own, across, True),
        (k_own, ahead, has_ahead),
        (k_own, behind, has_behind),
        (k_in.at[0], ahead, has_ahead),
        (k_in.at[0], behind, has_behind),
        (k_in.at[3], ahead, jnp.logical_and(has_ahead, has_behind)),
    )
    value_plan = (
        (v_ref, across, True),
        (v_ref, ahead, has_ahead),
        (v_ref, behind, has_behind),
        (v_in.at[2], across, has_ahead),
        (v_in.at[1], across, has_behind),
        (v_in.at[6], across, has_spare),
        (v_in.at[2], behind, jnp.logical_and(has_ahead, has_behind)),
    )

    def key_shift(i):
        return shift(key_plan[i][0], k_in, k_send, k_recv, i, key_plan[i][1])

    def value_shift(i):
        return shift(value_plan[i][0], v_in, v_send, v_recv, i, value_plan[i][1])

    def on(allowed, act):
        if allowed is True:
            act()
        elif allowed is not False:
            pl.when(allowed)(act)

    def start_keys(*which):
        for i in which:
            on(key_plan[i][2], lambda: key_shift(i).start())

    def start_values(*which):
        for i in which:
            on(value_plan[i][2], lambda: value_shift(i).start())

    def key_wait(j):
        shift(k_own, k_in, k_send, k_recv, j, sp).wait_recv()

    def value_wait(j):
        shift(v_ref, v_in, v_send, v_recv, j, sp).wait_recv()

    def doc_shift(j):
        return shift(doc_ref, doc_in, c_send, c_recv, j, reader(j))

    for j in range(slots):
        pl.when(inside(reader(j)))(lambda: doc_shift(j).start())
    start_keys(0, 1, 2)
    start_values(0, 1, 2)

    query_gains = column(qg_ref[...])
    for h in range(heads):
        q_aug[h, :HEAD, :] = turned(
            q_ref[:, h * HEAD : (h + 1) * HEAD], query_gains
        ).astype(jnp.bfloat16)
        labels = lax.broadcasted_iota(jnp.int32, (HEAD, length), 0)
        q_aug[h, HEAD:, :] = jnp.where(doc_ref[...] == labels, DOC_QUERY, 0.0).astype(
            jnp.bfloat16
        )

    def take(keys, values, docs, first):
        doc_col = jnp.broadcast_to(docs[...].astype(jnp.float32), (HEAD, length)).T
        lanes = lax.broadcasted_iota(jnp.int32, (length, HEAD), 1).astype(jnp.float32)
        k_aug[:, :HEAD] = keys[...]
        k_aug[:, HEAD:] = jnp.where(doc_col == lanes, DOC_KEY, 0.0).astype(jnp.bfloat16)
        vt_s[...] = values[...].T
        for h in range(heads):
            s = jnp.dot(k_aug[...], q_aug[h], preferred_element_type=jnp.float32)
            top = jnp.max(s, axis=0, keepdims=True)
            if not first:
                top = jnp.maximum(m_s[h], top)
            e = jnp.exp2((s - top) * EXP2_SCALE)
            den = jnp.sum(e, axis=0, keepdims=True)
            part = jnp.dot(
                vt_s[...], e.astype(jnp.bfloat16), preferred_element_type=jnp.float32
            )
            if first:
                l_s[h] = den
                acc_s[h] = part
            else:
                old = jnp.exp2((m_s[h] - top) * EXP2_SCALE)
                l_s[h] = l_s[h] * old + den
                acc_s[h] = acc_s[h] * old + part
            m_s[h] = top

    take(k_own, v_ref, doc_ref, True)

    key_wait(0)
    start_keys(3, 4)

    @pl.when(has_ahead)
    def _():
        value_wait(2)
        start_values(3, 6)

    @pl.when(has_behind)
    def _():
        value_wait(1)
        start_values(4)

    def step(j, carry):
        @pl.when(exists(j))
        def _():
            @pl.when(jnp.logical_and(j != 0, j != 3))
            def _():
                key_wait(j)

            @pl.when(jnp.logical_and(j != 1, j != 2))
            def _():
                value_wait(j)

            shift(doc_ref, doc_in, c_send, c_recv, j, sp).wait_recv()
            take(k_in.at[j], v_in.at[j], doc_in.at[j], False)

        @pl.when(jnp.logical_and(j == 1, has_behind))
        def _():
            key_wait(3)
            start_keys(5)

        @pl.when(jnp.logical_and(j == 2, has_spare))
        def _():
            value_wait(6)
            start_values(5)

        return carry

    lax.fori_loop(0, slots, step, 0)

    for h in range(heads):
        out = acc_s[h] / l_s[h]
        att_s[:, h * HEAD : (h + 1) * HEAD] = out.T.astype(jnp.bfloat16)

    def exchange(k):
        there = lax.rem(tp + k, n_tp)
        return pltpu.make_async_remote_copy(
            src_ref=att_s.at[pl.ds(pl.multiple_of(there * rows, rows), rows), :],
            dst_ref=all_s.at[tp],
            send_sem=t_send.at[k],
            recv_sem=t_recv.at[k],
            device_id=(sp, there),
            device_id_type=MESH,
        )

    for k in range(n_tp - 1, 0, -1):
        exchange(k).start()
    wo_copy.wait()

    def weight_rows(i):
        return wo_v[pl.ds(pl.multiple_of(i * width, width), width), :]

    projected = jnp.dot(
        att_s[pl.ds(pl.multiple_of(tp * rows, rows), rows), :],
        weight_rows(tp),
        preferred_element_type=jnp.float32,
    )
    for k in range(1, n_tp):
        exchange(k).wait_recv()
        source = lax.rem(tp - k + n_tp, n_tp)
        projected += jnp.dot(
            all_s[source], weight_rows(source), preferred_element_type=jnp.float32
        )
    hidden = (res_ref[...].astype(jnp.float32) + projected).astype(jnp.bfloat16)
    hid_s[...] = hidden
    wide = hidden.astype(jnp.float32)
    mean = jnp.mean(wide * wide, axis=-1, keepdims=True)
    nrm_s[...] = (wide * lax.rsqrt(mean + norm_eps) * gain_ref[...]).astype(jnp.bfloat16)

    def tell(i, block):
        return pltpu.make_async_remote_copy(
            src_ref=meta_s,
            dst_ref=metas.at[block],
            send_sem=m_send.at[i],
            recv_sem=m_recv.at[block],
            device_id=place(lax.rem(plane + i, groups) * members + pos),
            device_id_type=MESH,
        )

    def pass_on(source, block, way, c):
        part = pl.ds(c * piece, piece)
        return pltpu.make_async_remote_copy(
            src_ref=source.at[part],
            dst_ref=blocks.at[block, part],
            send_sem=z_send.at[way, block, c],
            recv_sem=z_recv.at[block, c],
            device_id=place(me + (2 * way - 1) * members),
            device_id_type=MESH,
        )

    def dispatch(block, peer, landing):
        return pltpu.make_async_remote_copy(
            src_ref=picked.at[block, region(peer)],
            dst_ref=arrived.at[block, region(landing)],
            send_sem=d_send.at[block, peer],
            recv_sem=d_recv.at[block, landing],
            device_id=place(plane * members + peer),
            device_id_type=MESH,
        )

    def give_home(block, origin, c):
        part = pl.ds(c * piece, piece)
        return pltpu.make_async_remote_copy(
            src_ref=answer.at[block, part],
            dst_ref=homing.at[origin, part],
            send_sem=h_send.at[block, c],
            recv_sem=h_recv.at[origin, c],
            device_id=place(block * members + pos),
            device_id_type=MESH,
        )

    def give_back(source, origin, member, landing):
        return pltpu.make_async_remote_copy(
            src_ref=source.at[region(member)],
            dst_ref=returned.at[region(origin * members + landing)],
            send_sem=r_send.at[origin, member],
            recv_sem=r_recv.at[origin, landing],
            device_id=place(plane * members + member),
            device_id_type=MESH,
        )

    def give_across(block, member, landing):
        return pltpu.make_async_remote_copy(
            src_ref=answer.at[block, region(member)],
            dst_ref=back.at[block, region(landing)],
            send_sem=b_send.at[block, member],
            recv_sem=b_recv.at[block, landing],
            device_id=place(plane * members + member),
            device_id_type=MESH,
        )

    def give_next(block, way, c):
        part = pl.ds(c * piece, piece)
        return pltpu.make_async_remote_copy(
            src_ref=joined.at[block, part],
            dst_ref=midway.at[way, part],
            send_sem=j_send.at[block, c],
            recv_sem=y_recv.at[way, c],
            device_id=place(me + (1 - 2 * way) * members),
            device_id_type=MESH,
        )

    def give_sum(block, way, c):
        part = pl.ds(c * piece, piece)
        return pltpu.make_async_remote_copy(
            src_ref=joined.at[block, part],
            dst_ref=summed.at[way, part],
            send_sem=j_send.at[block, c],
            recv_sem=s_recv.at[way, c],
            device_id=place(block * members + pos),
            device_id_type=MESH,
        )

    def others(act, first=1):
        def one(i, carry):
            act(lax.rem(pos + i, members))
            return carry

        lax.fori_loop(first, members, one, 0)

    for i in range(1, groups):
        tell(i, plane).start()
    for way in range(2):

        @pl.when(level(plane + 2 * way - 1))
        def _():
            for c in range(PIECES):
                pass_on(nrm_s, plane, way, c).start()

    def slot_rows(meta):
        experts = lax.broadcasted_iota(jnp.int32, (devices, rows), 0).astype(jnp.float32)
        hits = [experts == meta[k : k + 1, :] for k in range(top_count)]
        named = sum(hit.astype(jnp.float32) for hit in hits)
        ahead = (
            lax.broadcasted_iota(jnp.int32, (rows, rows), 0)
            < lax.broadcasted_iota(jnp.int32, (rows, rows), 1)
        )
        before = jnp.dot(
            named.astype(jnp.bfloat16),
            ahead.astype(jnp.float32).astype(jnp.bfloat16),
            preferred_element_type=jnp.float32,
        )
        return [
            meta[k : k + 1, :] * capacity
            + jnp.sum(jnp.where(hits[k], before, 0.0), axis=0, keepdims=True)
            for k in range(top_count)
        ]

    def slot_numbers(group):
        return (
            lax.broadcasted_iota(jnp.int32, (rows, rows), 0) + group * rows
        ).astype(jnp.float32)

    def gather(source, meta, block):
        numbers = slot_numbers(plane)
        choice = sum((numbers == row).astype(jnp.float32) for row in slot_rows(meta))
        picked[block] = jnp.dot(
            choice.astype(jnp.bfloat16), source[...], preferred_element_type=jnp.float32
        ).astype(jnp.bfloat16)
        others(lambda peer: dispatch(block, peer, pos).start())
        arrived[block, region(pos), :] = picked[block, region(pos), :]

    def expert(block):
        others(lambda peer: dispatch(block, peer, peer).wait_recv())
        x = arrived[block]
        gate_part = jnp.dot(x, gate_v[...], preferred_element_type=jnp.float32)
        up_part = jnp.dot(x, up_v[...], preferred_element_type=jnp.float32)
        activity = (jax.nn.silu(gate_part) * up_part).astype(jnp.bfloat16)
        answer[block] = jnp.dot(
            activity, down_v[...], preferred_element_type=jnp.float32
        ).astype(jnp.bfloat16)

    def both_ways(distance, act):
        def one(way, carry):
            block = plane - (2 * way - 1) * distance

            @pl.when(level(block))
            def _():
                act(block, way)

            return carry

        lax.fori_loop(0, 2, one, 0)

    gather(nrm_s, meta_s[...], plane)
    own_slots = slot_rows(meta_s[...])
    for g in range(groups):
        numbers = slot_numbers(g)
        weights = sum(
            jnp.where(numbers == own_slots[k], meta_s[top_count + k : top_count + k + 1, :], 0.0)
            for k in range(top_count)
        ).T
        high = weights.astype(jnp.bfloat16)
        spread[g, 0] = high
        spread[g, 1] = (weights - high.astype(jnp.float32)).astype(jnp.bfloat16)
    for load in loads:
        load.wait()

    def receive(block, way, c):
        pass_on(nrm_s, block, way, c).wait_recv()

        @pl.when(level(plane + 2 * way - 1))
        def _():
            pass_on(blocks.at[block], block, way, c).start()

    def collect(block, way):
        tell(1, block).wait_recv()
        gather(blocks.at[block], metas[block], block)

    def beyond(way):
        return level(plane - (1 - 2 * way))

    def past(block, way):
        return level(block + (1 - 2 * way))

    def relayed(distance, far):
        return far if distance == 2 else distance == 3

    def serve(block, way, distance):
        expert(block)
        joint = relayed(distance, beyond(way))

        def raw():
            for c in range(PIECES):
                give_home(block, plane, c).start()

        def through():
            others(lambda member: give_across(block, member, pos).start())
            back[block, region(pos), :] = answer[block, region(pos), :]

        if joint is True:
            through()
        elif joint is False:
            raw()
        else:
            pl.when(joint)(through)
            pl.when(jnp.logical_not(joint))(raw)

    def join(block):
        others(lambda member: give_across(block, member, member).wait_recv())
        meta = metas[block]
        numbers = slot_numbers(plane)
        lines = slot_rows(meta)
        weights = sum(
            jnp.where(numbers == lines[k], meta[top_count + k : top_count + k + 1, :], 0.0)
            for k in range(top_count)
        ).T
        high = weights.astype(jnp.bfloat16)
        low = (weights - high.astype(jnp.float32)).astype(jnp.bfloat16)
        joined[block] = (
            jnp.dot(high, back[block], preferred_element_type=jnp.float32)
            + jnp.dot(low, back[block], preferred_element_type=jnp.float32)
        ).astype(jnp.bfloat16)

    def begin_chain(block, way):
        join(block)
        for c in range(PIECES):
            give_next(block, way, c).start()

    def extend_chain(block, way):
        @pl.when(beyond(way))
        def _():
            join(block)
            for c in range(PIECES):
                part = pl.ds(c * piece, piece)
                give_next(block, way, c).wait_recv()
                joined[block, part, :] = (
                    joined[block, part, :].astype(jnp.float32)
                    + midway[way, part, :].astype(jnp.float32)
                ).astype(jnp.bfloat16)
                give_sum(block, way, c).start()

    def serve_at(distance):
        both_ways(distance, functools.partial(serve, distance=distance))

    def share(origin, way, distance):
        def pieces():
            for c in range(PIECES):
                give_home(origin, origin, c).wait_recv()
                for i in range(c * members // PIECES, (c + 1) * members // PIECES):

                    @pl.when(pos != i)
                    def _():
                        give_back(homing.at[origin], origin, i, pos).start()

            returned[region(origin * members + pos), :] = homing[origin, region(pos), :]

        on(raw_from(origin, way, distance), pieces)

    def raw_from(origin, way, distance):
        joint = relayed(distance, level(origin - (2 * way - 1)))
        return not joint if isinstance(joint, bool) else jnp.logical_not(joint)

    def share_at(distance):
        if distance != 3:
            both_ways(distance, functools.partial(share, distance=distance))

    for distance in range(1, groups):
        for c in range(PIECES):
            if c == PIECES - 1:
                if distance == 1:
                    expert(plane)
                    others(lambda member: give_back(answer.at[plane], plane, member, pos).start())
                    returned[region(me), :] = answer[plane, region(pos), :]
                else:
                    serve_at(distance - 1)
            both_ways(distance, functools.partial(receive, c=c))
        both_ways(distance, collect)
        if distance > 2:
            share_at(distance - 2)
    serve_at(groups - 1)
    if groups > 3:
        both_ways(3, begin_chain)
    share_at(max(1, groups - 2))
    both_ways(2, extend_chain)
    share_at(groups - 1)

    total = hid_s[...].astype(jnp.float32)

    def combine(group):
        back = returned[pl.ds(pl.multiple_of(group * rows, rows), rows), :]
        part = jnp.dot(spread[group, 0], back, preferred_element_type=jnp.float32)
        return part + jnp.dot(spread[group, 1], back, preferred_element_type=jnp.float32)

    def gathered(origin):
        others(lambda member: give_back(homing.at[origin], origin, member, member).wait_recv())
        return combine(origin)

    total_s[...] = total + gathered(plane)

    def add(origin, way, distance):
        def slots_back():
            total_s[...] += gathered(origin)

        def sum_back():
            for c in range(PIECES):
                give_sum(origin, 1 - way, c).wait_recv()
            total_s[...] += summed[1 - way].astype(jnp.float32)

        raw = raw_from(origin, way, distance)
        on(raw, slots_back)
        if distance == 2:
            pl.when(jnp.logical_not(raw))(sum_back)

    for distance in range(1, groups):
        if distance != 3:
            both_ways(distance, functools.partial(add, distance=distance))
    new_ref[...] = total_s[...].astype(jnp.bfloat16)

    for i in range(1, groups):
        tell(i, plane).wait_send()
    for way in range(2):

        @pl.when(level(plane + 2 * way - 1))
        def _():
            for c in range(PIECES):
                pass_on(nrm_s, plane, way, c).wait_send()

    def sent(block, way, distance):
        @pl.when(level(plane + 2 * way - 1))
        def _():
            for c in range(PIECES):
                pass_on(nrm_s, block, way, c).wait_send()

        others(lambda peer: dispatch(block, peer, pos).wait_send())

        def shared():
            others(lambda member: give_back(homing.at[block], block, member, pos).wait_send())

        def raw():
            for c in range(PIECES):
                give_home(block, plane, c).wait_send()

        def through():
            others(lambda member: give_across(block, member, pos).wait_send())
            for c in range(PIECES):
                give_next(block, way, c).wait_send()

        if distance != 3:
            on(raw_from(block, way, distance), shared)
        joint = relayed(distance, beyond(way))
        if joint is True:
            through()
        elif joint is False:
            raw()
        else:
            pl.when(joint)(through)
            pl.when(jnp.logical_not(joint))(raw)

    others(lambda peer: dispatch(plane, peer, pos).wait_send())
    others(lambda member: give_back(answer.at[plane], plane, member, pos).wait_send())
    for distance in range(1, groups):
        both_ways(distance, functools.partial(sent, distance=distance))


    for i in range(slots):
        on(key_plan[i][2], lambda: key_shift(i).wait_send())
        pl.when(inside(reader(i)))(lambda: doc_shift(i).wait_send())
    for i in range(slots + 1):
        on(value_plan[i][2], lambda: value_shift(i).wait_send())
    for k in range(1, n_tp):
        exchange(k).wait_send()


def run_layer(
    query_proj, key_proj, value_proj, docs, query_gain, key_gain, expert_ids, route_weights,
    residual, norm_gain, output_weight, gate_weight, up_weight, down_weight, capacity,
):
    n_sp, n_tp = lax.axis_size("sp"), lax.axis_size("tp")
    length = key_proj.shape[0]
    heads = query_proj.shape[1] // HEAD
    rows, model = residual.shape
    top_count = expert_ids.shape[0]
    members = rows // capacity
    groups = n_sp * n_tp // members
    slots = len(OFFSETS)
    block = (length, HEAD)
    narrow = jnp.bfloat16
    vmem = pl.BlockSpec(memory_space=pltpu.VMEM)
    anywhere = pl.BlockSpec(memory_space=pl.ANY)
    buffer = pltpu.VMEM((groups, rows, model), narrow)
    dma = pltpu.SemaphoreType.DMA
    return pl.pallas_call(
        functools.partial(layer_kernel, n_sp, n_tp, capacity, top_count),
        out_shape=jax.ShapeDtypeStruct(residual.shape, narrow),
        in_specs=[vmem] * 10 + [anywhere] * 4,
        out_specs=vmem,
        scratch_shapes=[
            pltpu.VMEM(output_weight.shape, narrow),
            pltpu.VMEM(gate_weight.shape[1:], narrow),
            pltpu.VMEM(up_weight.shape[1:], narrow),
            pltpu.VMEM(down_weight.shape[1:], narrow),
            pltpu.VMEM((HEAD // 2, length), jnp.float32),
            pltpu.VMEM((HEAD // 2, length), jnp.float32),
            pltpu.VMEM((8, rows), jnp.float32),
            pltpu.VMEM((heads, 2 * HEAD, length), narrow),
            pltpu.VMEM(block, narrow),
            pltpu.VMEM((slots,) + block, narrow),
            pltpu.VMEM((slots + 1,) + block, narrow),
            pltpu.VMEM((slots,) + docs.shape, jnp.int32),
            pltpu.VMEM((length, 2 * HEAD), narrow),
            pltpu.VMEM((HEAD, length), narrow),
            pltpu.VMEM((heads, 1, length), jnp.float32),
            pltpu.VMEM((heads, 1, length), jnp.float32),
            pltpu.VMEM((heads, HEAD, length), jnp.float32),
            pltpu.VMEM((length, heads * HEAD), narrow),
            pltpu.VMEM((n_tp, rows, heads * HEAD), narrow),
            pltpu.VMEM((rows, model), narrow),
            pltpu.VMEM((rows, model), narrow),
            pltpu.VMEM((groups, 8, rows), jnp.float32),
            buffer,
            buffer,
            buffer,
            buffer,
            buffer,
            pltpu.VMEM((groups * rows, model), narrow),
            pltpu.VMEM((groups, 2, rows, rows), narrow),
            pltpu.VMEM((rows, model), jnp.float32),
            buffer,
            buffer,
            pltpu.VMEM((2, rows, model), narrow),
            pltpu.VMEM((2, rows, model), narrow),
            dma((slots,)),
            dma((slots,)),
            dma((slots + 1,)),
            dma((slots + 1,)),
            dma((slots,)),
            dma((slots,)),
            dma((n_tp,)),
            dma((n_tp,)),
            dma((groups,)),
            dma((groups,)),
            dma((2, groups, PIECES)),
            dma((groups, PIECES)),
            dma((groups, members)),
            dma((groups, members)),
            dma((groups, PIECES)),
            dma((groups, PIECES)),
            dma((groups, members)),
            dma((groups, members)),
            dma((groups, members)),
            dma((groups, members)),
            dma((groups, PIECES)),
            dma((2, PIECES)),
            dma((2, PIECES)),
            dma((4,)),
        ],
        compiler_params=pltpu.CompilerParams(
            collective_id=1, has_side_effects=True, vmem_limit_bytes=60 * 1024 * 1024
        ),
    )(
        query_proj, key_proj, value_proj, docs,
        query_gain.reshape(1, -1), key_gain.reshape(1, -1), expert_ids, route_weights,
        residual, norm_gain.reshape(1, -1),
        output_weight, gate_weight, up_weight, down_weight,
    )


def rotary_tables(first_row, length):
    freq_count = HEAD // 4
    inverse = 1.0 / rope_base ** (jnp.arange(freq_count, dtype=jnp.float32) / freq_count)
    position = first_row + jnp.arange(length, dtype=jnp.int32)
    grid_row = (position // GRID_W).astype(jnp.float32)
    grid_col = (position % GRID_W).astype(jnp.float32)
    angles = jnp.concatenate(
        [grid_row[:, None] * inverse[None, :], grid_col[:, None] * inverse[None, :]], axis=1
    )
    return (jnp.cos(angles), jnp.sin(angles))


def norm_rotate(projected, gains, cosine, sine_table):
    length = projected.shape[0]
    values_wide = projected.astype(jnp.float32).reshape(length, -1, HEAD)
    scaled = (
        values_wide
        * lax.rsqrt(jnp.mean(values_wide * values_wide, axis=-1, keepdims=True) + norm_eps)
        * gains
    )
    half_size = HEAD // 2
    first_half = scaled[..., :half_size]
    second_half = scaled[..., half_size:]
    cosine_rows = cosine[:, None, :]
    sine_rows = sine_table[:, None, :]
    turned = jnp.concatenate(
        [
            first_half * cosine_rows - second_half * sine_rows,
            first_half * sine_rows + second_half * cosine_rows,
        ],
        axis=-1,
    )
    return turned.reshape(length, -1).astype(jnp.bfloat16)


def attention_kernel(
    n_sp, n_tp, q_ref, k_ref, vt_ref, doc_ref, res_ref, gain_ref, wo_hbm,
    hid_ref, nrm_ref,
    wo_v, k_in, vt_in, doc_in, k_aug, m_s, l_s, acc_s, att_s, all_s,
    send, recv, t_send, t_recv, w_sem,
):
    sp = lax.axis_index("sp")
    tp = lax.axis_index("tp")
    heads = q_ref.shape[0]
    rows = res_ref.shape[0]
    width = att_s.shape[1]
    slots = 2 * REACH

    def distance(j):
        return (j // 2 + 1) * (1 - 2 * (j % 2))

    def inside(index):
        return jnp.logical_and(index >= 0, index < n_sp)

    wo_copy = pltpu.make_async_copy(wo_hbm, wo_v, w_sem)
    wo_copy.start()

    barrier = pltpu.get_barrier_semaphore()
    for j in range(slots):
        there = sp + distance(j)

        @pl.when(inside(there))
        def _():
            pl.semaphore_signal(barrier, inc=1, device_id=(there, tp), device_id_type=MESH)

    for k in range(1, n_tp):
        pl.semaphore_signal(
            barrier, inc=1, device_id=(sp, lax.rem(tp + k, n_tp)), device_id_type=MESH
        )
    beside = jnp.minimum(sp, REACH) + jnp.minimum(n_sp - 1 - sp, REACH)
    pl.semaphore_wait(barrier, n_tp - 1 + beside)

    def copies(j):
        there = (sp + distance(j), tp)
        return [
            pltpu.make_async_remote_copy(
                src_ref=one,
                dst_ref=into.at[j],
                send_sem=send.at[j, i],
                recv_sem=recv.at[j, i],
                device_id=there,
                device_id_type=MESH,
            )
            for i, (one, into) in enumerate(((k_ref, k_in), (vt_ref, vt_in), (doc_ref, doc_in)))
        ]

    for j in range(slots):

        @pl.when(inside(sp + distance(j)))
        def _():
            for copy in copies(j):
                copy.start()

    def take(keys, values_t, docs, first):
        length = keys.shape[0]
        doc_col = jnp.broadcast_to(docs[0:1, :], (HEAD, length)).T
        lanes = lax.broadcasted_iota(jnp.int32, (length, HEAD), 1).astype(jnp.float32)
        k_aug[:, :HEAD] = keys[...]
        k_aug[:, HEAD:] = jnp.where(doc_col == lanes, DOC_KEY, 0.0).astype(jnp.bfloat16)
        for h in range(heads):
            s = jnp.dot(k_aug[...], q_ref[h], preferred_element_type=jnp.float32)
            top = jnp.max(s, axis=0, keepdims=True)
            if not first:
                top = jnp.maximum(m_s[h], top)
            e = jnp.exp2((s - top) * EXP2_SCALE)
            den = jnp.sum(e, axis=0, keepdims=True)
            part = jnp.dot(
                values_t[...], e.astype(jnp.bfloat16), preferred_element_type=jnp.float32
            )
            if first:
                l_s[h] = den
                acc_s[h] = part
            else:
                old = jnp.exp2((m_s[h] - top) * EXP2_SCALE)
                l_s[h] = l_s[h] * old + den
                acc_s[h] = acc_s[h] * old + part
            m_s[h] = top

    take(k_ref, vt_ref, doc_ref, True)

    def step(j, carry):
        @pl.when(inside(sp - distance(j)))
        def _():
            for copy in copies(j):
                copy.wait_recv()
            take(k_in.at[j], vt_in.at[j], doc_in.at[j], False)

        return carry

    lax.fori_loop(0, slots, step, 0)

    for h in range(heads):
        out = acc_s[h] / l_s[h]
        att_s[:, h * HEAD : (h + 1) * HEAD] = out.T.astype(jnp.bfloat16)

    def exchange(k):
        there = lax.rem(tp + k, n_tp)
        return pltpu.make_async_remote_copy(
            src_ref=att_s.at[pl.ds(pl.multiple_of(there * rows, rows), rows), :],
            dst_ref=all_s.at[tp],
            send_sem=t_send.at[k],
            recv_sem=t_recv.at[k],
            device_id=(sp, there),
            device_id_type=MESH,
        )

    for k in range(n_tp - 1, 0, -1):
        exchange(k).start()
    wo_copy.wait()

    def weight_rows(i):
        return wo_v[pl.ds(pl.multiple_of(i * width, width), width), :]

    projected = jnp.dot(
        att_s[pl.ds(pl.multiple_of(tp * rows, rows), rows), :],
        weight_rows(tp),
        preferred_element_type=jnp.float32,
    )
    for k in range(1, n_tp):
        exchange(k).wait_recv()
        source = lax.rem(tp - k + n_tp, n_tp)
        projected += jnp.dot(
            all_s[source], weight_rows(source), preferred_element_type=jnp.float32
        )
    hidden = (res_ref[...].astype(jnp.float32) + projected).astype(jnp.bfloat16)
    hid_ref[...] = hidden
    wide = hidden.astype(jnp.float32)
    mean = jnp.mean(wide * wide, axis=-1, keepdims=True)
    nrm_ref[...] = (wide * lax.rsqrt(mean + norm_eps) * gain_ref[...]).astype(jnp.bfloat16)

    for j in range(slots):

        @pl.when(inside(sp + distance(j)))
        def _():
            for copy in copies(j):
                copy.wait_send()

    for k in range(1, n_tp):
        exchange(k).wait_send()


def attend(q_aug, key_norm, value_t, doc_rows, residual, norm_gain, output_weight):
    n_sp, n_tp = lax.axis_size("sp"), lax.axis_size("tp")
    heads, deep, length = q_aug.shape
    rows, model = residual.shape
    vmem = pl.BlockSpec(memory_space=pltpu.VMEM)
    slots = 2 * REACH
    return pl.pallas_call(
        functools.partial(attention_kernel, n_sp, n_tp),
        out_shape=[jax.ShapeDtypeStruct((rows, model), jnp.bfloat16)] * 2,
        in_specs=[vmem] * 6 + [pl.BlockSpec(memory_space=pl.ANY)],
        out_specs=[vmem] * 2,
        scratch_shapes=[
            pltpu.VMEM(output_weight.shape, jnp.bfloat16),
            pltpu.VMEM((slots,) + key_norm.shape, jnp.bfloat16),
            pltpu.VMEM((slots,) + value_t.shape, jnp.bfloat16),
            pltpu.VMEM((slots,) + doc_rows.shape, jnp.float32),
            pltpu.VMEM((length, deep), jnp.bfloat16),
            pltpu.VMEM((heads, 1, length), jnp.float32),
            pltpu.VMEM((heads, 1, length), jnp.float32),
            pltpu.VMEM((heads, HEAD, length), jnp.float32),
            pltpu.VMEM((length, heads * HEAD), jnp.bfloat16),
            pltpu.VMEM((n_tp, rows, heads * HEAD), jnp.bfloat16),
            pltpu.SemaphoreType.DMA((slots, 3)),
            pltpu.SemaphoreType.DMA((slots, 3)),
            pltpu.SemaphoreType.DMA((n_tp,)),
            pltpu.SemaphoreType.DMA((n_tp,)),
            pltpu.SemaphoreType.DMA(()),
        ],
        compiler_params=pltpu.CompilerParams(
            collective_id=1, has_side_effects=True, vmem_limit_bytes=48 * 1024 * 1024
        ),
    )(q_aug, key_norm, value_t, doc_rows, residual, norm_gain.reshape(1, -1), output_weight)


def plain_on_device(
    residual,
    query_proj,
    key_proj,
    value_proj,
    query_gain,
    key_gain,
    document_ids,
    output_weight,
    norm_gain,
    expert_ids,
    route_weights,
    gate_weight,
    up_weight,
    down_weight,
):
    rows_here = query_proj.shape[0]
    cosine, sine_table = rotary_tables(lax.axis_index("sp") * rows_here, rows_here)
    query_norm = norm_rotate(query_proj, query_gain, cosine, sine_table)
    key_norm = norm_rotate(key_proj, key_gain, cosine, sine_table)
    heads = query_proj.shape[1] // HEAD
    docs = document_ids.astype(jnp.float32)
    query_t = jnp.transpose(query_norm.reshape(rows_here, heads, HEAD), (1, 2, 0))
    query_doc = jnp.where(
        docs[None, :] == jnp.arange(HEAD, dtype=jnp.float32)[:, None], DOC_QUERY, 0.0
    ).astype(jnp.bfloat16)
    q_aug = jnp.concatenate(
        [query_t, jnp.broadcast_to(query_doc[None], (heads, HEAD, rows_here))], axis=1
    )
    doc_rows = jnp.broadcast_to(docs[None, :], (8, rows_here))
    hidden, normed = attend(
        q_aug, key_norm, value_proj.T, doc_rows, residual, norm_gain, output_weight
    )
    token_rows = residual.shape[0]
    top_count = expert_ids.shape[1]
    experts_all = lax.axis_size("sp") * lax.axis_size("tp")
    capacity = max(2, 2 * token_rows * top_count // experts_all)
    flat_ids = expert_ids.reshape(-1)
    order = jnp.arange(flat_ids.shape[0], dtype=jnp.int32)
    earlier = jnp.logical_and(
        flat_ids[:, None] == flat_ids[None, :], order[None, :] < order[:, None]
    )
    arrival = jnp.sum(earlier.astype(jnp.int32), axis=1)
    slot_index = flat_ids * capacity + arrival
    slot_grid = slot_index.reshape(token_rows, top_count)
    placing = jnp.sum(
        (
            jnp.arange(experts_all * capacity, dtype=jnp.int32)[:, None, None] == slot_grid[None]
        ).astype(jnp.float32),
        axis=2,
    ).astype(jnp.bfloat16)
    outgoing = jnp.dot(placing, normed, preferred_element_type=jnp.float32).astype(jnp.bfloat16)
    spread = jnp.sum(
        jnp.where(
            jnp.arange(experts_all * capacity, dtype=jnp.int32)[None, None, :]
            == slot_grid[:, :, None],
            route_weights[:, :, None],
            0.0,
        ),
        axis=1,
    )
    high = spread.astype(jnp.bfloat16)
    low = (spread - high.astype(jnp.float32)).astype(jnp.bfloat16)
    outgoing = outgoing.reshape(experts_all, capacity, normed.shape[1])
    arrived = lax.all_to_all(outgoing, ("sp", "tp"), split_axis=0, concat_axis=0, tiled=True)
    sources, slots, width = arrived.shape
    flat_rows = arrived.reshape(sources * slots, width)
    gate_part = jnp.dot(flat_rows, gate_weight[0], preferred_element_type=jnp.float32)
    up_part = jnp.dot(flat_rows, up_weight[0], preferred_element_type=jnp.float32)
    activity = (jax.nn.silu(gate_part) * up_part).astype(jnp.bfloat16)
    expert_out = jnp.dot(activity, down_weight[0], preferred_element_type=jnp.float32).astype(
        jnp.bfloat16
    )
    returned = lax.all_to_all(
        expert_out.reshape(sources, slots, width),
        ("sp", "tp"),
        split_axis=0,
        concat_axis=0,
        tiled=True,
    )
    rows_back = returned.reshape(experts_all * capacity, -1)
    combined = jnp.dot(high, rows_back, preferred_element_type=jnp.float32) + jnp.dot(
        low, rows_back, preferred_element_type=jnp.float32
    )
    return (hidden.astype(jnp.float32) + combined).astype(jnp.bfloat16)


def on_device(*arrays):
    (
        residual, query_proj, key_proj, value_proj, query_gain, key_gain, document_ids,
        output_weight, norm_gain, expert_ids, route_weights, gate_weight, up_weight, down_weight,
    ) = arrays
    token_rows = residual.shape[0]
    top_count = expert_ids.shape[1]
    experts_all = lax.axis_size("sp") * lax.axis_size("tp")
    capacity = max(2, 2 * token_rows * top_count // experts_all)
    if (
        capacity % 16 == 0
        and token_rows == HEAD
        and token_rows % capacity == 0
        and experts_all % (token_rows // capacity) == 0
        and experts_all * capacity > 2 * token_rows
        and 2 * top_count <= 8
        and lax.axis_size("sp") % 2 == 0
    ):
        return run_layer(
            query_proj, key_proj, value_proj, document_ids.reshape(1, -1), query_gain, key_gain,
            expert_ids.T, route_weights.T, residual, norm_gain, output_weight,
            gate_weight, up_weight, down_weight, capacity,
        )
    return plain_on_device(*arrays)


def solution(mesh):
    in_specs = (
        P(("sp", "tp"), None),
        P("sp", "tp"),
        P("sp", "tp"),
        P("sp", "tp"),
        P(),
        P(),
        P("sp"),
        P(),
        P(),
        P(("sp", "tp"), None),
        P(("sp", "tp"), None),
        P(("sp", "tp"), None, None),
        P(("sp", "tp"), None, None),
        P(("sp", "tp"), None, None),
    )
    out_specs = P(("sp", "tp"), None)
    return jax.shard_map(
        on_device, mesh=mesh, in_specs=in_specs, out_specs=out_specs, check_vma=False
    )
```

```python
import functools
import math

import jax
import jax.numpy as jnp
from jax import lax
from jax.experimental import pallas as pl
from jax.experimental.pallas import tpu as pltpu
from jax.sharding import PartitionSpec as P

HEAD = 128
GRID_W = 64
REACH = 3


norm_eps = 1e-06
rope_base = 10000.0
masked_low = -1e30
MESH = pl.DeviceIdType.MESH
DOC_KEY = 128.0
DOC_QUERY = 64.0
PIECES = 4
HALVES = 2
LINE = 4
OFFSETS = (1, -2, 2, -1, 3, -3)
EXP2_SCALE = math.log2(math.e) / math.sqrt(HEAD)


def layer_kernel(
    n_sp, n_tp, capacity, top_count,
    q_hbm, k_hbm, v_hbm, doc_hbm, qg_hbm, kg_hbm, ids_hbm, rw_hbm, res_hbm, gain_hbm,
    wo_hbm, gate_hbm, up_hbm, down_hbm,
    new_ref,
    k_ref, v_ref, kg_ref, doc_ref, q_ref, qg_ref, ids_ref, rw_ref, res_ref, gain_ref,
    wo_v, gate_v, up_v, down_v, cos_s, sin_s, meta_s, q_aug, k_own, k_in, v_in, doc_in,
    k_aug, vt_s, m_s, l_s, acc_s, att_s, all_s, hid_s, nrm_s,
    metas, blocks, picked, arrived, answer, homing, returned, spread, total_s,
    back, joined, midway, summed,
    k_send, k_recv, v_send, v_recv, c_send, c_recv, t_send, t_recv,
    m_send, m_recv, z_send, z_recv, d_send, d_recv, h_send, h_recv, r_send, r_recv,
    b_send, b_recv, j_send, y_recv, s_recv, w_sem,
):
    devices = n_sp * n_tp
    rows = res_ref.shape[0]
    members = rows // capacity
    groups = devices // members
    piece = rows // PIECES
    sp = lax.axis_index("sp")
    tp = lax.axis_index("tp")
    me = sp * n_tp + tp
    plane = lax.div(me, members)
    pos = lax.rem(me, members)

    fetches = [
        pltpu.make_async_copy(source, into, w_sem.at[i])
        for i, (source, into) in enumerate(
            (
                (kg_hbm, kg_ref), (k_hbm, k_ref), (v_hbm, v_ref), (doc_hbm, doc_ref),
                (ids_hbm, ids_ref), (rw_hbm, rw_ref), (qg_hbm, qg_ref), (q_hbm, q_ref),
                (wo_hbm, wo_v), (res_hbm, res_ref), (gain_hbm, gain_ref),
                (gate_hbm.at[0], gate_v), (up_hbm.at[0], up_v), (down_hbm.at[0], down_v),
            )
        )
    ]
    for fetch in fetches:
        fetch.start()

    def fetched(*which):
        for i in which:
            fetches[i].wait()

    def place(device):
        return (lax.div(device, n_tp), lax.rem(device, n_tp))

    def region(index):
        return pl.ds(pl.multiple_of(index * capacity, capacity), capacity)

    length = k_ref.shape[0]
    heads = q_ref.shape[1] // HEAD
    width = att_s.shape[1]
    slots = len(OFFSETS)
    half = HEAD // 2
    side = 1 - 2 * lax.rem(sp, 2)
    across, ahead, behind = sp + side, sp + 2 * side, sp - 2 * side

    def inside(index):
        return jnp.logical_and(index >= 0, index < n_sp)

    has_ahead, has_behind = inside(ahead), inside(behind)
    has_spare = inside(sp + 4 * side)

    def offset(j):
        return sum(jnp.where(j == i, o, 0) for i, o in enumerate(OFFSETS))

    def exists(j):
        return inside(sp + side * offset(j))

    def reader(j):
        odd = OFFSETS[j] % 2 == 1
        return sp + side * OFFSETS[j] if odd else sp - side * OFFSETS[j]

    barrier = pltpu.get_barrier_semaphore()

    def greet(i, carry):
        there = lax.rem(me + i, devices)
        pl.semaphore_signal(barrier, inc=1, device_id=place(there), device_id_type=MESH)
        return carry

    lax.fori_loop(1, devices, greet, 0)

    def column(row):
        return jnp.broadcast_to(row, (HEAD, HEAD)).T[:, :1]

    freq_count = HEAD // 4
    exponent = lax.broadcasted_iota(jnp.int32, (freq_count, 1), 0).astype(jnp.float32) / freq_count
    inverse = jnp.exp2(exponent * -math.log2(rope_base))
    position = sp * length + lax.broadcasted_iota(jnp.int32, (1, length), 1)
    grid_row = lax.div(position, GRID_W).astype(jnp.float32)
    grid_col = lax.rem(position, GRID_W).astype(jnp.float32)
    angles = jnp.concatenate([inverse * grid_row, inverse * grid_col], axis=0)
    cos_s[...] = jnp.cos(angles)
    sin_s[...] = jnp.sin(angles)

    def turned(projected, gains):
        wide = projected.astype(jnp.float32).T
        scaled = (
            wide * lax.rsqrt(jnp.mean(wide * wide, axis=0, keepdims=True) + norm_eps) * gains
        )
        upper, lower = scaled[:half], scaled[half:]
        cosine, sine = cos_s[...], sin_s[...]
        return jnp.concatenate(
            [upper * cosine - lower * sine, upper * sine + lower * cosine], axis=0
        )

    fetched(0, 1)
    k_own[...] = turned(k_ref[...], column(kg_ref[...])).T.astype(jnp.bfloat16)
    fetched(2, 3, 4, 5)
    for k in range(top_count):
        for r, table in ((k, ids_ref), (top_count + k, rw_ref)):
            meta_s[r : r + 1, :] = table[k : k + 1, :].astype(jnp.float32)
    pl.semaphore_wait(barrier, devices - 1)

    def tell(i, block):
        return pltpu.make_async_remote_copy(
            src_ref=meta_s,
            dst_ref=metas.at[block],
            send_sem=m_send.at[i],
            recv_sem=m_recv.at[block],
            device_id=place(lax.rem(plane + i, groups) * members + pos),
            device_id_type=MESH,
        )

    def shift(source, into, sends, receives, i, there):
        return pltpu.make_async_remote_copy(
            src_ref=source,
            dst_ref=into.at[i],
            send_sem=sends.at[i],
            recv_sem=receives.at[i],
            device_id=(there, tp),
            device_id_type=MESH,
        )

    key_plan = (
        (k_own, across, True),
        (k_own, ahead, has_ahead),
        (k_own, behind, has_behind),
        (k_in.at[0], ahead, has_ahead),
        (k_in.at[0], behind, has_behind),
        (k_in.at[3], ahead, jnp.logical_and(has_ahead, has_behind)),
    )
    value_plan = (
        (v_ref, across, True),
        (v_ref, ahead, has_ahead),
        (v_ref, behind, has_behind),
        (v_in.at[2], across, has_ahead),
        (v_in.at[1], across, has_behind),
        (v_in.at[6], across, has_spare),
        (v_in.at[2], behind, jnp.logical_and(has_ahead, has_behind)),
    )

    def key_shift(i):
        return shift(key_plan[i][0], k_in, k_send, k_recv, i, key_plan[i][1])

    def value_shift(i):
        return shift(value_plan[i][0], v_in, v_send, v_recv, i, value_plan[i][1])

    def on(allowed, act):
        if allowed is True:
            act()
        elif allowed is not False:
            pl.when(allowed)(act)

    def start_keys(*which):
        for i in which:
            on(key_plan[i][2], lambda: key_shift(i).start())

    def start_values(*which):
        for i in which:
            on(value_plan[i][2], lambda: value_shift(i).start())

    def key_wait(j):
        shift(k_own, k_in, k_send, k_recv, j, sp).wait_recv()

    def value_wait(j):
        shift(v_ref, v_in, v_send, v_recv, j, sp).wait_recv()

    def doc_shift(j):
        return shift(doc_ref, doc_in, c_send, c_recv, j, reader(j))

    for j in range(slots):
        pl.when(inside(reader(j)))(lambda: doc_shift(j).start())
    start_keys(0, 1, 2)
    start_values(0, 1, 2)
    for i in range(1, groups):
        tell(i, plane).start()

    fetched(6, 7)
    query_gains = column(qg_ref[...])
    for h in range(heads):
        q_aug[h, :HEAD, :] = turned(
            q_ref[:, h * HEAD : (h + 1) * HEAD], query_gains
        ).astype(jnp.bfloat16)
        labels = lax.broadcasted_iota(jnp.int32, (HEAD, length), 0)
        q_aug[h, HEAD:, :] = jnp.where(doc_ref[...] == labels, DOC_QUERY, 0.0).astype(
            jnp.bfloat16
        )

    def take(keys, values, docs, first):
        doc_col = jnp.broadcast_to(docs[...].astype(jnp.float32), (HEAD, length)).T
        lanes = lax.broadcasted_iota(jnp.int32, (length, HEAD), 1).astype(jnp.float32)
        k_aug[:, :HEAD] = keys[...]
        k_aug[:, HEAD:] = jnp.where(doc_col == lanes, DOC_KEY, 0.0).astype(jnp.bfloat16)
        vt_s[...] = values[...].T
        for h in range(heads):
            s = jnp.dot(k_aug[...], q_aug[h], preferred_element_type=jnp.float32)
            top = jnp.max(s, axis=0, keepdims=True)
            if not first:
                top = jnp.maximum(m_s[h], top)
            e = jnp.exp2((s - top) * EXP2_SCALE)
            den = jnp.sum(e, axis=0, keepdims=True)
            part = jnp.dot(
                vt_s[...], e.astype(jnp.bfloat16), preferred_element_type=jnp.float32
            )
            if first:
                l_s[h] = den
                acc_s[h] = part
            else:
                old = jnp.exp2((m_s[h] - top) * EXP2_SCALE)
                l_s[h] = l_s[h] * old + den
                acc_s[h] = acc_s[h] * old + part
            m_s[h] = top

    take(k_own, v_ref, doc_ref, True)

    key_wait(0)
    start_keys(3, 4)

    @pl.when(has_ahead)
    def _():
        value_wait(2)
        start_values(3, 6)

    @pl.when(has_behind)
    def _():
        value_wait(1)
        start_values(4)

    def step(j, carry):
        @pl.when(exists(j))
        def _():
            @pl.when(jnp.logical_and(j != 0, j != 3))
            def _():
                key_wait(j)

            @pl.when(jnp.logical_and(j != 1, j != 2))
            def _():
                value_wait(j)

            shift(doc_ref, doc_in, c_send, c_recv, j, sp).wait_recv()
            take(k_in.at[j], v_in.at[j], doc_in.at[j], False)

        @pl.when(jnp.logical_and(j == 1, has_behind))
        def _():
            key_wait(3)
            start_keys(5)

        @pl.when(jnp.logical_and(j == 2, has_spare))
        def _():
            value_wait(6)
            start_values(5)

        return carry

    lax.fori_loop(0, slots, step, 0)

    for h in range(heads):
        out = acc_s[h] / l_s[h]
        att_s[:, h * HEAD : (h + 1) * HEAD] = out.T.astype(jnp.bfloat16)

    part_rows = rows // HALVES

    def exchange(k, half):
        there = lax.rem(tp + k, n_tp)
        here = pl.ds(pl.multiple_of(there * rows + half * part_rows, part_rows), part_rows)
        return pltpu.make_async_remote_copy(
            src_ref=att_s.at[here, :],
            dst_ref=all_s.at[tp, pl.ds(half * part_rows, part_rows)],
            send_sem=t_send.at[k, half],
            recv_sem=t_recv.at[k, half],
            device_id=(sp, there),
            device_id_type=MESH,
        )

    for half in range(HALVES):
        for k in range(n_tp - 1, 0, -1):
            exchange(k, half).start()
    fetched(8, 9, 10)

    def weight_rows(i):
        return wo_v[pl.ds(pl.multiple_of(i * width, width), width), :]

    total_s[...] = res_ref[...].astype(jnp.float32) + jnp.dot(
        att_s[pl.ds(pl.multiple_of(tp * rows, rows), rows), :],
        weight_rows(tp),
        preferred_element_type=jnp.float32,
    )

    def project(half):
        part = pl.ds(half * part_rows, part_rows)
        projected = total_s[part, :]
        for k in range(1, n_tp):
            exchange(k, half).wait_recv()
            source = lax.rem(tp - k + n_tp, n_tp)
            projected += jnp.dot(
                all_s[source, part, :], weight_rows(source), preferred_element_type=jnp.float32
            )
        hidden = projected.astype(jnp.bfloat16)
        hid_s[part, :] = hidden
        wide = hidden.astype(jnp.float32)
        mean = jnp.mean(wide * wide, axis=-1, keepdims=True)
        nrm_s[part, :] = (wide * lax.rsqrt(mean + norm_eps) * gain_ref[...]).astype(jnp.bfloat16)

    def pass_on(source, block, way, c):
        part = pl.ds(c * piece, piece)
        return pltpu.make_async_remote_copy(
            src_ref=source.at[part],
            dst_ref=blocks.at[block, part],
            send_sem=z_send.at[way, block, c],
            recv_sem=z_recv.at[block, c],
            device_id=place(me + (2 * way - 1) * members),
            device_id_type=MESH,
        )

    def dispatch(block, peer, landing):
        return pltpu.make_async_remote_copy(
            src_ref=picked.at[block, region(peer)],
            dst_ref=arrived.at[block, region(landing)],
            send_sem=d_send.at[block, peer],
            recv_sem=d_recv.at[block, landing],
            device_id=place(plane * members + peer),
            device_id_type=MESH,
        )

    def give_home(block, origin, c):
        part = pl.ds(c * piece, piece)
        return pltpu.make_async_remote_copy(
            src_ref=answer.at[block, part],
            dst_ref=homing.at[origin, part],
            send_sem=h_send.at[block, c],
            recv_sem=h_recv.at[origin, c],
            device_id=place(block * members + pos),
            device_id_type=MESH,
        )

    def give_back(source, origin, member, landing):
        return pltpu.make_async_remote_copy(
            src_ref=source.at[region(member)],
            dst_ref=returned.at[region(origin * members + landing)],
            send_sem=r_send.at[origin, member],
            recv_sem=r_recv.at[origin, landing],
            device_id=place(plane * members + member),
            device_id_type=MESH,
        )

    def give_across(block, member, landing):
        return pltpu.make_async_remote_copy(
            src_ref=answer.at[block, region(member)],
            dst_ref=back.at[block, region(landing)],
            send_sem=b_send.at[block, member],
            recv_sem=b_recv.at[block, landing],
            device_id=place(plane * members + member),
            device_id_type=MESH,
        )

    def give_next(block, way, c):
        part = pl.ds(c * piece, piece)
        return pltpu.make_async_remote_copy(
            src_ref=joined.at[block, part],
            dst_ref=midway.at[way, part],
            send_sem=j_send.at[block, c],
            recv_sem=y_recv.at[way, c],
            device_id=place(me + (1 - 2 * way) * members),
            device_id_type=MESH,
        )

    def give_sum(block, way, c):
        part = pl.ds(c * piece, piece)
        return pltpu.make_async_remote_copy(
            src_ref=joined.at[block, part],
            dst_ref=summed.at[way, part],
            send_sem=j_send.at[block, c],
            recv_sem=s_recv.at[way, c],
            device_id=place(block * members + pos),
            device_id_type=MESH,
        )

    def others(act, first=1):
        def one(i, carry):
            act(lax.rem(pos + i, members))
            return carry

        lax.fori_loop(first, members, one, 0)

    low_side = plane < groups // 2
    toward = jnp.where(low_side, 1, -1)
    seen = jnp.where(low_side, 0, 1)
    inward, outward = 1 - seen, seen
    is_end = jnp.logical_or(plane == 0, plane == groups - 1)
    is_inner = jnp.logical_not(is_end)
    first = jnp.where(is_end, plane + toward, plane - toward)
    second = jnp.where(is_end, plane + 3 * toward, plane + 2 * toward)
    third = jnp.where(is_end, plane + 2 * toward, plane + toward)
    early, late = range(PIECES // 2), range(PIECES // 2, PIECES)

    def push(source, block, way, which):
        for c in which:
            pass_on(source, block, way, c).start()

    def landed(block, which):
        for c in which:
            pass_on(nrm_s, block, 0, c).wait_recv()

    def hop(block, way, which):
        for c in which:
            landed(block, (c,))
            push(blocks.at[block], block, way, (c,))

    for half in range(HALVES):
        project(half)
        ready = range(half * PIECES // HALVES, (half + 1) * PIECES // HALVES)

        @pl.when(is_end)
        def _():
            push(nrm_s, plane, inward, ready)

        @pl.when(is_inner)
        def _():
            for c in ready:
                push(nrm_s, plane, outward, (c,))
                if c in early:
                    push(nrm_s, plane, inward, (c,))

    def slot_rows(meta):
        experts = lax.broadcasted_iota(jnp.int32, (devices, rows), 0).astype(jnp.float32)
        hits = [experts == meta[k : k + 1, :] for k in range(top_count)]
        named = sum(hit.astype(jnp.float32) for hit in hits)
        ahead = (
            lax.broadcasted_iota(jnp.int32, (rows, rows), 0)
            < lax.broadcasted_iota(jnp.int32, (rows, rows), 1)
        )
        before = jnp.dot(
            named.astype(jnp.bfloat16),
            ahead.astype(jnp.float32).astype(jnp.bfloat16),
            preferred_element_type=jnp.float32,
        )
        return [
            meta[k : k + 1, :] * capacity
            + jnp.sum(jnp.where(hits[k], before, 0.0), axis=0, keepdims=True)
            for k in range(top_count)
        ]

    def slot_numbers(group):
        return (
            lax.broadcasted_iota(jnp.int32, (rows, rows), 0) + group * rows
        ).astype(jnp.float32)

    def gather(source, meta, block):
        numbers = slot_numbers(plane)
        choice = sum((numbers == row).astype(jnp.float32) for row in slot_rows(meta))
        picked[block] = jnp.dot(
            choice.astype(jnp.bfloat16), source[...], preferred_element_type=jnp.float32
        ).astype(jnp.bfloat16)
        others(lambda peer: dispatch(block, peer, pos).start())
        arrived[block, region(pos), :] = picked[block, region(pos), :]

    def expert(block):
        others(lambda peer: dispatch(block, peer, peer).wait_recv())
        x = arrived[block]
        gate_part = jnp.dot(x, gate_v[...], preferred_element_type=jnp.float32)
        up_part = jnp.dot(x, up_v[...], preferred_element_type=jnp.float32)
        activity = (jax.nn.silu(gate_part) * up_part).astype(jnp.bfloat16)
        answer[block] = jnp.dot(
            activity, down_v[...], preferred_element_type=jnp.float32
        ).astype(jnp.bfloat16)

    gather(nrm_s, meta_s[...], plane)
    own_slots = slot_rows(meta_s[...])
    for g in range(groups):
        numbers = slot_numbers(g)
        weights = sum(
            jnp.where(numbers == own_slots[k], meta_s[top_count + k : top_count + k + 1, :], 0.0)
            for k in range(top_count)
        ).T
        high = weights.astype(jnp.bfloat16)
        spread[g, 0] = high
        spread[g, 1] = (weights - high.astype(jnp.float32)).astype(jnp.bfloat16)
    fetched(11, 12, 13)

    def collect(block):
        tell(1, block).wait_recv()
        gather(blocks.at[block], metas[block], block)

    def serve_home(block):
        expert(block)
        for c in range(PIECES):
            give_home(block, plane, c).start()

    def serve_across(block):
        expert(block)
        others(lambda member: give_across(block, member, pos).start())
        back[block, region(pos), :] = answer[block, region(pos), :]

    def join(block):
        others(lambda member: give_across(block, member, member).wait_recv())
        meta = metas[block]
        numbers = slot_numbers(plane)
        lines = slot_rows(meta)
        weights = sum(
            jnp.where(numbers == lines[k], meta[top_count + k : top_count + k + 1, :], 0.0)
            for k in range(top_count)
        ).T
        high = weights.astype(jnp.bfloat16)
        low = (weights - high.astype(jnp.float32)).astype(jnp.bfloat16)
        joined[block] = (
            jnp.dot(high, back[block], preferred_element_type=jnp.float32)
            + jnp.dot(low, back[block], preferred_element_type=jnp.float32)
        ).astype(jnp.bfloat16)

    def share(origin):
        for c in range(PIECES):
            give_home(origin, origin, c).wait_recv()
            for i in range(c * members // PIECES, (c + 1) * members // PIECES):

                @pl.when(pos != i)
                def _():
                    give_back(homing.at[origin], origin, i, pos).start()

        returned[region(origin * members + pos), :] = homing[origin, region(pos), :]

    @pl.when(is_inner)
    def _():
        hop(first, inward, range(PIECES - 1))
        hop(second, outward, (0,))
        hop(first, inward, (PIECES - 1,))
        push(nrm_s, plane, inward, late)
        hop(second, outward, (1,))

    @pl.when(is_end)
    def _():
        landed(first, range(PIECES))

    collect(first)
    expert(plane)
    others(lambda member: give_back(answer.at[plane], plane, member, pos).start())
    returned[region(me), :] = answer[plane, region(pos), :]

    @pl.when(is_inner)
    def _():
        hop(second, outward, range(2, PIECES))
        hop(third, outward, early)

    @pl.when(is_end)
    def _():
        landed(second, range(PIECES))

    collect(second)
    serve_home(first)

    @pl.when(is_end)
    def _():
        serve_across(second)
        landed(third, range(PIECES))

    @pl.when(is_inner)
    def _():
        hop(third, outward, late)

    collect(third)

    @pl.when(is_inner)
    def _():
        serve_across(second)

    @pl.when(is_end)
    def _():
        join(second)
        for c in range(PIECES):
            give_next(second, seen, c).start()

    serve_home(third)
    share(first)

    @pl.when(is_inner)
    def _():
        join(second)
        for c in range(PIECES):
            part = pl.ds(c * piece, piece)
            give_next(second, seen, c).wait_recv()
            joined[second, part, :] = (
                joined[second, part, :].astype(jnp.float32)
                + midway[seen, part, :].astype(jnp.float32)
            ).astype(jnp.bfloat16)
            give_sum(second, seen, c).start()
        share(third)
        share(second)

    total = hid_s[...].astype(jnp.float32)

    def combine(group):
        back = returned[pl.ds(pl.multiple_of(group * rows, rows), rows), :]
        part = jnp.dot(spread[group, 0], back, preferred_element_type=jnp.float32)
        return part + jnp.dot(spread[group, 1], back, preferred_element_type=jnp.float32)

    def gathered(origin):
        others(lambda member: give_back(homing.at[origin], origin, member, member).wait_recv())
        return combine(origin)

    total_s[...] = total + gathered(plane) + gathered(first)

    @pl.when(is_inner)
    def _():
        total_s[...] += gathered(third)
        total_s[...] += gathered(second)

    @pl.when(is_end)
    def _():
        for c in range(PIECES):
            give_sum(third, 1 - seen, c).wait_recv()
        total_s[...] += summed[1 - seen].astype(jnp.float32)

    new_ref[...] = total_s[...].astype(jnp.bfloat16)

    for i in range(1, groups):
        tell(i, plane).wait_send()

    def gone(block, way):
        for c in range(PIECES):
            pass_on(nrm_s, block, way, c).wait_send()

    gone(plane, inward)

    @pl.when(is_inner)
    def _():
        gone(plane, outward)
        gone(first, inward)
        gone(second, outward)
        gone(third, outward)

    others(lambda peer: dispatch(plane, peer, pos).wait_send())
    others(lambda member: give_back(answer.at[plane], plane, member, pos).wait_send())
    for block in (first, second, third):
        others(lambda peer: dispatch(block, peer, pos).wait_send())
    for block in (first, third):
        for c in range(PIECES):
            give_home(block, plane, c).wait_send()
    others(lambda member: give_across(second, member, pos).wait_send())
    for c in range(PIECES):
        give_next(second, seen, c).wait_send()
    others(lambda member: give_back(homing.at[first], first, member, pos).wait_send())

    @pl.when(is_inner)
    def _():
        for block in (second, third):
            others(lambda member: give_back(homing.at[block], block, member, pos).wait_send())

    for i in range(slots):
        on(key_plan[i][2], lambda: key_shift(i).wait_send())
        pl.when(inside(reader(i)))(lambda: doc_shift(i).wait_send())
    for i in range(slots + 1):
        on(value_plan[i][2], lambda: value_shift(i).wait_send())
    for k in range(1, n_tp):
        for half in range(HALVES):
            exchange(k, half).wait_send()


def run_layer(
    query_proj, key_proj, value_proj, docs, query_gain, key_gain, expert_ids, route_weights,
    residual, norm_gain, output_weight, gate_weight, up_weight, down_weight, capacity,
):
    n_sp, n_tp = lax.axis_size("sp"), lax.axis_size("tp")
    length = key_proj.shape[0]
    heads = query_proj.shape[1] // HEAD
    rows, model = residual.shape
    top_count = expert_ids.shape[0]
    members = rows // capacity
    groups = n_sp * n_tp // members
    slots = len(OFFSETS)
    block = (length, HEAD)
    narrow = jnp.bfloat16
    vmem = pl.BlockSpec(memory_space=pltpu.VMEM)
    buffer = pltpu.VMEM((groups, rows, model), narrow)
    dma = pltpu.SemaphoreType.DMA
    return pl.pallas_call(
        functools.partial(layer_kernel, n_sp, n_tp, capacity, top_count),
        out_shape=jax.ShapeDtypeStruct(residual.shape, narrow),
        in_specs=[pl.BlockSpec(memory_space=pltpu.HBM)] * 14,
        out_specs=vmem,
        scratch_shapes=[
            pltpu.VMEM(block, narrow),
            pltpu.VMEM(block, narrow),
            pltpu.VMEM((1, HEAD), jnp.float32),
            pltpu.VMEM(docs.shape, jnp.int32),
            pltpu.VMEM(query_proj.shape, narrow),
            pltpu.VMEM((1, HEAD), jnp.float32),
            pltpu.VMEM(expert_ids.shape, jnp.int32),
            pltpu.VMEM(route_weights.shape, jnp.float32),
            pltpu.VMEM(residual.shape, narrow),
            pltpu.VMEM((1, model), jnp.float32),
            pltpu.VMEM(output_weight.shape, narrow),
            pltpu.VMEM(gate_weight.shape[1:], narrow),
            pltpu.VMEM(up_weight.shape[1:], narrow),
            pltpu.VMEM(down_weight.shape[1:], narrow),
            pltpu.VMEM((HEAD // 2, length), jnp.float32),
            pltpu.VMEM((HEAD // 2, length), jnp.float32),
            pltpu.VMEM((8, rows), jnp.float32),
            pltpu.VMEM((heads, 2 * HEAD, length), narrow),
            pltpu.VMEM(block, narrow),
            pltpu.VMEM((slots,) + block, narrow),
            pltpu.VMEM((slots + 1,) + block, narrow),
            pltpu.VMEM((slots,) + docs.shape, jnp.int32),
            pltpu.VMEM((length, 2 * HEAD), narrow),
            pltpu.VMEM((HEAD, length), narrow),
            pltpu.VMEM((heads, 1, length), jnp.float32),
            pltpu.VMEM((heads, 1, length), jnp.float32),
            pltpu.VMEM((heads, HEAD, length), jnp.float32),
            pltpu.VMEM((length, heads * HEAD), narrow),
            pltpu.VMEM((n_tp, rows, heads * HEAD), narrow),
            pltpu.VMEM((rows, model), narrow),
            pltpu.VMEM((rows, model), narrow),
            pltpu.VMEM((groups, 8, rows), jnp.float32),
            buffer,
            buffer,
            buffer,
            buffer,
            buffer,
            pltpu.VMEM((groups * rows, model), narrow),
            pltpu.VMEM((groups, 2, rows, rows), narrow),
            pltpu.VMEM((rows, model), jnp.float32),
            buffer,
            buffer,
            pltpu.VMEM((2, rows, model), narrow),
            pltpu.VMEM((2, rows, model), narrow),
            dma((slots,)),
            dma((slots,)),
            dma((slots + 1,)),
            dma((slots + 1,)),
            dma((slots,)),
            dma((slots,)),
            dma((n_tp, HALVES)),
            dma((n_tp, HALVES)),
            dma((groups,)),
            dma((groups,)),
            dma((2, groups, PIECES)),
            dma((groups, PIECES)),
            dma((groups, members)),
            dma((groups, members)),
            dma((groups, PIECES)),
            dma((groups, PIECES)),
            dma((groups, members)),
            dma((groups, members)),
            dma((groups, members)),
            dma((groups, members)),
            dma((groups, PIECES)),
            dma((2, PIECES)),
            dma((2, PIECES)),
            dma((14,)),
        ],
        compiler_params=pltpu.CompilerParams(
            collective_id=1, has_side_effects=True, vmem_limit_bytes=60 * 1024 * 1024
        ),
    )(
        query_proj, key_proj, value_proj, docs,
        query_gain.reshape(1, -1), key_gain.reshape(1, -1), expert_ids, route_weights,
        residual, norm_gain.reshape(1, -1),
        output_weight, gate_weight, up_weight, down_weight,
    )


def rotary_tables(first_row, length):
    freq_count = HEAD // 4
    inverse = 1.0 / rope_base ** (jnp.arange(freq_count, dtype=jnp.float32) / freq_count)
    position = first_row + jnp.arange(length, dtype=jnp.int32)
    grid_row = (position // GRID_W).astype(jnp.float32)
    grid_col = (position % GRID_W).astype(jnp.float32)
    angles = jnp.concatenate(
        [grid_row[:, None] * inverse[None, :], grid_col[:, None] * inverse[None, :]], axis=1
    )
    return (jnp.cos(angles), jnp.sin(angles))


def norm_rotate(projected, gains, cosine, sine_table):
    length = projected.shape[0]
    values_wide = projected.astype(jnp.float32).reshape(length, -1, HEAD)
    scaled = (
        values_wide
        * lax.rsqrt(jnp.mean(values_wide * values_wide, axis=-1, keepdims=True) + norm_eps)
        * gains
    )
    half_size = HEAD // 2
    first_half = scaled[..., :half_size]
    second_half = scaled[..., half_size:]
    cosine_rows = cosine[:, None, :]
    sine_rows = sine_table[:, None, :]
    turned = jnp.concatenate(
        [
            first_half * cosine_rows - second_half * sine_rows,
            first_half * sine_rows + second_half * cosine_rows,
        ],
        axis=-1,
    )
    return turned.reshape(length, -1).astype(jnp.bfloat16)


def attention_kernel(
    n_sp, n_tp, q_ref, k_ref, vt_ref, doc_ref, res_ref, gain_ref, wo_hbm,
    hid_ref, nrm_ref,
    wo_v, k_in, vt_in, doc_in, k_aug, m_s, l_s, acc_s, att_s, all_s,
    send, recv, t_send, t_recv, w_sem,
):
    sp = lax.axis_index("sp")
    tp = lax.axis_index("tp")
    heads = q_ref.shape[0]
    rows = res_ref.shape[0]
    width = att_s.shape[1]
    slots = 2 * REACH

    def distance(j):
        return (j // 2 + 1) * (1 - 2 * (j % 2))

    def inside(index):
        return jnp.logical_and(index >= 0, index < n_sp)

    wo_copy = pltpu.make_async_copy(wo_hbm, wo_v, w_sem)
    wo_copy.start()

    barrier = pltpu.get_barrier_semaphore()
    for j in range(slots):
        there = sp + distance(j)

        @pl.when(inside(there))
        def _():
            pl.semaphore_signal(barrier, inc=1, device_id=(there, tp), device_id_type=MESH)

    for k in range(1, n_tp):
        pl.semaphore_signal(
            barrier, inc=1, device_id=(sp, lax.rem(tp + k, n_tp)), device_id_type=MESH
        )
    beside = jnp.minimum(sp, REACH) + jnp.minimum(n_sp - 1 - sp, REACH)
    pl.semaphore_wait(barrier, n_tp - 1 + beside)

    def copies(j):
        there = (sp + distance(j), tp)
        return [
            pltpu.make_async_remote_copy(
                src_ref=one,
                dst_ref=into.at[j],
                send_sem=send.at[j, i],
                recv_sem=recv.at[j, i],
                device_id=there,
                device_id_type=MESH,
            )
            for i, (one, into) in enumerate(((k_ref, k_in), (vt_ref, vt_in), (doc_ref, doc_in)))
        ]

    for j in range(slots):

        @pl.when(inside(sp + distance(j)))
        def _():
            for copy in copies(j):
                copy.start()

    def take(keys, values_t, docs, first):
        length = keys.shape[0]
        doc_col = jnp.broadcast_to(docs[0:1, :], (HEAD, length)).T
        lanes = lax.broadcasted_iota(jnp.int32, (length, HEAD), 1).astype(jnp.float32)
        k_aug[:, :HEAD] = keys[...]
        k_aug[:, HEAD:] = jnp.where(doc_col == lanes, DOC_KEY, 0.0).astype(jnp.bfloat16)
        for h in range(heads):
            s = jnp.dot(k_aug[...], q_ref[h], preferred_element_type=jnp.float32)
            top = jnp.max(s, axis=0, keepdims=True)
            if not first:
                top = jnp.maximum(m_s[h], top)
            e = jnp.exp2((s - top) * EXP2_SCALE)
            den = jnp.sum(e, axis=0, keepdims=True)
            part = jnp.dot(
                values_t[...], e.astype(jnp.bfloat16), preferred_element_type=jnp.float32
            )
            if first:
                l_s[h] = den
                acc_s[h] = part
            else:
                old = jnp.exp2((m_s[h] - top) * EXP2_SCALE)
                l_s[h] = l_s[h] * old + den
                acc_s[h] = acc_s[h] * old + part
            m_s[h] = top

    take(k_ref, vt_ref, doc_ref, True)

    def step(j, carry):
        @pl.when(inside(sp - distance(j)))
        def _():
            for copy in copies(j):
                copy.wait_recv()
            take(k_in.at[j], vt_in.at[j], doc_in.at[j], False)

        return carry

    lax.fori_loop(0, slots, step, 0)

    for h in range(heads):
        out = acc_s[h] / l_s[h]
        att_s[:, h * HEAD : (h + 1) * HEAD] = out.T.astype(jnp.bfloat16)

    def exchange(k):
        there = lax.rem(tp + k, n_tp)
        return pltpu.make_async_remote_copy(
            src_ref=att_s.at[pl.ds(pl.multiple_of(there * rows, rows), rows), :],
            dst_ref=all_s.at[tp],
            send_sem=t_send.at[k],
            recv_sem=t_recv.at[k],
            device_id=(sp, there),
            device_id_type=MESH,
        )

    for k in range(n_tp - 1, 0, -1):
        exchange(k).start()
    wo_copy.wait()

    def weight_rows(i):
        return wo_v[pl.ds(pl.multiple_of(i * width, width), width), :]

    projected = jnp.dot(
        att_s[pl.ds(pl.multiple_of(tp * rows, rows), rows), :],
        weight_rows(tp),
        preferred_element_type=jnp.float32,
    )
    for k in range(1, n_tp):
        exchange(k).wait_recv()
        source = lax.rem(tp - k + n_tp, n_tp)
        projected += jnp.dot(
            all_s[source], weight_rows(source), preferred_element_type=jnp.float32
        )
    hidden = (res_ref[...].astype(jnp.float32) + projected).astype(jnp.bfloat16)
    hid_ref[...] = hidden
    wide = hidden.astype(jnp.float32)
    mean = jnp.mean(wide * wide, axis=-1, keepdims=True)
    nrm_ref[...] = (wide * lax.rsqrt(mean + norm_eps) * gain_ref[...]).astype(jnp.bfloat16)

    for j in range(slots):

        @pl.when(inside(sp + distance(j)))
        def _():
            for copy in copies(j):
                copy.wait_send()

    for k in range(1, n_tp):
        exchange(k).wait_send()


def attend(q_aug, key_norm, value_t, doc_rows, residual, norm_gain, output_weight):
    n_sp, n_tp = lax.axis_size("sp"), lax.axis_size("tp")
    heads, deep, length = q_aug.shape
    rows, model = residual.shape
    vmem = pl.BlockSpec(memory_space=pltpu.VMEM)
    slots = 2 * REACH
    return pl.pallas_call(
        functools.partial(attention_kernel, n_sp, n_tp),
        out_shape=[jax.ShapeDtypeStruct((rows, model), jnp.bfloat16)] * 2,
        in_specs=[vmem] * 6 + [pl.BlockSpec(memory_space=pl.ANY)],
        out_specs=[vmem] * 2,
        scratch_shapes=[
            pltpu.VMEM(output_weight.shape, jnp.bfloat16),
            pltpu.VMEM((slots,) + key_norm.shape, jnp.bfloat16),
            pltpu.VMEM((slots,) + value_t.shape, jnp.bfloat16),
            pltpu.VMEM((slots,) + doc_rows.shape, jnp.float32),
            pltpu.VMEM((length, deep), jnp.bfloat16),
            pltpu.VMEM((heads, 1, length), jnp.float32),
            pltpu.VMEM((heads, 1, length), jnp.float32),
            pltpu.VMEM((heads, HEAD, length), jnp.float32),
            pltpu.VMEM((length, heads * HEAD), jnp.bfloat16),
            pltpu.VMEM((n_tp, rows, heads * HEAD), jnp.bfloat16),
            pltpu.SemaphoreType.DMA((slots, 3)),
            pltpu.SemaphoreType.DMA((slots, 3)),
            pltpu.SemaphoreType.DMA((n_tp,)),
            pltpu.SemaphoreType.DMA((n_tp,)),
            pltpu.SemaphoreType.DMA(()),
        ],
        compiler_params=pltpu.CompilerParams(
            collective_id=1, has_side_effects=True, vmem_limit_bytes=48 * 1024 * 1024
        ),
    )(q_aug, key_norm, value_t, doc_rows, residual, norm_gain.reshape(1, -1), output_weight)


def plain_on_device(
    residual,
    query_proj,
    key_proj,
    value_proj,
    query_gain,
    key_gain,
    document_ids,
    output_weight,
    norm_gain,
    expert_ids,
    route_weights,
    gate_weight,
    up_weight,
    down_weight,
):
    rows_here = query_proj.shape[0]
    cosine, sine_table = rotary_tables(lax.axis_index("sp") * rows_here, rows_here)
    query_norm = norm_rotate(query_proj, query_gain, cosine, sine_table)
    key_norm = norm_rotate(key_proj, key_gain, cosine, sine_table)
    heads = query_proj.shape[1] // HEAD
    docs = document_ids.astype(jnp.float32)
    query_t = jnp.transpose(query_norm.reshape(rows_here, heads, HEAD), (1, 2, 0))
    query_doc = jnp.where(
        docs[None, :] == jnp.arange(HEAD, dtype=jnp.float32)[:, None], DOC_QUERY, 0.0
    ).astype(jnp.bfloat16)
    q_aug = jnp.concatenate(
        [query_t, jnp.broadcast_to(query_doc[None], (heads, HEAD, rows_here))], axis=1
    )
    doc_rows = jnp.broadcast_to(docs[None, :], (8, rows_here))
    hidden, normed = attend(
        q_aug, key_norm, value_proj.T, doc_rows, residual, norm_gain, output_weight
    )
    token_rows = residual.shape[0]
    top_count = expert_ids.shape[1]
    experts_all = lax.axis_size("sp") * lax.axis_size("tp")
    capacity = max(2, 2 * token_rows * top_count // experts_all)
    flat_ids = expert_ids.reshape(-1)
    order = jnp.arange(flat_ids.shape[0], dtype=jnp.int32)
    earlier = jnp.logical_and(
        flat_ids[:, None] == flat_ids[None, :], order[None, :] < order[:, None]
    )
    arrival = jnp.sum(earlier.astype(jnp.int32), axis=1)
    slot_index = flat_ids * capacity + arrival
    slot_grid = slot_index.reshape(token_rows, top_count)
    placing = jnp.sum(
        (
            jnp.arange(experts_all * capacity, dtype=jnp.int32)[:, None, None] == slot_grid[None]
        ).astype(jnp.float32),
        axis=2,
    ).astype(jnp.bfloat16)
    outgoing = jnp.dot(placing, normed, preferred_element_type=jnp.float32).astype(jnp.bfloat16)
    spread = jnp.sum(
        jnp.where(
            jnp.arange(experts_all * capacity, dtype=jnp.int32)[None, None, :]
            == slot_grid[:, :, None],
            route_weights[:, :, None],
            0.0,
        ),
        axis=1,
    )
    high = spread.astype(jnp.bfloat16)
    low = (spread - high.astype(jnp.float32)).astype(jnp.bfloat16)
    outgoing = outgoing.reshape(experts_all, capacity, normed.shape[1])
    arrived = lax.all_to_all(outgoing, ("sp", "tp"), split_axis=0, concat_axis=0, tiled=True)
    sources, slots, width = arrived.shape
    flat_rows = arrived.reshape(sources * slots, width)
    gate_part = jnp.dot(flat_rows, gate_weight[0], preferred_element_type=jnp.float32)
    up_part = jnp.dot(flat_rows, up_weight[0], preferred_element_type=jnp.float32)
    activity = (jax.nn.silu(gate_part) * up_part).astype(jnp.bfloat16)
    expert_out = jnp.dot(activity, down_weight[0], preferred_element_type=jnp.float32).astype(
        jnp.bfloat16
    )
    returned = lax.all_to_all(
        expert_out.reshape(sources, slots, width),
        ("sp", "tp"),
        split_axis=0,
        concat_axis=0,
        tiled=True,
    )
    rows_back = returned.reshape(experts_all * capacity, -1)
    combined = jnp.dot(high, rows_back, preferred_element_type=jnp.float32) + jnp.dot(
        low, rows_back, preferred_element_type=jnp.float32
    )
    return (hidden.astype(jnp.float32) + combined).astype(jnp.bfloat16)


def on_device(*arrays):
    (
        residual, query_proj, key_proj, value_proj, query_gain, key_gain, document_ids,
        output_weight, norm_gain, expert_ids, route_weights, gate_weight, up_weight, down_weight,
    ) = arrays
    token_rows = residual.shape[0]
    top_count = expert_ids.shape[1]
    experts_all = lax.axis_size("sp") * lax.axis_size("tp")
    capacity = max(2, 2 * token_rows * top_count // experts_all)
    if (
        capacity % 16 == 0
        and token_rows == HEAD
        and token_rows % capacity == 0
        and experts_all % (token_rows // capacity) == 0
        and experts_all * capacity == LINE * token_rows
        and 2 * top_count <= 8
        and lax.axis_size("sp") % 2 == 0
    ):
        return run_layer(
            query_proj, key_proj, value_proj, document_ids.reshape(1, -1), query_gain, key_gain,
            expert_ids.T, route_weights.T, residual, norm_gain, output_weight,
            gate_weight, up_weight, down_weight, capacity,
        )
    return plain_on_device(*arrays)


def solution(mesh):
    in_specs = (
        P(("sp", "tp"), None),
        P("sp", "tp"),
        P("sp", "tp"),
        P("sp", "tp"),
        P(),
        P(),
        P("sp"),
        P(),
        P(),
        P(("sp", "tp"), None),
        P(("sp", "tp"), None),
        P(("sp", "tp"), None, None),
        P(("sp", "tp"), None, None),
        P(("sp", "tp"), None, None),
    )
    out_specs = P(("sp", "tp"), None)
    return jax.shard_map(
        on_device, mesh=mesh, in_specs=in_specs, out_specs=out_specs, check_vma=False
    )
```

```python
import functools
import math

import jax
import jax.numpy as jnp
from jax import lax
from jax.experimental import pallas as pl
from jax.experimental.pallas import tpu as pltpu
from jax.sharding import PartitionSpec as P

HEAD = 128
GRID_W = 64
REACH = 3


norm_eps = 1e-06
rope_base = 10000.0
masked_low = -1e30
MESH = pl.DeviceIdType.MESH
DOC_KEY = 128.0
DOC_QUERY = 64.0
PIECES = 4
ONES = 16
DOC_MARK = 32.0
HALVES = 2
LINE = 4
OFFSETS = (1, -2, 2, -1, 3, -3)
EXP2_SCALE = math.log2(math.e) / math.sqrt(HEAD)


def layer_kernel(
    n_sp, n_tp, capacity, top_count,
    q_hbm, k_hbm, v_hbm, doc_hbm, qg_hbm, kg_hbm, ids_hbm, rw_hbm, res_hbm, gain_hbm,
    wo_hbm, gate_hbm, up_hbm, down_hbm,
    new_ref,
    k_ref, v_ref, kg_ref, doc_ref, q_ref, qg_ref, ids_ref, rw_ref, res_ref, gain_ref,
    wo_v, gate_v, up_v, down_v, cos_s, sin_s, meta_s, q_aug, k_own, k_in, v_in, doc_in,
    k_aug, vt_s, m_s, acc_s, att_s, all_s, hid_s, nrm_s,
    metas, blocks, picked, arrived, answer, homing, returned, spread, total_s,
    back, joined, midway, summed,
    k_send, k_recv, v_send, v_recv, c_send, c_recv, t_send, t_recv,
    m_send, m_recv, z_send, z_recv, d_send, d_recv, h_send, h_recv, r_send, r_recv,
    b_send, b_recv, j_send, y_recv, s_recv, w_sem,
):
    devices = n_sp * n_tp
    rows = res_ref.shape[0]
    members = rows // capacity
    groups = devices // members
    piece = rows // PIECES
    sp = lax.axis_index("sp")
    tp = lax.axis_index("tp")
    me = sp * n_tp + tp
    plane = lax.div(me, members)
    pos = lax.rem(me, members)

    fetches = [
        pltpu.make_async_copy(source, into, w_sem.at[i])
        for i, (source, into) in enumerate(
            (
                (kg_hbm, kg_ref), (k_hbm, k_ref), (v_hbm, v_ref), (doc_hbm, doc_ref),
                (ids_hbm, ids_ref), (rw_hbm, rw_ref), (qg_hbm, qg_ref), (q_hbm, q_ref),
                (wo_hbm, wo_v), (res_hbm, res_ref), (gain_hbm, gain_ref),
                (gate_hbm.at[0], gate_v), (up_hbm.at[0], up_v), (down_hbm.at[0], down_v),
            )
        )
    ]
    for fetch in fetches:
        fetch.start()

    def fetched(*which):
        for i in which:
            fetches[i].wait()

    def place(device):
        return (lax.div(device, n_tp), lax.rem(device, n_tp))

    def region(index):
        return pl.ds(pl.multiple_of(index * capacity, capacity), capacity)

    length = k_ref.shape[0]
    heads = q_ref.shape[1] // HEAD
    width = att_s.shape[1]
    slots = len(OFFSETS)
    half = HEAD // 2
    side = 1 - 2 * lax.rem(sp, 2)
    across, ahead, behind = sp + side, sp + 2 * side, sp - 2 * side

    def inside(index):
        return jnp.logical_and(index >= 0, index < n_sp)

    has_ahead, has_behind = inside(ahead), inside(behind)
    has_spare = inside(sp + 4 * side)

    def offset(j):
        return sum(jnp.where(j == i, o, 0) for i, o in enumerate(OFFSETS))

    def exists(j):
        return inside(sp + side * offset(j))

    def reader(j):
        odd = OFFSETS[j] % 2 == 1
        return sp + side * OFFSETS[j] if odd else sp - side * OFFSETS[j]

    barrier = pltpu.get_barrier_semaphore()

    def greet(i, carry):
        there = lax.rem(me + i, devices)
        pl.semaphore_signal(barrier, inc=1, device_id=place(there), device_id_type=MESH)
        return carry

    lax.fori_loop(1, devices, greet, 0)

    def column(row):
        return jnp.broadcast_to(row, (HEAD, HEAD)).T[:, :1]

    freq_count = HEAD // 4
    exponent = lax.broadcasted_iota(jnp.int32, (freq_count, 1), 0).astype(jnp.float32) / freq_count
    inverse = jnp.exp2(exponent * -math.log2(rope_base))
    position = sp * length + lax.broadcasted_iota(jnp.int32, (1, length), 1)
    grid_row = lax.div(position, GRID_W).astype(jnp.float32)
    grid_col = lax.rem(position, GRID_W).astype(jnp.float32)
    angles = jnp.concatenate([inverse * grid_row, inverse * grid_col], axis=0)
    cos_s[...] = jnp.cos(angles)
    sin_s[...] = jnp.sin(angles)

    def turned(projected, gains):
        wide = projected.astype(jnp.float32).T
        scaled = (
            wide * lax.rsqrt(jnp.mean(wide * wide, axis=0, keepdims=True) + norm_eps) * gains
        )
        upper, lower = scaled[:half], scaled[half:]
        cosine, sine = cos_s[...], sin_s[...]
        return jnp.concatenate(
            [upper * cosine - lower * sine, upper * sine + lower * cosine], axis=0
        )

    fetched(0, 1)
    k_own[...] = turned(k_ref[...], column(kg_ref[...])).T.astype(jnp.bfloat16)
    fetched(2, 3, 4, 5)
    for k in range(top_count):
        for r, table in ((k, ids_ref), (top_count + k, rw_ref)):
            meta_s[r : r + 1, :] = table[k : k + 1, :].astype(jnp.float32)
    pl.semaphore_wait(barrier, devices - 1)

    def tell(i, block):
        return pltpu.make_async_remote_copy(
            src_ref=meta_s,
            dst_ref=metas.at[block],
            send_sem=m_send.at[i],
            recv_sem=m_recv.at[block],
            device_id=place(lax.rem(plane + i, groups) * members + pos),
            device_id_type=MESH,
        )

    def shift(source, into, sends, receives, i, there):
        return pltpu.make_async_remote_copy(
            src_ref=source,
            dst_ref=into.at[i],
            send_sem=sends.at[i],
            recv_sem=receives.at[i],
            device_id=(there, tp),
            device_id_type=MESH,
        )

    key_plan = (
        (k_own, across, True),
        (k_own, ahead, has_ahead),
        (k_own, behind, has_behind),
        (k_in.at[0], ahead, has_ahead),
        (k_in.at[0], behind, has_behind),
        (k_in.at[3], ahead, jnp.logical_and(has_ahead, has_behind)),
    )
    value_plan = (
        (v_ref, across, True),
        (v_ref, ahead, has_ahead),
        (v_ref, behind, has_behind),
        (v_in.at[2], across, has_ahead),
        (v_in.at[1], across, has_behind),
        (v_in.at[6], across, has_spare),
        (v_in.at[2], behind, jnp.logical_and(has_ahead, has_behind)),
    )

    def key_shift(i):
        return shift(key_plan[i][0], k_in, k_send, k_recv, i, key_plan[i][1])

    def value_shift(i):
        return shift(value_plan[i][0], v_in, v_send, v_recv, i, value_plan[i][1])

    def on(allowed, act):
        if allowed is True:
            act()
        elif allowed is not False:
            pl.when(allowed)(act)

    def start_keys(*which):
        for i in which:
            on(key_plan[i][2], lambda: key_shift(i).start())

    def start_values(*which):
        for i in which:
            on(value_plan[i][2], lambda: value_shift(i).start())

    def key_wait(j):
        shift(k_own, k_in, k_send, k_recv, j, sp).wait_recv()

    def value_wait(j):
        shift(v_ref, v_in, v_send, v_recv, j, sp).wait_recv()

    def doc_shift(j):
        return shift(doc_ref, doc_in, c_send, c_recv, j, reader(j))

    for j in range(slots):
        pl.when(inside(reader(j)))(lambda: doc_shift(j).start())
    start_keys(0, 1, 2)
    start_values(0, 1, 2)
    for i in range(1, groups):
        tell(i, plane).start()

    fetched(6, 7)
    query_gains = column(qg_ref[...]) * EXP2_SCALE
    for h in range(heads):
        q_aug[h, :HEAD, :] = turned(
            q_ref[:, h * HEAD : (h + 1) * HEAD], query_gains
        ).astype(jnp.bfloat16)
        labels = lax.broadcasted_iota(jnp.int32, (HEAD, length), 0)
        q_aug[h, HEAD:, :] = jnp.where(doc_ref[...] == labels, DOC_MARK, 0.0).astype(
            jnp.bfloat16
        )

    def take(keys, values, docs, first):
        doc_col = jnp.broadcast_to(docs[...].astype(jnp.float32), (HEAD, length)).T
        lanes = lax.broadcasted_iota(jnp.int32, (length, HEAD), 1).astype(jnp.float32)
        k_aug[:, :HEAD] = keys[...]
        k_aug[:, HEAD:] = jnp.where(doc_col == lanes, DOC_MARK, 0.0).astype(jnp.bfloat16)
        vt_s[:HEAD, :] = values[...].T
        for h in range(heads):
            s = jnp.dot(k_aug[...], q_aug[h], preferred_element_type=jnp.float32)
            top = jnp.max(s, axis=0, keepdims=True)
            if not first:
                top = jnp.maximum(m_s[h], top)
            e = jnp.exp2(s - top).astype(jnp.bfloat16)
            part = jnp.dot(vt_s[...], e, preferred_element_type=jnp.float32)
            acc_s[h] = part if first else acc_s[h] * jnp.exp2(m_s[h] - top) + part
            m_s[h] = top

    vt_s[HEAD:, :] = jnp.ones((ONES, length), jnp.bfloat16)
    take(k_own, v_ref, doc_ref, True)

    key_wait(0)
    start_keys(3, 4)

    @pl.when(has_ahead)
    def _():
        value_wait(2)
        start_values(3, 6)

    @pl.when(has_behind)
    def _():
        value_wait(1)
        start_values(4)

    def step(j, carry):
        @pl.when(exists(j))
        def _():
            @pl.when(jnp.logical_and(j != 0, j != 3))
            def _():
                key_wait(j)

            @pl.when(jnp.logical_and(j != 1, j != 2))
            def _():
                value_wait(j)

            shift(doc_ref, doc_in, c_send, c_recv, j, sp).wait_recv()
            take(k_in.at[j], v_in.at[j], doc_in.at[j], False)

        @pl.when(jnp.logical_and(j == 1, has_behind))
        def _():
            key_wait(3)
            start_keys(5)

        @pl.when(jnp.logical_and(j == 2, has_spare))
        def _():
            value_wait(6)
            start_values(5)

        return carry

    lax.fori_loop(0, slots, step, 0)

    for h in range(heads):
        out = acc_s[h, :HEAD, :] / acc_s[h, HEAD : HEAD + 1, :]
        att_s[:, h * HEAD : (h + 1) * HEAD] = out.T.astype(jnp.bfloat16)

    part_rows = rows // HALVES

    def exchange(k, half):
        there = lax.rem(tp + k, n_tp)
        here = pl.ds(pl.multiple_of(there * rows + half * part_rows, part_rows), part_rows)
        return pltpu.make_async_remote_copy(
            src_ref=att_s.at[here, :],
            dst_ref=all_s.at[tp, pl.ds(half * part_rows, part_rows)],
            send_sem=t_send.at[k, half],
            recv_sem=t_recv.at[k, half],
            device_id=(sp, there),
            device_id_type=MESH,
        )

    for half in range(HALVES):
        for k in range(n_tp - 1, 0, -1):
            exchange(k, half).start()
    fetched(8, 9, 10)

    def weight_rows(i):
        return wo_v[pl.ds(pl.multiple_of(i * width, width), width), :]

    total_s[...] = res_ref[...].astype(jnp.float32) + jnp.dot(
        att_s[pl.ds(pl.multiple_of(tp * rows, rows), rows), :],
        weight_rows(tp),
        preferred_element_type=jnp.float32,
    )

    def project(half):
        part = pl.ds(half * part_rows, part_rows)
        projected = total_s[part, :]
        for k in range(1, n_tp):
            exchange(k, half).wait_recv()
            source = lax.rem(tp - k + n_tp, n_tp)
            projected += jnp.dot(
                all_s[source, part, :], weight_rows(source), preferred_element_type=jnp.float32
            )
        hidden = projected.astype(jnp.bfloat16)
        hid_s[part, :] = hidden
        wide = hidden.astype(jnp.float32)
        mean = jnp.mean(wide * wide, axis=-1, keepdims=True)
        nrm_s[part, :] = (wide * lax.rsqrt(mean + norm_eps) * gain_ref[...]).astype(jnp.bfloat16)

    def pass_on(source, block, way, c):
        part = pl.ds(c * piece, piece)
        return pltpu.make_async_remote_copy(
            src_ref=source.at[part],
            dst_ref=blocks.at[block, part],
            send_sem=z_send.at[way, block, c],
            recv_sem=z_recv.at[block, c],
            device_id=place(me + (2 * way - 1) * members),
            device_id_type=MESH,
        )

    def dispatch(block, peer, landing):
        return pltpu.make_async_remote_copy(
            src_ref=picked.at[block, region(peer)],
            dst_ref=arrived.at[block, region(landing)],
            send_sem=d_send.at[block, peer],
            recv_sem=d_recv.at[block, landing],
            device_id=place(plane * members + peer),
            device_id_type=MESH,
        )

    def give_home(block, origin, c):
        part = pl.ds(c * piece, piece)
        return pltpu.make_async_remote_copy(
            src_ref=answer.at[block, part],
            dst_ref=homing.at[origin, part],
            send_sem=h_send.at[block, c],
            recv_sem=h_recv.at[origin, c],
            device_id=place(block * members + pos),
            device_id_type=MESH,
        )

    def give_back(source, origin, member, landing):
        return pltpu.make_async_remote_copy(
            src_ref=source.at[region(member)],
            dst_ref=returned.at[region(origin * members + landing)],
            send_sem=r_send.at[origin, member],
            recv_sem=r_recv.at[origin, landing],
            device_id=place(plane * members + member),
            device_id_type=MESH,
        )

    def give_across(block, member, landing):
        return pltpu.make_async_remote_copy(
            src_ref=answer.at[block, region(member)],
            dst_ref=back.at[block, region(landing)],
            send_sem=b_send.at[block, member],
            recv_sem=b_recv.at[block, landing],
            device_id=place(plane * members + member),
            device_id_type=MESH,
        )

    def give_next(block, way, c):
        part = pl.ds(c * piece, piece)
        return pltpu.make_async_remote_copy(
            src_ref=joined.at[block, part],
            dst_ref=midway.at[way, part],
            send_sem=j_send.at[block, c],
            recv_sem=y_recv.at[way, c],
            device_id=place(me + (1 - 2 * way) * members),
            device_id_type=MESH,
        )

    def give_sum(block, way, c):
        part = pl.ds(c * piece, piece)
        return pltpu.make_async_remote_copy(
            src_ref=joined.at[block, part],
            dst_ref=summed.at[way, part],
            send_sem=j_send.at[block, c],
            recv_sem=s_recv.at[way, c],
            device_id=place(block * members + pos),
            device_id_type=MESH,
        )

    def others(act, first=1):
        def one(i, carry):
            act(lax.rem(pos + i, members))
            return carry

        lax.fori_loop(first, members, one, 0)

    low_side = plane < groups // 2
    toward = jnp.where(low_side, 1, -1)
    seen = jnp.where(low_side, 0, 1)
    inward, outward = 1 - seen, seen
    is_end = jnp.logical_or(plane == 0, plane == groups - 1)
    is_inner = jnp.logical_not(is_end)
    first = jnp.where(is_end, plane + toward, plane - toward)
    second = jnp.where(is_end, plane + 3 * toward, plane + 2 * toward)
    third = jnp.where(is_end, plane + 2 * toward, plane + toward)
    early, late = range(PIECES // 2), range(PIECES // 2, PIECES)

    def push(source, block, way, which):
        for c in which:
            pass_on(source, block, way, c).start()

    def landed(block, which):
        for c in which:
            pass_on(nrm_s, block, 0, c).wait_recv()

    def hop(block, way, which):
        for c in which:
            landed(block, (c,))
            push(blocks.at[block], block, way, (c,))

    for half in range(HALVES):
        project(half)
        ready = range(half * PIECES // HALVES, (half + 1) * PIECES // HALVES)

        @pl.when(is_end)
        def _():
            push(nrm_s, plane, inward, ready)

        @pl.when(is_inner)
        def _():
            for c in ready:
                push(nrm_s, plane, outward, (c,))
                if c in early:
                    push(nrm_s, plane, inward, (c,))

    def slot_rows(meta):
        experts = lax.broadcasted_iota(jnp.int32, (devices, rows), 0).astype(jnp.float32)
        hits = [experts == meta[k : k + 1, :] for k in range(top_count)]
        named = sum(hit.astype(jnp.float32) for hit in hits)
        ahead = (
            lax.broadcasted_iota(jnp.int32, (rows, rows), 0)
            < lax.broadcasted_iota(jnp.int32, (rows, rows), 1)
        )
        before = jnp.dot(
            named.astype(jnp.bfloat16),
            ahead.astype(jnp.float32).astype(jnp.bfloat16),
            preferred_element_type=jnp.float32,
        )
        return [
            meta[k : k + 1, :] * capacity
            + jnp.sum(jnp.where(hits[k], before, 0.0), axis=0, keepdims=True)
            for k in range(top_count)
        ]

    def slot_numbers(group):
        return (
            lax.broadcasted_iota(jnp.int32, (rows, rows), 0) + group * rows
        ).astype(jnp.float32)

    def gather(source, meta, block):
        numbers = slot_numbers(plane)
        choice = sum((numbers == row).astype(jnp.float32) for row in slot_rows(meta))
        picked[block] = jnp.dot(
            choice.astype(jnp.bfloat16), source[...], preferred_element_type=jnp.float32
        ).astype(jnp.bfloat16)
        others(lambda peer: dispatch(block, peer, pos).start())
        arrived[block, region(pos), :] = picked[block, region(pos), :]

    def expert(block):
        others(lambda peer: dispatch(block, peer, peer).wait_recv())
        x = arrived[block]
        gate_part = jnp.dot(x, gate_v[...], preferred_element_type=jnp.float32)
        up_part = jnp.dot(x, up_v[...], preferred_element_type=jnp.float32)
        activity = (jax.nn.silu(gate_part) * up_part).astype(jnp.bfloat16)
        answer[block] = jnp.dot(
            activity, down_v[...], preferred_element_type=jnp.float32
        ).astype(jnp.bfloat16)

    gather(nrm_s, meta_s[...], plane)
    own_slots = slot_rows(meta_s[...])
    for g in range(groups):
        numbers = slot_numbers(g)
        weights = sum(
            jnp.where(numbers == own_slots[k], meta_s[top_count + k : top_count + k + 1, :], 0.0)
            for k in range(top_count)
        ).T
        high = weights.astype(jnp.bfloat16)
        spread[g, 0] = high
        spread[g, 1] = (weights - high.astype(jnp.float32)).astype(jnp.bfloat16)
    fetched(11, 12, 13)

    def collect(block):
        tell(1, block).wait_recv()
        gather(blocks.at[block], metas[block], block)

    def serve_home(block):
        expert(block)
        for c in range(PIECES):
            give_home(block, plane, c).start()

    def serve_across(block):
        expert(block)
        others(lambda member: give_across(block, member, pos).start())
        back[block, region(pos), :] = answer[block, region(pos), :]

    def join(block):
        others(lambda member: give_across(block, member, member).wait_recv())
        meta = metas[block]
        numbers = slot_numbers(plane)
        lines = slot_rows(meta)
        weights = sum(
            jnp.where(numbers == lines[k], meta[top_count + k : top_count + k + 1, :], 0.0)
            for k in range(top_count)
        ).T
        high = weights.astype(jnp.bfloat16)
        low = (weights - high.astype(jnp.float32)).astype(jnp.bfloat16)
        joined[block] = (
            jnp.dot(high, back[block], preferred_element_type=jnp.float32)
            + jnp.dot(low, back[block], preferred_element_type=jnp.float32)
        ).astype(jnp.bfloat16)

    def share(origin):
        for c in range(PIECES):
            give_home(origin, origin, c).wait_recv()
            for i in range(c * members // PIECES, (c + 1) * members // PIECES):

                @pl.when(pos != i)
                def _():
                    give_back(homing.at[origin], origin, i, pos).start()

        returned[region(origin * members + pos), :] = homing[origin, region(pos), :]

    @pl.when(is_inner)
    def _():
        hop(first, inward, range(PIECES - 1))
        hop(second, outward, (0,))
        hop(first, inward, (PIECES - 1,))
        push(nrm_s, plane, inward, late)
        hop(second, outward, (1,))

    @pl.when(is_end)
    def _():
        landed(first, range(PIECES))

    collect(first)
    expert(plane)
    others(lambda member: give_back(answer.at[plane], plane, member, pos).start())
    returned[region(me), :] = answer[plane, region(pos), :]

    @pl.when(is_inner)
    def _():
        hop(second, outward, range(2, PIECES))
        hop(third, outward, early)

    @pl.when(is_end)
    def _():
        landed(second, range(PIECES))

    collect(second)
    serve_home(first)

    @pl.when(is_end)
    def _():
        serve_across(second)
        landed(third, range(PIECES))
        join(second)
        for c in range(PIECES):
            give_next(second, seen, c).start()

    @pl.when(is_inner)
    def _():
        hop(third, outward, late)

    collect(third)

    @pl.when(is_inner)
    def _():
        serve_across(second)

    serve_home(third)
    share(first)

    @pl.when(is_inner)
    def _():
        join(second)
        for c in range(PIECES):
            part = pl.ds(c * piece, piece)
            give_next(second, seen, c).wait_recv()
            joined[second, part, :] = (
                joined[second, part, :].astype(jnp.float32)
                + midway[seen, part, :].astype(jnp.float32)
            ).astype(jnp.bfloat16)
            give_sum(second, seen, c).start()
        share(third)
        share(second)

    total = hid_s[...].astype(jnp.float32)

    def combine(group):
        back = returned[pl.ds(pl.multiple_of(group * rows, rows), rows), :]
        part = jnp.dot(spread[group, 0], back, preferred_element_type=jnp.float32)
        return part + jnp.dot(spread[group, 1], back, preferred_element_type=jnp.float32)

    def gathered(origin):
        others(lambda member: give_back(homing.at[origin], origin, member, member).wait_recv())
        return combine(origin)

    total_s[...] = total + gathered(plane) + gathered(first)

    @pl.when(is_inner)
    def _():
        total_s[...] += gathered(third)
        total_s[...] += gathered(second)

    @pl.when(is_end)
    def _():
        for c in range(PIECES):
            give_sum(third, 1 - seen, c).wait_recv()
        total_s[...] += summed[1 - seen].astype(jnp.float32)

    new_ref[...] = total_s[...].astype(jnp.bfloat16)

    for i in range(1, groups):
        tell(i, plane).wait_send()

    def gone(block, way):
        for c in range(PIECES):
            pass_on(nrm_s, block, way, c).wait_send()

    gone(plane, inward)

    @pl.when(is_inner)
    def _():
        gone(plane, outward)
        gone(first, inward)
        gone(second, outward)
        gone(third, outward)

    others(lambda peer: dispatch(plane, peer, pos).wait_send())
    others(lambda member: give_back(answer.at[plane], plane, member, pos).wait_send())
    for block in (first, second, third):
        others(lambda peer: dispatch(block, peer, pos).wait_send())
    for block in (first, third):
        for c in range(PIECES):
            give_home(block, plane, c).wait_send()
    others(lambda member: give_across(second, member, pos).wait_send())
    for c in range(PIECES):
        give_next(second, seen, c).wait_send()
    others(lambda member: give_back(homing.at[first], first, member, pos).wait_send())

    @pl.when(is_inner)
    def _():
        for block in (second, third):
            others(lambda member: give_back(homing.at[block], block, member, pos).wait_send())

    for i in range(slots):
        on(key_plan[i][2], lambda: key_shift(i).wait_send())
        pl.when(inside(reader(i)))(lambda: doc_shift(i).wait_send())
    for i in range(slots + 1):
        on(value_plan[i][2], lambda: value_shift(i).wait_send())
    for k in range(1, n_tp):
        for half in range(HALVES):
            exchange(k, half).wait_send()


def run_layer(
    query_proj, key_proj, value_proj, docs, query_gain, key_gain, expert_ids, route_weights,
    residual, norm_gain, output_weight, gate_weight, up_weight, down_weight, capacity,
):
    n_sp, n_tp = lax.axis_size("sp"), lax.axis_size("tp")
    length = key_proj.shape[0]
    heads = query_proj.shape[1] // HEAD
    rows, model = residual.shape
    top_count = expert_ids.shape[0]
    members = rows // capacity
    groups = n_sp * n_tp // members
    slots = len(OFFSETS)
    block = (length, HEAD)
    narrow = jnp.bfloat16
    vmem = pl.BlockSpec(memory_space=pltpu.VMEM)
    buffer = pltpu.VMEM((groups, rows, model), narrow)
    dma = pltpu.SemaphoreType.DMA
    return pl.pallas_call(
        functools.partial(layer_kernel, n_sp, n_tp, capacity, top_count),
        out_shape=jax.ShapeDtypeStruct(residual.shape, narrow),
        in_specs=[pl.BlockSpec(memory_space=pltpu.HBM)] * 14,
        out_specs=vmem,
        scratch_shapes=[
            pltpu.VMEM(block, narrow),
            pltpu.VMEM(block, narrow),
            pltpu.VMEM((1, HEAD), jnp.float32),
            pltpu.VMEM(docs.shape, jnp.int32),
            pltpu.VMEM(query_proj.shape, narrow),
            pltpu.VMEM((1, HEAD), jnp.float32),
            pltpu.VMEM(expert_ids.shape, jnp.int32),
            pltpu.VMEM(route_weights.shape, jnp.float32),
            pltpu.VMEM(residual.shape, narrow),
            pltpu.VMEM((1, model), jnp.float32),
            pltpu.VMEM(output_weight.shape, narrow),
            pltpu.VMEM(gate_weight.shape[1:], narrow),
            pltpu.VMEM(up_weight.shape[1:], narrow),
            pltpu.VMEM(down_weight.shape[1:], narrow),
            pltpu.VMEM((HEAD // 2, length), jnp.float32),
            pltpu.VMEM((HEAD // 2, length), jnp.float32),
            pltpu.VMEM((8, rows), jnp.float32),
            pltpu.VMEM((heads, 2 * HEAD, length), narrow),
            pltpu.VMEM(block, narrow),
            pltpu.VMEM((slots,) + block, narrow),
            pltpu.VMEM((slots + 1,) + block, narrow),
            pltpu.VMEM((slots,) + docs.shape, jnp.int32),
            pltpu.VMEM((length, 2 * HEAD), narrow),
            pltpu.VMEM((HEAD + ONES, length), narrow),
            pltpu.VMEM((heads, 1, length), jnp.float32),
            pltpu.VMEM((heads, HEAD + ONES, length), jnp.float32),
            pltpu.VMEM((length, heads * HEAD), narrow),
            pltpu.VMEM((n_tp, rows, heads * HEAD), narrow),
            pltpu.VMEM((rows, model), narrow),
            pltpu.VMEM((rows, model), narrow),
            pltpu.VMEM((groups, 8, rows), jnp.float32),
            buffer,
            buffer,
            buffer,
            buffer,
            buffer,
            pltpu.VMEM((groups * rows, model), narrow),
            pltpu.VMEM((groups, 2, rows, rows), narrow),
            pltpu.VMEM((rows, model), jnp.float32),
            buffer,
            buffer,
            pltpu.VMEM((2, rows, model), narrow),
            pltpu.VMEM((2, rows, model), narrow),
            dma((slots,)),
            dma((slots,)),
            dma((slots + 1,)),
            dma((slots + 1,)),
            dma((slots,)),
            dma((slots,)),
            dma((n_tp, HALVES)),
            dma((n_tp, HALVES)),
            dma((groups,)),
            dma((groups,)),
            dma((2, groups, PIECES)),
            dma((groups, PIECES)),
            dma((groups, members)),
            dma((groups, members)),
            dma((groups, PIECES)),
            dma((groups, PIECES)),
            dma((groups, members)),
            dma((groups, members)),
            dma((groups, members)),
            dma((groups, members)),
            dma((groups, PIECES)),
            dma((2, PIECES)),
            dma((2, PIECES)),
            dma((14,)),
        ],
        compiler_params=pltpu.CompilerParams(
            collective_id=1, has_side_effects=True, vmem_limit_bytes=60 * 1024 * 1024
        ),
    )(
        query_proj, key_proj, value_proj, docs,
        query_gain.reshape(1, -1), key_gain.reshape(1, -1), expert_ids, route_weights,
        residual, norm_gain.reshape(1, -1),
        output_weight, gate_weight, up_weight, down_weight,
    )


def rotary_tables(first_row, length):
    freq_count = HEAD // 4
    inverse = 1.0 / rope_base ** (jnp.arange(freq_count, dtype=jnp.float32) / freq_count)
    position = first_row + jnp.arange(length, dtype=jnp.int32)
    grid_row = (position // GRID_W).astype(jnp.float32)
    grid_col = (position % GRID_W).astype(jnp.float32)
    angles = jnp.concatenate(
        [grid_row[:, None] * inverse[None, :], grid_col[:, None] * inverse[None, :]], axis=1
    )
    return (jnp.cos(angles), jnp.sin(angles))


def norm_rotate(projected, gains, cosine, sine_table):
    length = projected.shape[0]
    values_wide = projected.astype(jnp.float32).reshape(length, -1, HEAD)
    scaled = (
        values_wide
        * lax.rsqrt(jnp.mean(values_wide * values_wide, axis=-1, keepdims=True) + norm_eps)
        * gains
    )
    half_size = HEAD // 2
    first_half = scaled[..., :half_size]
    second_half = scaled[..., half_size:]
    cosine_rows = cosine[:, None, :]
    sine_rows = sine_table[:, None, :]
    turned = jnp.concatenate(
        [
            first_half * cosine_rows - second_half * sine_rows,
            first_half * sine_rows + second_half * cosine_rows,
        ],
        axis=-1,
    )
    return turned.reshape(length, -1).astype(jnp.bfloat16)


def attention_kernel(
    n_sp, n_tp, q_ref, k_ref, vt_ref, doc_ref, res_ref, gain_ref, wo_hbm,
    hid_ref, nrm_ref,
    wo_v, k_in, vt_in, doc_in, k_aug, m_s, l_s, acc_s, att_s, all_s,
    send, recv, t_send, t_recv, w_sem,
):
    sp = lax.axis_index("sp")
    tp = lax.axis_index("tp")
    heads = q_ref.shape[0]
    rows = res_ref.shape[0]
    width = att_s.shape[1]
    slots = 2 * REACH

    def distance(j):
        return (j // 2 + 1) * (1 - 2 * (j % 2))

    def inside(index):
        return jnp.logical_and(index >= 0, index < n_sp)

    wo_copy = pltpu.make_async_copy(wo_hbm, wo_v, w_sem)
    wo_copy.start()

    barrier = pltpu.get_barrier_semaphore()
    for j in range(slots):
        there = sp + distance(j)

        @pl.when(inside(there))
        def _():
            pl.semaphore_signal(barrier, inc=1, device_id=(there, tp), device_id_type=MESH)

    for k in range(1, n_tp):
        pl.semaphore_signal(
            barrier, inc=1, device_id=(sp, lax.rem(tp + k, n_tp)), device_id_type=MESH
        )
    beside = jnp.minimum(sp, REACH) + jnp.minimum(n_sp - 1 - sp, REACH)
    pl.semaphore_wait(barrier, n_tp - 1 + beside)

    def copies(j):
        there = (sp + distance(j), tp)
        return [
            pltpu.make_async_remote_copy(
                src_ref=one,
                dst_ref=into.at[j],
                send_sem=send.at[j, i],
                recv_sem=recv.at[j, i],
                device_id=there,
                device_id_type=MESH,
            )
            for i, (one, into) in enumerate(((k_ref, k_in), (vt_ref, vt_in), (doc_ref, doc_in)))
        ]

    for j in range(slots):

        @pl.when(inside(sp + distance(j)))
        def _():
            for copy in copies(j):
                copy.start()

    def take(keys, values_t, docs, first):
        length = keys.shape[0]
        doc_col = jnp.broadcast_to(docs[0:1, :], (HEAD, length)).T
        lanes = lax.broadcasted_iota(jnp.int32, (length, HEAD), 1).astype(jnp.float32)
        k_aug[:, :HEAD] = keys[...]
        k_aug[:, HEAD:] = jnp.where(doc_col == lanes, DOC_KEY, 0.0).astype(jnp.bfloat16)
        for h in range(heads):
            s = jnp.dot(k_aug[...], q_ref[h], preferred_element_type=jnp.float32)
            top = jnp.max(s, axis=0, keepdims=True)
            if not first:
                top = jnp.maximum(m_s[h], top)
            e = jnp.exp2((s - top) * EXP2_SCALE)
            den = jnp.sum(e, axis=0, keepdims=True)
            part = jnp.dot(
                values_t[...], e.astype(jnp.bfloat16), preferred_element_type=jnp.float32
            )
            if first:
                l_s[h] = den
                acc_s[h] = part
            else:
                old = jnp.exp2((m_s[h] - top) * EXP2_SCALE)
                l_s[h] = l_s[h] * old + den
                acc_s[h] = acc_s[h] * old + part
            m_s[h] = top

    take(k_ref, vt_ref, doc_ref, True)

    def step(j, carry):
        @pl.when(inside(sp - distance(j)))
        def _():
            for copy in copies(j):
                copy.wait_recv()
            take(k_in.at[j], vt_in.at[j], doc_in.at[j], False)

        return carry

    lax.fori_loop(0, slots, step, 0)

    for h in range(heads):
        out = acc_s[h] / l_s[h]
        att_s[:, h * HEAD : (h + 1) * HEAD] = out.T.astype(jnp.bfloat16)

    def exchange(k):
        there = lax.rem(tp + k, n_tp)
        return pltpu.make_async_remote_copy(
            src_ref=att_s.at[pl.ds(pl.multiple_of(there * rows, rows), rows), :],
            dst_ref=all_s.at[tp],
            send_sem=t_send.at[k],
            recv_sem=t_recv.at[k],
            device_id=(sp, there),
            device_id_type=MESH,
        )

    for k in range(n_tp - 1, 0, -1):
        exchange(k).start()
    wo_copy.wait()

    def weight_rows(i):
        return wo_v[pl.ds(pl.multiple_of(i * width, width), width), :]

    projected = jnp.dot(
        att_s[pl.ds(pl.multiple_of(tp * rows, rows), rows), :],
        weight_rows(tp),
        preferred_element_type=jnp.float32,
    )
    for k in range(1, n_tp):
        exchange(k).wait_recv()
        source = lax.rem(tp - k + n_tp, n_tp)
        projected += jnp.dot(
            all_s[source], weight_rows(source), preferred_element_type=jnp.float32
        )
    hidden = (res_ref[...].astype(jnp.float32) + projected).astype(jnp.bfloat16)
    hid_ref[...] = hidden
    wide = hidden.astype(jnp.float32)
    mean = jnp.mean(wide * wide, axis=-1, keepdims=True)
    nrm_ref[...] = (wide * lax.rsqrt(mean + norm_eps) * gain_ref[...]).astype(jnp.bfloat16)

    for j in range(slots):

        @pl.when(inside(sp + distance(j)))
        def _():
            for copy in copies(j):
                copy.wait_send()

    for k in range(1, n_tp):
        exchange(k).wait_send()


def attend(q_aug, key_norm, value_t, doc_rows, residual, norm_gain, output_weight):
    n_sp, n_tp = lax.axis_size("sp"), lax.axis_size("tp")
    heads, deep, length = q_aug.shape
    rows, model = residual.shape
    vmem = pl.BlockSpec(memory_space=pltpu.VMEM)
    slots = 2 * REACH
    return pl.pallas_call(
        functools.partial(attention_kernel, n_sp, n_tp),
        out_shape=[jax.ShapeDtypeStruct((rows, model), jnp.bfloat16)] * 2,
        in_specs=[vmem] * 6 + [pl.BlockSpec(memory_space=pl.ANY)],
        out_specs=[vmem] * 2,
        scratch_shapes=[
            pltpu.VMEM(output_weight.shape, jnp.bfloat16),
            pltpu.VMEM((slots,) + key_norm.shape, jnp.bfloat16),
            pltpu.VMEM((slots,) + value_t.shape, jnp.bfloat16),
            pltpu.VMEM((slots,) + doc_rows.shape, jnp.float32),
            pltpu.VMEM((length, deep), jnp.bfloat16),
            pltpu.VMEM((heads, 1, length), jnp.float32),
            pltpu.VMEM((heads, 1, length), jnp.float32),
            pltpu.VMEM((heads, HEAD, length), jnp.float32),
            pltpu.VMEM((length, heads * HEAD), jnp.bfloat16),
            pltpu.VMEM((n_tp, rows, heads * HEAD), jnp.bfloat16),
            pltpu.SemaphoreType.DMA((slots, 3)),
            pltpu.SemaphoreType.DMA((slots, 3)),
            pltpu.SemaphoreType.DMA((n_tp,)),
            pltpu.SemaphoreType.DMA((n_tp,)),
            pltpu.SemaphoreType.DMA(()),
        ],
        compiler_params=pltpu.CompilerParams(
            collective_id=1, has_side_effects=True, vmem_limit_bytes=48 * 1024 * 1024
        ),
    )(q_aug, key_norm, value_t, doc_rows, residual, norm_gain.reshape(1, -1), output_weight)


def plain_on_device(
    residual,
    query_proj,
    key_proj,
    value_proj,
    query_gain,
    key_gain,
    document_ids,
    output_weight,
    norm_gain,
    expert_ids,
    route_weights,
    gate_weight,
    up_weight,
    down_weight,
):
    rows_here = query_proj.shape[0]
    cosine, sine_table = rotary_tables(lax.axis_index("sp") * rows_here, rows_here)
    query_norm = norm_rotate(query_proj, query_gain, cosine, sine_table)
    key_norm = norm_rotate(key_proj, key_gain, cosine, sine_table)
    heads = query_proj.shape[1] // HEAD
    docs = document_ids.astype(jnp.float32)
    query_t = jnp.transpose(query_norm.reshape(rows_here, heads, HEAD), (1, 2, 0))
    query_doc = jnp.where(
        docs[None, :] == jnp.arange(HEAD, dtype=jnp.float32)[:, None], DOC_QUERY, 0.0
    ).astype(jnp.bfloat16)
    q_aug = jnp.concatenate(
        [query_t, jnp.broadcast_to(query_doc[None], (heads, HEAD, rows_here))], axis=1
    )
    doc_rows = jnp.broadcast_to(docs[None, :], (8, rows_here))
    hidden, normed = attend(
        q_aug, key_norm, value_proj.T, doc_rows, residual, norm_gain, output_weight
    )
    token_rows = residual.shape[0]
    top_count = expert_ids.shape[1]
    experts_all = lax.axis_size("sp") * lax.axis_size("tp")
    capacity = max(2, 2 * token_rows * top_count // experts_all)
    flat_ids = expert_ids.reshape(-1)
    order = jnp.arange(flat_ids.shape[0], dtype=jnp.int32)
    earlier = jnp.logical_and(
        flat_ids[:, None] == flat_ids[None, :], order[None, :] < order[:, None]
    )
    arrival = jnp.sum(earlier.astype(jnp.int32), axis=1)
    slot_index = flat_ids * capacity + arrival
    slot_grid = slot_index.reshape(token_rows, top_count)
    placing = jnp.sum(
        (
            jnp.arange(experts_all * capacity, dtype=jnp.int32)[:, None, None] == slot_grid[None]
        ).astype(jnp.float32),
        axis=2,
    ).astype(jnp.bfloat16)
    outgoing = jnp.dot(placing, normed, preferred_element_type=jnp.float32).astype(jnp.bfloat16)
    spread = jnp.sum(
        jnp.where(
            jnp.arange(experts_all * capacity, dtype=jnp.int32)[None, None, :]
            == slot_grid[:, :, None],
            route_weights[:, :, None],
            0.0,
        ),
        axis=1,
    )
    high = spread.astype(jnp.bfloat16)
    low = (spread - high.astype(jnp.float32)).astype(jnp.bfloat16)
    outgoing = outgoing.reshape(experts_all, capacity, normed.shape[1])
    arrived = lax.all_to_all(outgoing, ("sp", "tp"), split_axis=0, concat_axis=0, tiled=True)
    sources, slots, width = arrived.shape
    flat_rows = arrived.reshape(sources * slots, width)
    gate_part = jnp.dot(flat_rows, gate_weight[0], preferred_element_type=jnp.float32)
    up_part = jnp.dot(flat_rows, up_weight[0], preferred_element_type=jnp.float32)
    activity = (jax.nn.silu(gate_part) * up_part).astype(jnp.bfloat16)
    expert_out = jnp.dot(activity, down_weight[0], preferred_element_type=jnp.float32).astype(
        jnp.bfloat16
    )
    returned = lax.all_to_all(
        expert_out.reshape(sources, slots, width),
        ("sp", "tp"),
        split_axis=0,
        concat_axis=0,
        tiled=True,
    )
    rows_back = returned.reshape(experts_all * capacity, -1)
    combined = jnp.dot(high, rows_back, preferred_element_type=jnp.float32) + jnp.dot(
        low, rows_back, preferred_element_type=jnp.float32
    )
    return (hidden.astype(jnp.float32) + combined).astype(jnp.bfloat16)


def on_device(*arrays):
    (
        residual, query_proj, key_proj, value_proj, query_gain, key_gain, document_ids,
        output_weight, norm_gain, expert_ids, route_weights, gate_weight, up_weight, down_weight,
    ) = arrays
    token_rows = residual.shape[0]
    top_count = expert_ids.shape[1]
    experts_all = lax.axis_size("sp") * lax.axis_size("tp")
    capacity = max(2, 2 * token_rows * top_count // experts_all)
    if (
        capacity % 16 == 0
        and token_rows == HEAD
        and token_rows % capacity == 0
        and experts_all % (token_rows // capacity) == 0
        and experts_all * capacity == LINE * token_rows
        and 2 * top_count <= 8
        and lax.axis_size("sp") % 2 == 0
    ):
        return run_layer(
            query_proj, key_proj, value_proj, document_ids.reshape(1, -1), query_gain, key_gain,
            expert_ids.T, route_weights.T, residual, norm_gain, output_weight,
            gate_weight, up_weight, down_weight, capacity,
        )
    return plain_on_device(*arrays)


def solution(mesh):
    in_specs = (
        P(("sp", "tp"), None),
        P("sp", "tp"),
        P("sp", "tp"),
        P("sp", "tp"),
        P(),
        P(),
        P("sp"),
        P(),
        P(),
        P(("sp", "tp"), None),
        P(("sp", "tp"), None),
        P(("sp", "tp"), None, None),
        P(("sp", "tp"), None, None),
        P(("sp", "tp"), None, None),
    )
    out_specs = P(("sp", "tp"), None)
    return jax.shard_map(
        on_device, mesh=mesh, in_specs=in_specs, out_specs=out_specs, check_vma=False
    )
```

```python
import functools
import math

import jax
import jax.numpy as jnp
from jax import lax
from jax.experimental import pallas as pl
from jax.experimental.pallas import tpu as pltpu
from jax.sharding import PartitionSpec as P

HEAD = 128
GRID_W = 64
REACH = 3


norm_eps = 1e-06
rope_base = 10000.0
masked_low = -1e30
MESH = pl.DeviceIdType.MESH
DOC_KEY = 128.0
DOC_QUERY = 64.0
PIECES = 4
ONES = 16
DOC_MARK = 32.0
HALVES = 2
LINE = 4
OFFSETS = (1, -2, 2, -1, 3, -3)
EXP2_SCALE = math.log2(math.e) / math.sqrt(HEAD)


def layer_kernel(
    n_sp, n_tp, capacity, top_count,
    q_hbm, k_hbm, v_hbm, doc_hbm, qg_hbm, kg_hbm, ids_hbm, rw_hbm, res_hbm, gain_hbm,
    wo_hbm, gate_hbm, up_hbm, down_hbm,
    new_ref,
    k_ref, v_ref, kg_ref, doc_ref, q_ref, qg_ref, ids_ref, rw_ref, res_ref, gain_ref,
    wo_v, gate_v, up_v, down_v, cos_s, sin_s, meta_s, q_aug, k_own, k_in, v_in, doc_in,
    k_aug, vt_s, m_s, acc_s, att_s, all_s, hid_s, nrm_s,
    metas, blocks, picked, arrived, answer, homing, returned, spread, total_s,
    back, joined, midway, summed,
    k_send, k_recv, v_send, v_recv, c_send, c_recv, t_send, t_recv,
    m_send, m_recv, z_send, z_recv, d_send, d_recv, h_send, h_recv, r_send, r_recv,
    b_send, b_recv, j_send, y_recv, s_recv, w_sem,
):
    devices = n_sp * n_tp
    rows = res_ref.shape[0]
    members = rows // capacity
    groups = devices // members
    piece = rows // PIECES
    sp = lax.axis_index("sp")
    tp = lax.axis_index("tp")
    me = sp * n_tp + tp
    plane = lax.div(me, members)
    pos = lax.rem(me, members)

    fetches = [
        pltpu.make_async_copy(source, into, w_sem.at[i])
        for i, (source, into) in enumerate(
            (
                (kg_hbm, kg_ref), (k_hbm, k_ref), (v_hbm, v_ref), (doc_hbm, doc_ref),
                (ids_hbm, ids_ref), (rw_hbm, rw_ref), (qg_hbm, qg_ref), (q_hbm, q_ref),
                (wo_hbm, wo_v), (res_hbm, res_ref), (gain_hbm, gain_ref),
                (gate_hbm.at[0], gate_v), (up_hbm.at[0], up_v), (down_hbm.at[0], down_v),
            )
        )
    ]
    for fetch in fetches:
        fetch.start()

    def fetched(*which):
        for i in which:
            fetches[i].wait()

    def place(device):
        return (lax.div(device, n_tp), lax.rem(device, n_tp))

    def region(index):
        return pl.ds(pl.multiple_of(index * capacity, capacity), capacity)

    length = k_ref.shape[0]
    heads = q_ref.shape[1] // HEAD
    width = att_s.shape[1]
    slots = len(OFFSETS)
    half = HEAD // 2
    side = 1 - 2 * lax.rem(sp, 2)
    across, ahead, behind = sp + side, sp + 2 * side, sp - 2 * side

    def inside(index):
        return jnp.logical_and(index >= 0, index < n_sp)

    has_ahead, has_behind = inside(ahead), inside(behind)
    has_spare = inside(sp + 4 * side)

    def offset(j):
        return sum(jnp.where(j == i, o, 0) for i, o in enumerate(OFFSETS))

    def exists(j):
        return inside(sp + side * offset(j))

    def reader(j):
        odd = OFFSETS[j] % 2 == 1
        return sp + side * OFFSETS[j] if odd else sp - side * OFFSETS[j]

    barrier = pltpu.get_barrier_semaphore()

    def greet(i, carry):
        there = lax.rem(me + i, devices)
        pl.semaphore_signal(barrier, inc=1, device_id=place(there), device_id_type=MESH)
        return carry

    lax.fori_loop(1, devices, greet, 0)

    def column(row):
        return jnp.broadcast_to(row, (HEAD, HEAD)).T[:, :1]

    freq_count = HEAD // 4
    exponent = lax.broadcasted_iota(jnp.int32, (freq_count, 1), 0).astype(jnp.float32) / freq_count
    inverse = jnp.exp2(exponent * -math.log2(rope_base))
    position = sp * length + lax.broadcasted_iota(jnp.int32, (1, length), 1)
    grid_row = lax.div(position, GRID_W).astype(jnp.float32)
    grid_col = lax.rem(position, GRID_W).astype(jnp.float32)
    angles = jnp.concatenate([inverse * grid_row, inverse * grid_col], axis=0)
    cos_s[...] = jnp.cos(angles)
    sin_s[...] = jnp.sin(angles)

    def turned(projected, gains):
        wide = projected.astype(jnp.float32).T
        scaled = (
            wide * lax.rsqrt(jnp.mean(wide * wide, axis=0, keepdims=True) + norm_eps) * gains
        )
        upper, lower = scaled[:half], scaled[half:]
        cosine, sine = cos_s[...], sin_s[...]
        return jnp.concatenate(
            [upper * cosine - lower * sine, upper * sine + lower * cosine], axis=0
        )

    fetched(0, 1)
    k_own[...] = turned(k_ref[...], column(kg_ref[...])).T.astype(jnp.bfloat16)
    fetched(2, 3, 4, 5)
    for k in range(top_count):
        for r, table in ((k, ids_ref), (top_count + k, rw_ref)):
            meta_s[r : r + 1, :] = table[k : k + 1, :].astype(jnp.float32)
    pl.semaphore_wait(barrier, devices - 1)

    def tell(i, block):
        return pltpu.make_async_remote_copy(
            src_ref=meta_s,
            dst_ref=metas.at[block],
            send_sem=m_send.at[i],
            recv_sem=m_recv.at[block],
            device_id=place(lax.rem(plane + i, groups) * members + pos),
            device_id_type=MESH,
        )

    def shift(source, into, sends, receives, i, there):
        return pltpu.make_async_remote_copy(
            src_ref=source,
            dst_ref=into.at[i],
            send_sem=sends.at[i],
            recv_sem=receives.at[i],
            device_id=(there, tp),
            device_id_type=MESH,
        )

    key_plan = (
        (k_own, across, True),
        (k_own, ahead, has_ahead),
        (k_own, behind, has_behind),
        (k_in.at[0], ahead, has_ahead),
        (k_in.at[0], behind, has_behind),
        (k_in.at[3], ahead, jnp.logical_and(has_ahead, has_behind)),
    )
    value_plan = (
        (v_ref, across, True),
        (v_ref, ahead, has_ahead),
        (v_ref, behind, has_behind),
        (v_in.at[2], across, has_ahead),
        (v_in.at[1], across, has_behind),
        (v_in.at[6], across, has_spare),
        (v_in.at[2], behind, jnp.logical_and(has_ahead, has_behind)),
    )

    def key_shift(i):
        return shift(key_plan[i][0], k_in, k_send, k_recv, i, key_plan[i][1])

    def value_shift(i):
        return shift(value_plan[i][0], v_in, v_send, v_recv, i, value_plan[i][1])

    def on(allowed, act):
        if allowed is True:
            act()
        elif allowed is not False:
            pl.when(allowed)(act)

    def start_keys(*which):
        for i in which:
            on(key_plan[i][2], lambda: key_shift(i).start())

    def start_values(*which):
        for i in which:
            on(value_plan[i][2], lambda: value_shift(i).start())

    def key_wait(j):
        shift(k_own, k_in, k_send, k_recv, j, sp).wait_recv()

    def value_wait(j):
        shift(v_ref, v_in, v_send, v_recv, j, sp).wait_recv()

    def doc_shift(j):
        return shift(doc_ref, doc_in, c_send, c_recv, j, reader(j))

    for j in range(slots):
        pl.when(inside(reader(j)))(lambda: doc_shift(j).start())
    start_keys(0, 1, 2)
    start_values(0, 1, 2)
    for i in range(1, groups):
        tell(i, plane).start()

    fetched(6, 7)
    query_gains = column(qg_ref[...]) * EXP2_SCALE
    for h in range(heads):
        q_aug[h, :HEAD, :] = turned(
            q_ref[:, h * HEAD : (h + 1) * HEAD], query_gains
        ).astype(jnp.bfloat16)
        labels = lax.broadcasted_iota(jnp.int32, (HEAD, length), 0)
        q_aug[h, HEAD:, :] = jnp.where(doc_ref[...] == labels, DOC_MARK, 0.0).astype(
            jnp.bfloat16
        )

    def take(keys, values, docs, first):
        doc_col = jnp.broadcast_to(docs[...].astype(jnp.float32), (HEAD, length)).T
        lanes = lax.broadcasted_iota(jnp.int32, (length, HEAD), 1).astype(jnp.float32)
        k_aug[:, :HEAD] = keys[...]
        k_aug[:, HEAD:] = jnp.where(doc_col == lanes, DOC_MARK, 0.0).astype(jnp.bfloat16)
        vt_s[:HEAD, :] = values[...].T
        for h in range(heads):
            s = jnp.dot(k_aug[...], q_aug[h], preferred_element_type=jnp.float32)
            top = jnp.max(s, axis=0, keepdims=True)
            if not first:
                top = jnp.maximum(m_s[h], top)
            e = jnp.exp2(s - top).astype(jnp.bfloat16)
            part = jnp.dot(vt_s[...], e, preferred_element_type=jnp.float32)
            acc_s[h] = part if first else acc_s[h] * jnp.exp2(m_s[h] - top) + part
            m_s[h] = top

    vt_s[HEAD:, :] = jnp.ones((ONES, length), jnp.bfloat16)
    take(k_own, v_ref, doc_ref, True)

    key_wait(0)
    start_keys(3, 4)

    @pl.when(has_ahead)
    def _():
        value_wait(2)
        start_values(3, 6)

    @pl.when(has_behind)
    def _():
        value_wait(1)
        start_values(4)

    def step(j, carry):
        @pl.when(exists(j))
        def _():
            @pl.when(jnp.logical_and(j != 0, j != 3))
            def _():
                key_wait(j)

            @pl.when(jnp.logical_and(j != 1, j != 2))
            def _():
                value_wait(j)

            shift(doc_ref, doc_in, c_send, c_recv, j, sp).wait_recv()
            take(k_in.at[j], v_in.at[j], doc_in.at[j], False)

        @pl.when(jnp.logical_and(j == 1, has_behind))
        def _():
            key_wait(3)
            start_keys(5)

        @pl.when(jnp.logical_and(j == 2, has_spare))
        def _():
            value_wait(6)
            start_values(5)

        return carry

    lax.fori_loop(0, slots, step, 0)

    for h in range(heads):
        out = acc_s[h, :HEAD, :] / acc_s[h, HEAD : HEAD + 1, :]
        att_s[:, h * HEAD : (h + 1) * HEAD] = out.T.astype(jnp.bfloat16)

    part_rows = rows // HALVES

    def exchange(k, half):
        there = lax.rem(tp + k, n_tp)
        here = pl.ds(pl.multiple_of(there * rows + half * part_rows, part_rows), part_rows)
        return pltpu.make_async_remote_copy(
            src_ref=att_s.at[here, :],
            dst_ref=all_s.at[tp, pl.ds(half * part_rows, part_rows)],
            send_sem=t_send.at[k, half],
            recv_sem=t_recv.at[k, half],
            device_id=(sp, there),
            device_id_type=MESH,
        )

    for half in range(HALVES):
        for k in range(n_tp - 1, 0, -1):
            exchange(k, half).start()
    fetched(8, 9, 10)

    def weight_rows(i):
        return wo_v[pl.ds(pl.multiple_of(i * width, width), width), :]

    total_s[...] = res_ref[...].astype(jnp.float32) + jnp.dot(
        att_s[pl.ds(pl.multiple_of(tp * rows, rows), rows), :],
        weight_rows(tp),
        preferred_element_type=jnp.float32,
    )

    def project(half):
        part = pl.ds(half * part_rows, part_rows)
        projected = total_s[part, :]
        for k in range(1, n_tp):
            exchange(k, half).wait_recv()
            source = lax.rem(tp - k + n_tp, n_tp)
            projected += jnp.dot(
                all_s[source, part, :], weight_rows(source), preferred_element_type=jnp.float32
            )
        hidden = projected.astype(jnp.bfloat16)
        hid_s[part, :] = hidden
        wide = hidden.astype(jnp.float32)
        mean = jnp.mean(wide * wide, axis=-1, keepdims=True)
        nrm_s[part, :] = (wide * lax.rsqrt(mean + norm_eps) * gain_ref[...]).astype(jnp.bfloat16)

    def pass_on(source, block, way, c):
        part = pl.ds(c * piece, piece)
        return pltpu.make_async_remote_copy(
            src_ref=source.at[part],
            dst_ref=blocks.at[block, part],
            send_sem=z_send.at[way, block, c],
            recv_sem=z_recv.at[block, c],
            device_id=place(me + (2 * way - 1) * members),
            device_id_type=MESH,
        )

    def dispatch(block, peer, landing):
        return pltpu.make_async_remote_copy(
            src_ref=picked.at[block, region(peer)],
            dst_ref=arrived.at[block, region(landing)],
            send_sem=d_send.at[block, peer],
            recv_sem=d_recv.at[block, landing],
            device_id=place(plane * members + peer),
            device_id_type=MESH,
        )

    def give_home(block, origin, c):
        part = pl.ds(c * piece, piece)
        return pltpu.make_async_remote_copy(
            src_ref=answer.at[block, part],
            dst_ref=homing.at[origin, part],
            send_sem=h_send.at[block, c],
            recv_sem=h_recv.at[origin, c],
            device_id=place(block * members + pos),
            device_id_type=MESH,
        )

    def give_back(source, origin, member, landing):
        return pltpu.make_async_remote_copy(
            src_ref=source.at[region(member)],
            dst_ref=returned.at[region(origin * members + landing)],
            send_sem=r_send.at[origin, member],
            recv_sem=r_recv.at[origin, landing],
            device_id=place(plane * members + member),
            device_id_type=MESH,
        )

    def give_across(block, member, landing):
        return pltpu.make_async_remote_copy(
            src_ref=answer.at[block, region(member)],
            dst_ref=back.at[block, region(landing)],
            send_sem=b_send.at[block, member],
            recv_sem=b_recv.at[block, landing],
            device_id=place(plane * members + member),
            device_id_type=MESH,
        )

    def give_next(block, way, c):
        part = pl.ds(c * piece, piece)
        return pltpu.make_async_remote_copy(
            src_ref=joined.at[block, part],
            dst_ref=midway.at[way, part],
            send_sem=j_send.at[block, c],
            recv_sem=y_recv.at[way, c],
            device_id=place(me + (1 - 2 * way) * members),
            device_id_type=MESH,
        )

    def give_sum(block, way, c):
        part = pl.ds(c * piece, piece)
        return pltpu.make_async_remote_copy(
            src_ref=joined.at[block, part],
            dst_ref=summed.at[way, part],
            send_sem=j_send.at[block, c],
            recv_sem=s_recv.at[way, c],
            device_id=place(block * members + pos),
            device_id_type=MESH,
        )

    def others(act, first=1):
        def one(i, carry):
            act(lax.rem(pos + i, members))
            return carry

        lax.fori_loop(first, members, one, 0)

    low_side = plane < groups // 2
    toward = jnp.where(low_side, 1, -1)
    seen = jnp.where(low_side, 0, 1)
    inward, outward = 1 - seen, seen
    is_end = jnp.logical_or(plane == 0, plane == groups - 1)
    is_inner = jnp.logical_not(is_end)
    first = jnp.where(is_end, plane + toward, plane - toward)
    second = jnp.where(is_end, plane + 3 * toward, plane + 2 * toward)
    third = jnp.where(is_end, plane + 2 * toward, plane + toward)
    early, late = range(PIECES // 2), range(PIECES // 2, PIECES)

    def push(source, block, way, which):
        for c in which:
            pass_on(source, block, way, c).start()

    def landed(block, which):
        for c in which:
            pass_on(nrm_s, block, 0, c).wait_recv()

    def hop(block, way, which):
        for c in which:
            landed(block, (c,))
            push(blocks.at[block], block, way, (c,))

    for half in range(HALVES):
        project(half)
        ready = range(half * PIECES // HALVES, (half + 1) * PIECES // HALVES)

        @pl.when(is_end)
        def _():
            push(nrm_s, plane, inward, ready)

        @pl.when(is_inner)
        def _():
            for c in ready:
                push(nrm_s, plane, outward, (c,))
                if c in early:
                    push(nrm_s, plane, inward, (c,))

    def slot_rows(meta):
        experts = lax.broadcasted_iota(jnp.int32, (devices, rows), 0).astype(jnp.float32)
        hits = [experts == meta[k : k + 1, :] for k in range(top_count)]
        named = sum(hit.astype(jnp.float32) for hit in hits)
        ahead = (
            lax.broadcasted_iota(jnp.int32, (rows, rows), 0)
            < lax.broadcasted_iota(jnp.int32, (rows, rows), 1)
        )
        before = jnp.dot(
            named.astype(jnp.bfloat16),
            ahead.astype(jnp.float32).astype(jnp.bfloat16),
            preferred_element_type=jnp.float32,
        )
        return [
            meta[k : k + 1, :] * capacity
            + jnp.sum(jnp.where(hits[k], before, 0.0), axis=0, keepdims=True)
            for k in range(top_count)
        ]

    def slot_numbers(group):
        return (
            lax.broadcasted_iota(jnp.int32, (rows, rows), 0) + group * rows
        ).astype(jnp.float32)

    def gather(source, meta, block):
        numbers = slot_numbers(plane)
        choice = sum((numbers == row).astype(jnp.float32) for row in slot_rows(meta))
        picked[block] = jnp.dot(
            choice.astype(jnp.bfloat16), source[...], preferred_element_type=jnp.float32
        ).astype(jnp.bfloat16)
        others(lambda peer: dispatch(block, peer, pos).start())
        arrived[block, region(pos), :] = picked[block, region(pos), :]

    def expert(block):
        others(lambda peer: dispatch(block, peer, peer).wait_recv())
        x = arrived[block]
        gate_part = jnp.dot(x, gate_v[...], preferred_element_type=jnp.float32)
        up_part = jnp.dot(x, up_v[...], preferred_element_type=jnp.float32)
        activity = (jax.nn.silu(gate_part) * up_part).astype(jnp.bfloat16)
        answer[block] = jnp.dot(
            activity, down_v[...], preferred_element_type=jnp.float32
        ).astype(jnp.bfloat16)

    gather(nrm_s, meta_s[...], plane)
    own_slots = slot_rows(meta_s[...])
    for g in range(groups):
        numbers = slot_numbers(g)
        weights = sum(
            jnp.where(numbers == own_slots[k], meta_s[top_count + k : top_count + k + 1, :], 0.0)
            for k in range(top_count)
        ).T
        high = weights.astype(jnp.bfloat16)
        spread[g, 0] = high
        spread[g, 1] = (weights - high.astype(jnp.float32)).astype(jnp.bfloat16)
    fetched(11, 12, 13)

    def collect(block):
        tell(1, block).wait_recv()
        gather(blocks.at[block], metas[block], block)

    def serve_home(block):
        expert(block)
        for c in range(PIECES):
            give_home(block, plane, c).start()

    def serve_across(block):
        expert(block)
        others(lambda member: give_across(block, member, pos).start())
        back[block, region(pos), :] = answer[block, region(pos), :]

    def join(block):
        others(lambda member: give_across(block, member, member).wait_recv())
        meta = metas[block]
        numbers = slot_numbers(plane)
        lines = slot_rows(meta)
        weights = sum(
            jnp.where(numbers == lines[k], meta[top_count + k : top_count + k + 1, :], 0.0)
            for k in range(top_count)
        ).T
        high = weights.astype(jnp.bfloat16)
        low = (weights - high.astype(jnp.float32)).astype(jnp.bfloat16)
        joined[block] = (
            jnp.dot(high, back[block], preferred_element_type=jnp.float32)
            + jnp.dot(low, back[block], preferred_element_type=jnp.float32)
        ).astype(jnp.bfloat16)

    def share(origin):
        for c in range(PIECES):
            give_home(origin, origin, c).wait_recv()
            for i in range(c * members // PIECES, (c + 1) * members // PIECES):

                @pl.when(pos != i)
                def _():
                    give_back(homing.at[origin], origin, i, pos).start()

        returned[region(origin * members + pos), :] = homing[origin, region(pos), :]

    @pl.when(is_inner)
    def _():
        hop(first, inward, range(PIECES - 1))
        hop(second, outward, (0,))
        hop(first, inward, (PIECES - 1,))
        push(nrm_s, plane, inward, late)
        hop(second, outward, (1,))

    @pl.when(is_end)
    def _():
        landed(first, range(PIECES))

    collect(first)
    expert(plane)
    others(lambda member: give_back(answer.at[plane], plane, member, pos).start())
    returned[region(me), :] = answer[plane, region(pos), :]

    @pl.when(is_inner)
    def _():
        hop(second, outward, range(2, PIECES))
        hop(third, outward, early)

    @pl.when(is_end)
    def _():
        landed(second, range(PIECES))

    collect(second)
    serve_home(first)

    @pl.when(is_end)
    def _():
        serve_across(second)
        landed(third, range(PIECES))
        join(second)
        for c in range(PIECES):
            give_next(second, seen, c).start()
        share(first)

    @pl.when(is_inner)
    def _():
        hop(third, outward, late)

    collect(third)

    @pl.when(is_inner)
    def _():
        serve_across(second)

    serve_home(third)

    @pl.when(is_inner)
    def _():
        share(first)
        join(second)
        for c in range(PIECES):
            part = pl.ds(c * piece, piece)
            give_next(second, seen, c).wait_recv()
            joined[second, part, :] = (
                joined[second, part, :].astype(jnp.float32)
                + midway[seen, part, :].astype(jnp.float32)
            ).astype(jnp.bfloat16)
            give_sum(second, seen, c).start()
        share(third)
        share(second)

    total = hid_s[...].astype(jnp.float32)

    def combine(group):
        back = returned[pl.ds(pl.multiple_of(group * rows, rows), rows), :]
        part = jnp.dot(spread[group, 0], back, preferred_element_type=jnp.float32)
        return part + jnp.dot(spread[group, 1], back, preferred_element_type=jnp.float32)

    def gathered(origin):
        others(lambda member: give_back(homing.at[origin], origin, member, member).wait_recv())
        return combine(origin)

    total_s[...] = total + gathered(plane) + gathered(first)

    @pl.when(is_inner)
    def _():
        total_s[...] += gathered(third)
        total_s[...] += gathered(second)

    @pl.when(is_end)
    def _():
        for c in range(PIECES):
            give_sum(third, 1 - seen, c).wait_recv()
        total_s[...] += summed[1 - seen].astype(jnp.float32)

    new_ref[...] = total_s[...].astype(jnp.bfloat16)

    for i in range(1, groups):
        tell(i, plane).wait_send()

    def gone(block, way):
        for c in range(PIECES):
            pass_on(nrm_s, block, way, c).wait_send()

    gone(plane, inward)

    @pl.when(is_inner)
    def _():
        gone(plane, outward)
        gone(first, inward)
        gone(second, outward)
        gone(third, outward)

    others(lambda peer: dispatch(plane, peer, pos).wait_send())
    others(lambda member: give_back(answer.at[plane], plane, member, pos).wait_send())
    for block in (first, second, third):
        others(lambda peer: dispatch(block, peer, pos).wait_send())
    for block in (first, third):
        for c in range(PIECES):
            give_home(block, plane, c).wait_send()
    others(lambda member: give_across(second, member, pos).wait_send())
    for c in range(PIECES):
        give_next(second, seen, c).wait_send()
    others(lambda member: give_back(homing.at[first], first, member, pos).wait_send())

    @pl.when(is_inner)
    def _():
        for block in (second, third):
            others(lambda member: give_back(homing.at[block], block, member, pos).wait_send())

    for i in range(slots):
        on(key_plan[i][2], lambda: key_shift(i).wait_send())
        pl.when(inside(reader(i)))(lambda: doc_shift(i).wait_send())
    for i in range(slots + 1):
        on(value_plan[i][2], lambda: value_shift(i).wait_send())
    for k in range(1, n_tp):
        for half in range(HALVES):
            exchange(k, half).wait_send()


def run_layer(
    query_proj, key_proj, value_proj, docs, query_gain, key_gain, expert_ids, route_weights,
    residual, norm_gain, output_weight, gate_weight, up_weight, down_weight, capacity,
):
    n_sp, n_tp = lax.axis_size("sp"), lax.axis_size("tp")
    length = key_proj.shape[0]
    heads = query_proj.shape[1] // HEAD
    rows, model = residual.shape
    top_count = expert_ids.shape[0]
    members = rows // capacity
    groups = n_sp * n_tp // members
    slots = len(OFFSETS)
    block = (length, HEAD)
    narrow = jnp.bfloat16
    vmem = pl.BlockSpec(memory_space=pltpu.VMEM)
    buffer = pltpu.VMEM((groups, rows, model), narrow)
    dma = pltpu.SemaphoreType.DMA
    return pl.pallas_call(
        functools.partial(layer_kernel, n_sp, n_tp, capacity, top_count),
        out_shape=jax.ShapeDtypeStruct(residual.shape, narrow),
        in_specs=[pl.BlockSpec(memory_space=pltpu.HBM)] * 14,
        out_specs=vmem,
        scratch_shapes=[
            pltpu.VMEM(block, narrow),
            pltpu.VMEM(block, narrow),
            pltpu.VMEM((1, HEAD), jnp.float32),
            pltpu.VMEM(docs.shape, jnp.int32),
            pltpu.VMEM(query_proj.shape, narrow),
            pltpu.VMEM((1, HEAD), jnp.float32),
            pltpu.VMEM(expert_ids.shape, jnp.int32),
            pltpu.VMEM(route_weights.shape, jnp.float32),
            pltpu.VMEM(residual.shape, narrow),
            pltpu.VMEM((1, model), jnp.float32),
            pltpu.VMEM(output_weight.shape, narrow),
            pltpu.VMEM(gate_weight.shape[1:], narrow),
            pltpu.VMEM(up_weight.shape[1:], narrow),
            pltpu.VMEM(down_weight.shape[1:], narrow),
            pltpu.VMEM((HEAD // 2, length), jnp.float32),
            pltpu.VMEM((HEAD // 2, length), jnp.float32),
            pltpu.VMEM((8, rows), jnp.float32),
            pltpu.VMEM((heads, 2 * HEAD, length), narrow),
            pltpu.VMEM(block, narrow),
            pltpu.VMEM((slots,) + block, narrow),
            pltpu.VMEM((slots + 1,) + block, narrow),
            pltpu.VMEM((slots,) + docs.shape, jnp.int32),
            pltpu.VMEM((length, 2 * HEAD), narrow),
            pltpu.VMEM((HEAD + ONES, length), narrow),
            pltpu.VMEM((heads, 1, length), jnp.float32),
            pltpu.VMEM((heads, HEAD + ONES, length), jnp.float32),
            pltpu.VMEM((length, heads * HEAD), narrow),
            pltpu.VMEM((n_tp, rows, heads * HEAD), narrow),
            pltpu.VMEM((rows, model), narrow),
            pltpu.VMEM((rows, model), narrow),
            pltpu.VMEM((groups, 8, rows), jnp.float32),
            buffer,
            buffer,
            buffer,
            buffer,
            buffer,
            pltpu.VMEM((groups * rows, model), narrow),
            pltpu.VMEM((groups, 2, rows, rows), narrow),
            pltpu.VMEM((rows, model), jnp.float32),
            buffer,
            buffer,
            pltpu.VMEM((2, rows, model), narrow),
            pltpu.VMEM((2, rows, model), narrow),
            dma((slots,)),
            dma((slots,)),
            dma((slots + 1,)),
            dma((slots + 1,)),
            dma((slots,)),
            dma((slots,)),
            dma((n_tp, HALVES)),
            dma((n_tp, HALVES)),
            dma((groups,)),
            dma((groups,)),
            dma((2, groups, PIECES)),
            dma((groups, PIECES)),
            dma((groups, members)),
            dma((groups, members)),
            dma((groups, PIECES)),
            dma((groups, PIECES)),
            dma((groups, members)),
            dma((groups, members)),
            dma((groups, members)),
            dma((groups, members)),
            dma((groups, PIECES)),
            dma((2, PIECES)),
            dma((2, PIECES)),
            dma((14,)),
        ],
        compiler_params=pltpu.CompilerParams(
            collective_id=1, has_side_effects=True, vmem_limit_bytes=60 * 1024 * 1024
        ),
    )(
        query_proj, key_proj, value_proj, docs,
        query_gain.reshape(1, -1), key_gain.reshape(1, -1), expert_ids, route_weights,
        residual, norm_gain.reshape(1, -1),
        output_weight, gate_weight, up_weight, down_weight,
    )


def rotary_tables(first_row, length):
    freq_count = HEAD // 4
    inverse = 1.0 / rope_base ** (jnp.arange(freq_count, dtype=jnp.float32) / freq_count)
    position = first_row + jnp.arange(length, dtype=jnp.int32)
    grid_row = (position // GRID_W).astype(jnp.float32)
    grid_col = (position % GRID_W).astype(jnp.float32)
    angles = jnp.concatenate(
        [grid_row[:, None] * inverse[None, :], grid_col[:, None] * inverse[None, :]], axis=1
    )
    return (jnp.cos(angles), jnp.sin(angles))


def norm_rotate(projected, gains, cosine, sine_table):
    length = projected.shape[0]
    values_wide = projected.astype(jnp.float32).reshape(length, -1, HEAD)
    scaled = (
        values_wide
        * lax.rsqrt(jnp.mean(values_wide * values_wide, axis=-1, keepdims=True) + norm_eps)
        * gains
    )
    half_size = HEAD // 2
    first_half = scaled[..., :half_size]
    second_half = scaled[..., half_size:]
    cosine_rows = cosine[:, None, :]
    sine_rows = sine_table[:, None, :]
    turned = jnp.concatenate(
        [
            first_half * cosine_rows - second_half * sine_rows,
            first_half * sine_rows + second_half * cosine_rows,
        ],
        axis=-1,
    )
    return turned.reshape(length, -1).astype(jnp.bfloat16)


def attention_kernel(
    n_sp, n_tp, q_ref, k_ref, vt_ref, doc_ref, res_ref, gain_ref, wo_hbm,
    hid_ref, nrm_ref,
    wo_v, k_in, vt_in, doc_in, k_aug, m_s, l_s, acc_s, att_s, all_s,
    send, recv, t_send, t_recv, w_sem,
):
    sp = lax.axis_index("sp")
    tp = lax.axis_index("tp")
    heads = q_ref.shape[0]
    rows = res_ref.shape[0]
    width = att_s.shape[1]
    slots = 2 * REACH

    def distance(j):
        return (j // 2 + 1) * (1 - 2 * (j % 2))

    def inside(index):
        return jnp.logical_and(index >= 0, index < n_sp)

    wo_copy = pltpu.make_async_copy(wo_hbm, wo_v, w_sem)
    wo_copy.start()

    barrier = pltpu.get_barrier_semaphore()
    for j in range(slots):
        there = sp + distance(j)

        @pl.when(inside(there))
        def _():
            pl.semaphore_signal(barrier, inc=1, device_id=(there, tp), device_id_type=MESH)

    for k in range(1, n_tp):
        pl.semaphore_signal(
            barrier, inc=1, device_id=(sp, lax.rem(tp + k, n_tp)), device_id_type=MESH
        )
    beside = jnp.minimum(sp, REACH) + jnp.minimum(n_sp - 1 - sp, REACH)
    pl.semaphore_wait(barrier, n_tp - 1 + beside)

    def copies(j):
        there = (sp + distance(j), tp)
        return [
            pltpu.make_async_remote_copy(
                src_ref=one,
                dst_ref=into.at[j],
                send_sem=send.at[j, i],
                recv_sem=recv.at[j, i],
                device_id=there,
                device_id_type=MESH,
            )
            for i, (one, into) in enumerate(((k_ref, k_in), (vt_ref, vt_in), (doc_ref, doc_in)))
        ]

    for j in range(slots):

        @pl.when(inside(sp + distance(j)))
        def _():
            for copy in copies(j):
                copy.start()

    def take(keys, values_t, docs, first):
        length = keys.shape[0]
        doc_col = jnp.broadcast_to(docs[0:1, :], (HEAD, length)).T
        lanes = lax.broadcasted_iota(jnp.int32, (length, HEAD), 1).astype(jnp.float32)
        k_aug[:, :HEAD] = keys[...]
        k_aug[:, HEAD:] = jnp.where(doc_col == lanes, DOC_KEY, 0.0).astype(jnp.bfloat16)
        for h in range(heads):
            s = jnp.dot(k_aug[...], q_ref[h], preferred_element_type=jnp.float32)
            top = jnp.max(s, axis=0, keepdims=True)
            if not first:
                top = jnp.maximum(m_s[h], top)
            e = jnp.exp2((s - top) * EXP2_SCALE)
            den = jnp.sum(e, axis=0, keepdims=True)
            part = jnp.dot(
                values_t[...], e.astype(jnp.bfloat16), preferred_element_type=jnp.float32
            )
            if first:
                l_s[h] = den
                acc_s[h] = part
            else:
                old = jnp.exp2((m_s[h] - top) * EXP2_SCALE)
                l_s[h] = l_s[h] * old + den
                acc_s[h] = acc_s[h] * old + part
            m_s[h] = top

    take(k_ref, vt_ref, doc_ref, True)

    def step(j, carry):
        @pl.when(inside(sp - distance(j)))
        def _():
            for copy in copies(j):
                copy.wait_recv()
            take(k_in.at[j], vt_in.at[j], doc_in.at[j], False)

        return carry

    lax.fori_loop(0, slots, step, 0)

    for h in range(heads):
        out = acc_s[h] / l_s[h]
        att_s[:, h * HEAD : (h + 1) * HEAD] = out.T.astype(jnp.bfloat16)

    def exchange(k):
        there = lax.rem(tp + k, n_tp)
        return pltpu.make_async_remote_copy(
            src_ref=att_s.at[pl.ds(pl.multiple_of(there * rows, rows), rows), :],
            dst_ref=all_s.at[tp],
            send_sem=t_send.at[k],
            recv_sem=t_recv.at[k],
            device_id=(sp, there),
            device_id_type=MESH,
        )

    for k in range(n_tp - 1, 0, -1):
        exchange(k).start()
    wo_copy.wait()

    def weight_rows(i):
        return wo_v[pl.ds(pl.multiple_of(i * width, width), width), :]

    projected = jnp.dot(
        att_s[pl.ds(pl.multiple_of(tp * rows, rows), rows), :],
        weight_rows(tp),
        preferred_element_type=jnp.float32,
    )
    for k in range(1, n_tp):
        exchange(k).wait_recv()
        source = lax.rem(tp - k + n_tp, n_tp)
        projected += jnp.dot(
            all_s[source], weight_rows(source), preferred_element_type=jnp.float32
        )
    hidden = (res_ref[...].astype(jnp.float32) + projected).astype(jnp.bfloat16)
    hid_ref[...] = hidden
    wide = hidden.astype(jnp.float32)
    mean = jnp.mean(wide * wide, axis=-1, keepdims=True)
    nrm_ref[...] = (wide * lax.rsqrt(mean + norm_eps) * gain_ref[...]).astype(jnp.bfloat16)

    for j in range(slots):

        @pl.when(inside(sp + distance(j)))
        def _():
            for copy in copies(j):
                copy.wait_send()

    for k in range(1, n_tp):
        exchange(k).wait_send()


def attend(q_aug, key_norm, value_t, doc_rows, residual, norm_gain, output_weight):
    n_sp, n_tp = lax.axis_size("sp"), lax.axis_size("tp")
    heads, deep, length = q_aug.shape
    rows, model = residual.shape
    vmem = pl.BlockSpec(memory_space=pltpu.VMEM)
    slots = 2 * REACH
    return pl.pallas_call(
        functools.partial(attention_kernel, n_sp, n_tp),
        out_shape=[jax.ShapeDtypeStruct((rows, model), jnp.bfloat16)] * 2,
        in_specs=[vmem] * 6 + [pl.BlockSpec(memory_space=pl.ANY)],
        out_specs=[vmem] * 2,
        scratch_shapes=[
            pltpu.VMEM(output_weight.shape, jnp.bfloat16),
            pltpu.VMEM((slots,) + key_norm.shape, jnp.bfloat16),
            pltpu.VMEM((slots,) + value_t.shape, jnp.bfloat16),
            pltpu.VMEM((slots,) + doc_rows.shape, jnp.float32),
            pltpu.VMEM((length, deep), jnp.bfloat16),
            pltpu.VMEM((heads, 1, length), jnp.float32),
            pltpu.VMEM((heads, 1, length), jnp.float32),
            pltpu.VMEM((heads, HEAD, length), jnp.float32),
            pltpu.VMEM((length, heads * HEAD), jnp.bfloat16),
            pltpu.VMEM((n_tp, rows, heads * HEAD), jnp.bfloat16),
            pltpu.SemaphoreType.DMA((slots, 3)),
            pltpu.SemaphoreType.DMA((slots, 3)),
            pltpu.SemaphoreType.DMA((n_tp,)),
            pltpu.SemaphoreType.DMA((n_tp,)),
            pltpu.SemaphoreType.DMA(()),
        ],
        compiler_params=pltpu.CompilerParams(
            collective_id=1, has_side_effects=True, vmem_limit_bytes=48 * 1024 * 1024
        ),
    )(q_aug, key_norm, value_t, doc_rows, residual, norm_gain.reshape(1, -1), output_weight)


def plain_on_device(
    residual,
    query_proj,
    key_proj,
    value_proj,
    query_gain,
    key_gain,
    document_ids,
    output_weight,
    norm_gain,
    expert_ids,
    route_weights,
    gate_weight,
    up_weight,
    down_weight,
):
    rows_here = query_proj.shape[0]
    cosine, sine_table = rotary_tables(lax.axis_index("sp") * rows_here, rows_here)
    query_norm = norm_rotate(query_proj, query_gain, cosine, sine_table)
    key_norm = norm_rotate(key_proj, key_gain, cosine, sine_table)
    heads = query_proj.shape[1] // HEAD
    docs = document_ids.astype(jnp.float32)
    query_t = jnp.transpose(query_norm.reshape(rows_here, heads, HEAD), (1, 2, 0))
    query_doc = jnp.where(
        docs[None, :] == jnp.arange(HEAD, dtype=jnp.float32)[:, None], DOC_QUERY, 0.0
    ).astype(jnp.bfloat16)
    q_aug = jnp.concatenate(
        [query_t, jnp.broadcast_to(query_doc[None], (heads, HEAD, rows_here))], axis=1
    )
    doc_rows = jnp.broadcast_to(docs[None, :], (8, rows_here))
    hidden, normed = attend(
        q_aug, key_norm, value_proj.T, doc_rows, residual, norm_gain, output_weight
    )
    token_rows = residual.shape[0]
    top_count = expert_ids.shape[1]
    experts_all = lax.axis_size("sp") * lax.axis_size("tp")
    capacity = max(2, 2 * token_rows * top_count // experts_all)
    flat_ids = expert_ids.reshape(-1)
    order = jnp.arange(flat_ids.shape[0], dtype=jnp.int32)
    earlier = jnp.logical_and(
        flat_ids[:, None] == flat_ids[None, :], order[None, :] < order[:, None]
    )
    arrival = jnp.sum(earlier.astype(jnp.int32), axis=1)
    slot_index = flat_ids * capacity + arrival
    slot_grid = slot_index.reshape(token_rows, top_count)
    placing = jnp.sum(
        (
            jnp.arange(experts_all * capacity, dtype=jnp.int32)[:, None, None] == slot_grid[None]
        ).astype(jnp.float32),
        axis=2,
    ).astype(jnp.bfloat16)
    outgoing = jnp.dot(placing, normed, preferred_element_type=jnp.float32).astype(jnp.bfloat16)
    spread = jnp.sum(
        jnp.where(
            jnp.arange(experts_all * capacity, dtype=jnp.int32)[None, None, :]
            == slot_grid[:, :, None],
            route_weights[:, :, None],
            0.0,
        ),
        axis=1,
    )
    high = spread.astype(jnp.bfloat16)
    low = (spread - high.astype(jnp.float32)).astype(jnp.bfloat16)
    outgoing = outgoing.reshape(experts_all, capacity, normed.shape[1])
    arrived = lax.all_to_all(outgoing, ("sp", "tp"), split_axis=0, concat_axis=0, tiled=True)
    sources, slots, width = arrived.shape
    flat_rows = arrived.reshape(sources * slots, width)
    gate_part = jnp.dot(flat_rows, gate_weight[0], preferred_element_type=jnp.float32)
    up_part = jnp.dot(flat_rows, up_weight[0], preferred_element_type=jnp.float32)
    activity = (jax.nn.silu(gate_part) * up_part).astype(jnp.bfloat16)
    expert_out = jnp.dot(activity, down_weight[0], preferred_element_type=jnp.float32).astype(
        jnp.bfloat16
    )
    returned = lax.all_to_all(
        expert_out.reshape(sources, slots, width),
        ("sp", "tp"),
        split_axis=0,
        concat_axis=0,
        tiled=True,
    )
    rows_back = returned.reshape(experts_all * capacity, -1)
    combined = jnp.dot(high, rows_back, preferred_element_type=jnp.float32) + jnp.dot(
        low, rows_back, preferred_element_type=jnp.float32
    )
    return (hidden.astype(jnp.float32) + combined).astype(jnp.bfloat16)


def on_device(*arrays):
    (
        residual, query_proj, key_proj, value_proj, query_gain, key_gain, document_ids,
        output_weight, norm_gain, expert_ids, route_weights, gate_weight, up_weight, down_weight,
    ) = arrays
    token_rows = residual.shape[0]
    top_count = expert_ids.shape[1]
    experts_all = lax.axis_size("sp") * lax.axis_size("tp")
    capacity = max(2, 2 * token_rows * top_count // experts_all)
    if (
        capacity % 16 == 0
        and token_rows == HEAD
        and token_rows % capacity == 0
        and experts_all % (token_rows // capacity) == 0
        and experts_all * capacity == LINE * token_rows
        and 2 * top_count <= 8
        and lax.axis_size("sp") % 2 == 0
    ):
        return run_layer(
            query_proj, key_proj, value_proj, document_ids.reshape(1, -1), query_gain, key_gain,
            expert_ids.T, route_weights.T, residual, norm_gain, output_weight,
            gate_weight, up_weight, down_weight, capacity,
        )
    return plain_on_device(*arrays)


def solution(mesh):
    in_specs = (
        P(("sp", "tp"), None),
        P("sp", "tp"),
        P("sp", "tp"),
        P("sp", "tp"),
        P(),
        P(),
        P("sp"),
        P(),
        P(),
        P(("sp", "tp"), None),
        P(("sp", "tp"), None),
        P(("sp", "tp"), None, None),
        P(("sp", "tp"), None, None),
        P(("sp", "tp"), None, None),
    )
    out_specs = P(("sp", "tp"), None)
    return jax.shard_map(
        on_device, mesh=mesh, in_specs=in_specs, out_specs=out_specs, check_vma=False
    )
```
